32 devices in a mesh: sp: 8 (over z, x), tp: 4 (over y, core).
Axes of the slice: x: 2, y: 2, z: 4, core: 2. Of those that a mesh axis runs over, the one named last changes fastest.
Arguments:
- query_small: bfloat16 [6144, 1024], P('sp', 'tp'), may hold values from -6 to 6
- key_small: bfloat16 [6144, 1024], P('sp', 'tp'), may hold values from -6 to 6
- value_small: bfloat16 [6144, 1024], P('sp', 'tp'), may hold values from -6 to 6
- gates_small: float32 [6144, 16], P('sp', 'tp'), as said below
- query_large: bfloat16 [6144, 1024], P('sp', 'tp'), may hold values from -6 to 6
- key_large: bfloat16 [6144, 1024], P('sp', 'tp'), may hold values from -6 to 6
- value_large: bfloat16 [6144, 1024], P('sp', 'tp'), may hold values from -6 to 6
- gates_large: float32 [6144, 8], P('sp', 'tp'), as said below
- residual: bfloat16 [6144, 2048], P(('sp', 'tp')), may hold values from -6 to 6
- mixer_small: bfloat16 [1024, 2048], P('tp'), may hold values from -1 to 1
- mixer_large: bfloat16 [1024, 2048], P('tp'), may hold values from -1 to 1
- mix_gain: float32 [2048], replicated, may hold values from 0.1 to 1.9
- value_weight: bfloat16 [2048, 5632], P('sp', 'tp'), may hold values from -0.125 to 0.125
- gate_weight: bfloat16 [2048, 5632], P('sp', 'tp'), may hold values from -0.125 to 0.125
- value_taps: float32 [3, 5632], P(None, 'tp'), may hold values from -3 to 3
- gate_taps: float32 [3, 5632], P(None, 'tp'), may hold values from -3 to 3
- down_weight: bfloat16 [5632, 2048], P('tp', 'sp'), may hold values from -0.078125 to 0.078125
- final_gain: float32 [2048], replicated, may hold values from 0.1 to 1.9
Outputs:
- layer_out: bfloat16 [6144, 2048], P(('sp', 'tp'))
The draws below stay inside these ranges and needn't reach their ends.
Inputs may be any that keep to these rules, and one draw needn't show every extreme that they name: `gates_small`: each column never rises from one position to the next, and its first entry is negative. `gates_large`: each column never rises from one position to the next, and its first entry is negative.
All inputs are finite; a program needn't handle non-finite values.
Results may differ from the reference program's by a relative error of at most 0.018.
Values may be sent and summed in bfloat16 or wider, within the bound.
A program may use at most 128 MiB of HBM per device.

```python
import math
import jax
import jax.numpy as jnp
from jax import lax

D = 2048
FF = 5632
HS = 16
DS = 64
HL = 8
DL = 128
TOK_DEV = 768
SEQUENCE_TOKENS = 6144


def plant_pair(key, head_group, head_dim, salt):
    base_level = jax.random.fold_in(key, salt)
    width = head_group * head_dim
    queries = jnp.clip(jax.random.normal(jax.random.fold_in(base_level, 1), (SEQUENCE_TOKENS, width), jnp.float32), -6.0, 6.0)
    key_rows = jnp.clip(jax.random.normal(jax.random.fold_in(base_level, 2), (SEQUENCE_TOKENS, width), jnp.float32), -6.0, 6.0)
    return (queries, key_rows)


def gate_totals(key, head_group, salt):
    base_level = jax.random.fold_in(key, salt)
    share_fast = 0.5
    rapid_decay = jax.random.uniform(jax.random.fold_in(base_level, 1), (head_group,), jnp.float32) < share_fast
    rate = jnp.where(rapid_decay, 1.0 / 40.0, 0.5 / SEQUENCE_TOKENS)
    block_count = SEQUENCE_TOKENS // TOK_DEV
    factor = jnp.exp(jax.random.uniform(jax.random.fold_in(base_level, 2), (block_count, head_group), jnp.float32, -0.7, 0.7))
    factor = jnp.repeat(factor, TOK_DEV, axis=0)
    jitter = jax.random.uniform(jax.random.fold_in(base_level, 3), (SEQUENCE_TOKENS, head_group), jnp.float32, 0.3, 1.7)
    forget_decrements = rate[None, :] * factor * jitter
    spike_locations = jax.random.randint(jax.random.fold_in(base_level, 4), (3, head_group), 0, SEQUENCE_TOKENS)
    spike_magnitudes = jax.random.uniform(jax.random.fold_in(base_level, 5), (3, head_group), jnp.float32, 0.22, 0.69)
    token_positions = jnp.arange(SEQUENCE_TOKENS)
    match_events = jnp.where(token_positions[:, None, None] == spike_locations[None, :, :], spike_magnitudes[None, :, :], 0.0)
    spike_events = jnp.sum(match_events, axis=1) * jnp.where(rapid_decay, 0.0, 1.0)[None, :]
    return jnp.cumsum(-(forget_decrements + spike_events), axis=0)


def draw_query_small(key, part):
    return plant_pair(key, HS, DS, 11)[0].astype(jnp.bfloat16)


def draw_key_small(key, part):
    return plant_pair(key, HS, DS, 11)[1].astype(jnp.bfloat16)


def draw_query_large(key, part):
    return plant_pair(key, HL, DL, 23)[0].astype(jnp.bfloat16)


def draw_key_large(key, part):
    return plant_pair(key, HL, DL, 23)[1].astype(jnp.bfloat16)


def draw_gates_small(key, part):
    return gate_totals(key, HS, 37)


def draw_gates_large(key, part):
    return gate_totals(key, HL, 41)


def shard_levels(own_key, extent, pieces, low, largest):
    factor_of = 1.0
    for position, shards_of in pieces:
        heights = jax.random.uniform(jax.random.fold_in(jax.random.fold_in(own_key, 6), position), (shards_of,), jnp.float32, low / len(pieces), largest / len(pieces))
        factor_of = factor_of * jnp.repeat(jnp.exp(heights), extent[position] // shards_of).reshape((-1,) + (1,) * (len(extent) - 1 - position))
    return factor_of


def gaussian(stream_key, extent, scale, reach, split=(), kind=jnp.bfloat16):
    array = scale * jax.random.normal(stream_key, extent, jnp.float32)
    if split:
        array = array * shard_levels(stream_key, extent, split, -0.22, 0.18)
    return jnp.clip(array, -reach, reach).astype(kind)


def setup_inputs(seed: int = 0) -> dict:
    key_list = jax.random.split(jax.random.key(seed), 19)
    return {
        "query_small": draw_query_small(jax.random.fold_in(key_list[18], 71), 0),
        "key_small": draw_key_small(jax.random.fold_in(key_list[18], 71), 0),
        "value_small": gaussian(key_list[2], (SEQUENCE_TOKENS, HS * DS), 1.0, 6.0, ((0, 8), (1, 4))),
        "gates_small": draw_gates_small(jax.random.fold_in(key_list[18], 71), 0),
        "query_large": draw_query_large(jax.random.fold_in(key_list[18], 71), 0),
        "key_large": draw_key_large(jax.random.fold_in(key_list[18], 71), 0),
        "value_large": gaussian(key_list[6], (SEQUENCE_TOKENS, HL * DL), 1.0, 6.0, ((0, 8), (1, 4))),
        "gates_large": draw_gates_large(jax.random.fold_in(key_list[18], 71), 0),
        "residual": gaussian(key_list[8], (SEQUENCE_TOKENS, D), 1.0, 6.0, ((0, 32),)),
        "mixer_small": gaussian(key_list[9], (HS * DS, D), ((HS * DS + HL * DL) // 64) ** -0.5, 1.0, ((0, 4),)),
        "mixer_large": gaussian(key_list[10], (HL * DL, D), ((HS * DS + HL * DL) // 64) ** -0.5, 1.0, ((0, 4),)),
        "mix_gain": jnp.clip(1.0 + 0.18 * jax.random.normal(key_list[11], (D,), jnp.float32), 0.1, 1.9),
        "value_weight": gaussian(key_list[12], (D, FF), D ** -0.5, 0.125, ((0, 8), (1, 4))),
        "gate_weight": gaussian(key_list[13], (D, FF), D ** -0.5, 0.125, ((0, 8), (1, 4))),
        "value_taps": gaussian(key_list[14], (3, FF), 0.577, 3.0, ((1, 4),), jnp.float32),
        "gate_taps": gaussian(key_list[15], (3, FF), 0.577, 3.0, ((1, 4),), jnp.float32),
        "down_weight": gaussian(key_list[16], (FF, D), FF ** -0.5, 0.078125, ((0, 4), (1, 8))),
        "final_gain": jnp.clip(1.0 + 0.18 * jax.random.normal(key_list[17], (D,), jnp.float32), 0.1, 1.9),
    }


residual_scale = 2.0 ** 0.5
epsilon = 1e-05

def norm_rows(values, gain):
    center = lax.optimization_barrier(jnp.mean(values, axis=-1, keepdims=True))
    spread = lax.optimization_barrier(jnp.mean(jnp.square(values - center), axis=-1, keepdims=True))
    return (values - center) * lax.rsqrt(spread + epsilon) * gain.astype(jnp.float32)

def attend(queries, key_rows, value_rows, gates, head_dim):
    total_rows = queries.shape[0]
    heads_here = gates.shape[1]
    block_rows = math.gcd(total_rows, 256)
    block_count = total_rows // block_rows
    key_heads = key_rows.astype(jnp.float32).reshape(total_rows, heads_here, head_dim)
    value_heads = value_rows.astype(jnp.float32).reshape(total_rows, heads_here, head_dim)
    query_blocks = queries.reshape(block_count, block_rows, heads_here, head_dim)
    gate_blocks = gates.reshape(block_count, block_rows, heads_here)
    key_positions = jnp.arange(total_rows)

    def one_block(inputs):
        query_part, gate_part, first_row = inputs
        scores = jnp.einsum('qhd,khd->hqk', query_part.astype(jnp.float32), key_heads) * head_dim ** (-0.5)
        scores = scores + gate_part.T[:, :, None] - gates.T[:, None, :]
        token_positions = first_row + jnp.arange(block_rows)
        allowed = token_positions[:, None] >= key_positions[None, :]
        scores = jnp.where(allowed[None], scores, -jnp.inf)
        highest = lax.optimization_barrier(jnp.max(scores, axis=-1, keepdims=True))
        weights = jnp.exp(scores - highest)
        weight_sum = lax.optimization_barrier(jnp.sum(weights, axis=-1))
        rounded = lax.optimization_barrier(weights.astype(jnp.bfloat16)).astype(jnp.float32)
        output = jnp.einsum('hqk,khd->qhd', rounded, value_heads) / weight_sum.T[:, :, None]
        return output.astype(jnp.bfloat16)
    firsts = jnp.arange(block_count) * block_rows
    output = lax.map(one_block, (query_blocks, gate_blocks, firsts))
    return output.reshape(total_rows, heads_here * head_dim)

def causal_filter(rows_in, taps):
    values = rows_in.astype(jnp.float32)
    padded = jnp.concatenate([jnp.zeros((2, values.shape[1]), jnp.float32), values], axis=0)
    return taps[0] * padded[:-2] + taps[1] * padded[1:-1] + taps[2] * padded[2:]

def reference(query_small, key_small, value_small, gates_small, query_large, key_large, value_large, gates_large, residual, mixer_small, mixer_large, mix_gain, value_weight, gate_weight, value_taps, gate_taps, down_weight, final_gain):
    small_out = attend(query_small, key_small, value_small, gates_small, DS)
    large_out = attend(query_large, key_large, value_large, gates_large, DL)
    mix = jnp.dot(small_out, mixer_small, preferred_element_type=jnp.float32) + jnp.dot(large_out, mixer_large, preferred_element_type=jnp.float32)
    mixed = norm_rows(residual_scale * residual.astype(jnp.float32) + mix, mix_gain).astype(jnp.bfloat16)
    up_value = jnp.dot(mixed, value_weight, preferred_element_type=jnp.float32).astype(jnp.bfloat16)
    up_gate = jnp.dot(mixed, gate_weight, preferred_element_type=jnp.float32).astype(jnp.bfloat16)
    filt_value = causal_filter(up_value, value_taps)
    filt_gate = causal_filter(up_gate, gate_taps)
    hidden = (jax.nn.silu(filt_gate) * filt_value).astype(jnp.bfloat16)
    ffn = jnp.dot(hidden, down_weight, preferred_element_type=jnp.float32)
    return norm_rows(residual_scale * mixed.astype(jnp.float32) + ffn, final_gain).astype(jnp.bfloat16)
```

```python
import jax
import jax.numpy as jnp
from jax import lax
from jax.experimental import pallas as pl
from jax.experimental.pallas import tpu as pltpu
from jax.sharding import PartitionSpec as P


DS = 64
DL = 128


residual_scale = 2.0**0.5
epsilon = 1e-05


def passed_along(value, axis, steps):
    count = lax.axis_size(axis)
    first, last = (max(0, -steps), min(count, count - steps))
    return lax.ppermute(value, axis, [(source, source + steps) for source in range(first, last)])


def rotated(value, axis, steps):
    count = lax.axis_size(axis)
    return lax.ppermute(value, axis, [(s, (s + steps) % count) for s in range(count)])


def swapped(value, axis):
    return lax.ppermute(value, axis, [(s, s ^ 1) for s in range(lax.axis_size(axis))])


def norm_rows(values, gain):
    center = jnp.mean(values, axis=-1, keepdims=True)
    spread = jnp.mean(jnp.square(values - center), axis=-1, keepdims=True)
    return (values - center) * lax.rsqrt(spread + epsilon) * gain


def attend_body(small_count, diagonal, *refs):
    if diagonal:
        q_ref, k_ref, v_ref, gk_ref, gq_ref, peak_out, sum_out, acc_out = refs
    else:
        valid_ref, q_ref, k_ref, v_ref, gk_ref, gq_ref = refs[:6]
        peak_in, sum_in, acc_in, peak_out, sum_out, acc_out = refs[6:]
    head = pl.program_id(0)
    scale = jnp.where(head < small_count, DS ** (-0.5), DL ** (-0.5)).astype(jnp.float32)

    def logits():
        scores = lax.dot_general(
            q_ref[0], k_ref[...], (((1,), (1,)), ((), ())), preferred_element_type=jnp.float32
        )
        return scores * scale + (gq_ref[0] - gk_ref[0])

    if diagonal:
        scores = logits()
        query_rows = pl.program_id(1) * scores.shape[0]
        allowed = query_rows + lax.broadcasted_iota(
            jnp.int32, scores.shape, 0
        ) >= lax.broadcasted_iota(jnp.int32, scores.shape, 1)
        scores = jnp.where(allowed, scores, -jnp.inf)
        peak = jnp.max(scores, axis=-1, keepdims=True)
        weights = jnp.exp(scores - peak)
        peak_out[0] = peak
        sum_out[0] = jnp.sum(weights, axis=-1, keepdims=True)
        acc_out[0] = jnp.dot(
            weights.astype(jnp.bfloat16), v_ref[...], preferred_element_type=jnp.float32
        )
        return

    @pl.when(valid_ref[0] > 0)
    def _():
        scores = logits()
        peak = jnp.maximum(peak_in[0], jnp.max(scores, axis=-1, keepdims=True))
        factor = jnp.exp(peak_in[0] - peak)
        weights = jnp.exp(scores - peak)
        peak_out[0] = peak
        sum_out[0] = sum_in[0] * factor + jnp.sum(weights, axis=-1, keepdims=True)
        acc_out[0] = acc_in[0] * factor + jnp.dot(
            weights.astype(jnp.bfloat16), v_ref[...], preferred_element_type=jnp.float32
        )

    @pl.when(valid_ref[0] <= 0)
    def _():
        peak_out[0] = peak_in[0]
        sum_out[0] = sum_in[0]
        acc_out[0] = acc_in[0]


def attend(q_heads, key_value, key_gates, query_gates, small_count, state, valid):
    heads, rows, width = q_heads.shape
    per_small = width // DS
    groups = key_value.shape[1] // (2 * width)
    block = rows // 3 if rows % 3 == 0 and (rows // 3) % 128 == 0 else rows
    diagonal = state is None
    small_groups = small_count // per_small

    def group(h):
        return jnp.where(h < small_count, h // per_small, h - small_count + small_groups)

    per_query = pl.BlockSpec((1, block, 1), lambda h, i: (h, i, 0))
    wide = pl.BlockSpec((1, block, width), lambda h, i: (h, i, 0))
    in_specs = [
        wide,
        pl.BlockSpec((rows, width), lambda h, i: (0, group(h))),
        pl.BlockSpec((rows, width), lambda h, i: (0, groups + group(h))),
        pl.BlockSpec((1, 1, rows), lambda h, i: (h, 0, 0)),
        per_query,
    ]
    operands = [q_heads, key_value, key_value, key_gates[:, None, :], query_gates[:, :, None]]
    aliases = {}
    if not diagonal:
        in_specs = [pl.BlockSpec(memory_space=pltpu.SMEM)] + in_specs + [per_query, per_query, wide]
        operands = [valid] + operands + list(state)
        aliases = {6: 0, 7: 1, 8: 2}
    column = jax.ShapeDtypeStruct((heads, rows, 1), jnp.float32)

    def kernel(*refs):
        attend_body(small_count, diagonal, *refs)

    return pl.pallas_call(
        kernel,
        grid=(heads, rows // block),
        in_specs=in_specs,
        out_specs=[per_query, per_query, wide],
        out_shape=[column, column, jax.ShapeDtypeStruct((heads, rows, width), jnp.float32)],
        input_output_aliases=aliases,
        cost_estimate=pl.CostEstimate(
            flops=heads * rows * rows * width * 4,
            bytes_accessed=heads * rows * width * 12,
            transcendentals=heads * rows * rows,
        ),
        compiler_params=pltpu.CompilerParams(
            dimension_semantics=("arbitrary", "arbitrary"), vmem_limit_bytes=56 * 1024 * 1024
        ),
    )(*operands)


def per_device(
    query_small,
    key_small,
    value_small,
    gates_small,
    query_large,
    key_large,
    value_large,
    gates_large,
    residual,
    mixer_small,
    mixer_large,
    mix_gain,
    value_weight,
    gate_weight,
    value_taps,
    gate_taps,
    down_weight,
    final_gain,
):
    shard_rows = query_small.shape[0]
    sp_index = lax.axis_index("sp")
    tp_index = lax.axis_index("tp")
    tensor_parts = lax.axis_size("tp")
    sp_count = lax.axis_size("sp")
    splits = all(
        count % 2 == 0 and count * size % (2 * DL) == 0
        for count, size in ((gates_small.shape[1], DS), (gates_large.shape[1], DL))
    )
    team = 2 if splits and sp_count % 2 == 0 else 1
    pair_count = sp_count // team
    pair, side = sp_index // team, sp_index % team
    half_small = query_small.shape[1] // team
    small_count = gates_small.shape[1] // team
    large_count = gates_large.shape[1] // team

    def half(array, which):
        width = array.shape[1] // team
        return lax.dynamic_slice_in_dim(array, which * width, width, 1)

    def halves(parts, which):
        return jnp.concatenate([half(a, which) for a in parts], axis=1)

    def exchanged(parts):
        if team == 1:
            return jnp.concatenate(parts, axis=1)
        return in_order(halves(parts, side), swapped(halves(parts, 1 - side), "sp"), 0)

    def in_order(own, other, axis):
        return jnp.where(
            side == 0,
            jnp.concatenate([own, other], axis=axis),
            jnp.concatenate([other, own], axis=axis),
        )

    gate_parts = (gates_small, gates_large)
    key_value = exchanged((key_small, key_large, value_small, value_large))
    if team == 1:
        own_gates = jnp.concatenate(gate_parts, axis=1).T
    else:
        own_gates = in_order(
            halves(gate_parts, side).T, swapped(halves(gate_parts, 1 - side).T, "sp"), 1
        )
    queries = exchanged((query_small, query_large))

    width = DL
    per_small = width // DS
    lane_head = jnp.arange(width) // DS
    q_heads = []
    for h in range(small_count):
        columns = queries[:, (h // per_small) * width : (h // per_small + 1) * width]
        q_heads.append(jnp.where(lane_head == h % per_small, columns, 0).astype(jnp.bfloat16))
    for h in range(large_count):
        q_heads.append(queries[:, half_small + h * width : half_small + (h + 1) * width])
    q_heads = jnp.stack(q_heads)

    mixers = jnp.concatenate([mixer_small, mixer_large], axis=0)
    mixer_of = [mixers]
    for s in range(1, tensor_parts):
        mixer_of.append(rotated(mixers, "tp", -s))
    full_value = lax.all_gather(value_weight, "sp", axis=0, tiled=True)
    full_gate = lax.all_gather(gate_weight, "sp", axis=0, tiled=True)
    down_pieces = down_parts(down_weight)

    arriving, gates_arriving = [key_value], [own_gates]
    for step in range(1, pair_count):
        gates_arriving.append(passed_along(own_gates, "sp", step * team))
        arriving.append(passed_along(arriving[-1], "sp", team))
    state = attend(q_heads, key_value, own_gates, own_gates, small_count, None, None)
    for step in range(1, pair_count):
        valid = (pair >= step).astype(jnp.int32).reshape(1)
        state = attend(
            q_heads, arriving[step], gates_arriving[step], own_gates, small_count, state, valid
        )
    head_out = (state[2] / state[1]).astype(jnp.bfloat16)
    columns = []
    for g in range(small_count // per_small):
        merged = head_out[g * per_small]
        for h in range(1, per_small):
            merged = jnp.where(lane_head == h, head_out[g * per_small + h], merged)
        columns.append(merged)
    for h in range(large_count):
        columns.append(head_out[small_count + h])
    attended = jnp.concatenate(columns, axis=1)
    joined = attended
    if team == 2:
        own = lax.dynamic_slice_in_dim(attended, side * shard_rows, shard_rows, 0)
        other = swapped(
            lax.dynamic_slice_in_dim(attended, (1 - side) * shard_rows, shard_rows, 0), "sp"
        )
        joined = jnp.concatenate(
            [
                in_order(own[:, :half_small], other[:, :half_small], 1),
                in_order(own[:, half_small:], other[:, half_small:], 1),
            ],
            axis=1,
        )
    own_rows = shard_rows // tensor_parts
    arrived = lax.all_to_all(joined, "tp", split_axis=0, concat_axis=1, tiled=True)
    mix = jnp.zeros((own_rows, mixers.shape[1]), jnp.float32)
    for s in range(tensor_parts):
        source = (tp_index + s) % tensor_parts
        mix = mix + jnp.dot(
            lax.dynamic_slice_in_dim(arrived, source * joined.shape[1], joined.shape[1], 1),
            mixer_of[s],
            preferred_element_type=jnp.float32,
        )
    mixed = norm_rows(residual_scale * residual.astype(jnp.float32) + mix, mix_gain).astype(
        jnp.bfloat16
    )
    block_input = jnp.zeros((shard_rows, mixed.shape[1]), jnp.bfloat16)
    for s in range(tensor_parts):
        piece = mixed if s == 0 else rotated(mixed, "tp", -s)
        source = (tp_index + s) % tensor_parts
        block_input = lax.dynamic_update_slice_in_dim(block_input, piece, source * own_rows, 0)

    up_value = jnp.dot(block_input, full_value, preferred_element_type=jnp.float32).astype(
        jnp.bfloat16
    )
    up_gate = jnp.dot(block_input, full_gate, preferred_element_type=jnp.float32).astype(
        jnp.bfloat16
    )
    down_base, up_value = lax.optimization_barrier((down_weight, up_value))
    full_down = assembled(down_base, down_pieces)
    hidden_width = up_value.shape[1]
    trailing = jnp.concatenate([up_value[-2:], up_gate[-2:]], axis=1)
    earlier = passed_along(trailing, "sp", 1)
    padded_value = jnp.concatenate([earlier[:, :hidden_width], up_value], axis=0).astype(
        jnp.float32
    )
    padded_gate = jnp.concatenate([earlier[:, hidden_width:], up_gate], axis=0).astype(jnp.float32)
    filt_value = (
        value_taps[0] * padded_value[:-2]
        + value_taps[1] * padded_value[1:-1]
        + value_taps[2] * padded_value[2:]
    )
    filt_gate = (
        gate_taps[0] * padded_gate[:-2]
        + gate_taps[1] * padded_gate[1:-1]
        + gate_taps[2] * padded_gate[2:]
    )
    hidden = (jax.nn.silu(filt_gate) * filt_value).astype(jnp.bfloat16)

    def ffn_rows(s):
        target = (tp_index + s) % tensor_parts
        part = lax.dynamic_slice_in_dim(hidden, target * own_rows, own_rows, 0)
        return jnp.dot(part, full_down, preferred_element_type=jnp.float32)

    order = [tensor_parts // 2] + [s for s in range(1, tensor_parts) if s != tensor_parts // 2]
    received = [rotated(ffn_rows(s).astype(jnp.bfloat16), "tp", s) for s in order]
    ffn = ffn_rows(0)
    for part in received:
        ffn = ffn + part.astype(jnp.float32)
    return norm_rows(residual_scale * mixed.astype(jnp.float32) + ffn, final_gain).astype(
        jnp.bfloat16
    )


def down_parts(down_weight):
    pieces = []
    for s in range(1, lax.axis_size("sp")):
        pieces.append(rotated(down_weight, "sp", -s))
    return pieces


def assembled(own, pieces):
    count = lax.axis_size("sp")
    width = own.shape[1]
    index = lax.axis_index("sp")
    full = jnp.zeros((own.shape[0], count * width), own.dtype)
    for s, piece in enumerate([own] + pieces):
        full = lax.dynamic_update_slice_in_dim(full, piece, ((index + s) % count) * width, 1)
    return full


MESH = pl.DeviceIdType.MESH
LANES = 128
HALO = 16


def fits(sp_count, tp_count, arrays):
    query, gates_small, gates_large = arrays[0], arrays[3], arrays[7]
    query_large, value_weight = arrays[4], arrays[12]
    rows = query.shape[0]
    own = rows // tp_count
    return (
        tp_count == 4
        and sp_count % 4 == 0
        and query.shape[1] == 2 * LANES
        and query_large.shape[1] == 2 * LANES
        and gates_small.shape[1] == 2 * LANES // DS
        and gates_large.shape[1] == 2
        and rows % (3 * LANES) == 0
        and own % (2 * HALO) == 0
        and value_weight.shape[1] % LANES == 0
        and value_weight.shape[0] % HALO == 0
    )


def half_width(columns):
    return -(-columns // (2 * LANES)) * LANES


class Place:
    def __init__(self):
        self.count = lax.axis_size("sp")
        self.nz = self.count // 2
        self.sp = lax.axis_index("sp")
        self.tp = lax.axis_index("tp")
        self.z, self.x = self.sp // 2, self.sp % 2
        self.y, self.c = self.tp // 2, self.tp % 2
        self.parity = self.z % 2
        self.mate = self.z + 1 - 2 * self.parity

    def at(self, z=None, x=None, y=None, c=None):
        z = self.z if z is None else z
        x = self.x if x is None else x
        y = self.y if y is None else y
        c = self.c if c is None else c
        return (z * 2 + x, y * 2 + c)


class Traffic:
    def __init__(self):
        self.sent = []

    def start(self, copy, when=None):
        guarded(when, copy.start)
        self.sent.append((copy, when))

    def drain(self):
        for copy, when in self.sent:
            guarded(when, copy.wait_send)


def guarded(when, action):
    if when is None:
        action()
    else:

        @pl.when(when)
        def _():
            action()


def remote(source, target, send, receive, device):
    return pltpu.make_async_remote_copy(
        src_ref=source,
        dst_ref=target,
        send_sem=send,
        recv_sem=receive,
        device_id=device,
        device_id_type=MESH,
    )


def front_kernel(
    qs, ql, ks, kl, vs, vl, gt, ms, ml, wv, wg, wd, res, gain,
    o_wv, o_wg, o_wd, o_rows, o_mixed,
    q_buf, kv, gk, gq, peak, total, acc, o_buf, arrived, mixers, y_buf, zero, bounce_a, bounce_b,
    local_sem, x_send, x_recv, kv_send, kv_recv, g_send, g_recv,
    w_up, w_dn, w_zr, w_xs, w_xr, b_sem, m_local, m_send, m_recv,
    o_send, o_recv, a_send, a_recv, h_send, h_recv, a_local,
):
    me = Place()
    net = Traffic()
    nz, z, x, sp, tp = me.nz, me.z, me.x, me.sp, me.tp
    rows = qs.shape[0]
    own_rows = rows // 4
    other = 1 - x
    mine = pl.ds(pl.multiple_of(x * rows, LANES), rows)
    theirs = pl.ds(pl.multiple_of(other * rows, LANES), rows)
    own_lanes = pl.ds(pl.multiple_of(x * LANES, LANES), LANES)
    other_lanes = pl.ds(pl.multiple_of(other * LANES, LANES), LANES)
    weights = ((wv, o_wv), (wg, o_wg), (wd, o_wd))
    depth = wv.shape[0]
    full_width = wv.shape[1]
    width = half_width(full_width)

    def parts(which):
        return (
            (qs, q_buf.at[which, 0:LANES]),
            (ql, q_buf.at[which, LANES : 2 * LANES]),
            (ks, kv.at[z, which, 0:LANES]),
            (kl, kv.at[z, which, LANES : 2 * LANES]),
            (vs, kv.at[z, which, 2 * LANES : 3 * LANES]),
            (vl, kv.at[z, which, 3 * LANES : 4 * LANES]),
        )

    locals_ = []
    for i, (source, target) in enumerate(parts(mine)):
        net.start(
            remote(source.at[:, other_lanes], target, x_send.at[i], x_recv.at[i], me.at(x=other))
        )
        locals_.append(pltpu.make_async_copy(source.at[:, own_lanes], target, local_sem.at[i]))
    net.start(
        remote(gt.at[other], gk.at[z, :, mine], x_send.at[6], x_recv.at[6], me.at(x=other))
    )
    locals_.append(pltpu.make_async_copy(gt.at[x], gk.at[z, :, mine], local_sem.at[6]))
    for copy in locals_:
        copy.start()

    mixer_rows = 4 * LANES
    mixer_locals = []
    for h in range(2):
        for k, source in enumerate((ms, ml)):
            row = tp * mixer_rows + (2 * h + k) * LANES
            mixer_locals.append(
                pltpu.make_async_copy(
                    source.at[h * LANES : (h + 1) * LANES],
                    mixers.at[pl.ds(row, LANES)],
                    m_local.at[2 * h + k],
                )
            )
    for copy in mixer_locals:
        copy.start()

    def mixer_slot(t):
        return mixers.at[pl.ds(t * mixer_rows, mixer_rows)]

    def half_of(w, half):
        offset = pl.multiple_of(half * (full_width - width), LANES)
        source = weights[w][0]
        if w == 2:
            return source.at[pl.ds(offset, width), :]
        return source.at[:, pl.ds(offset, width)]

    def slot(w, which, zs, xs):
        shard = zs * 2 + xs
        if w == 2:
            return weights[w][1].at[which, shard]
        return weights[w][1].at[which, pl.ds(shard * depth, depth), :]

    def origin(w, which, zs, own):
        if not own:
            return slot(w, which, zs, x)
        return half_of(w, me.parity if which == 0 else 1 - me.parity)

    def both(a, b):
        return b if a is None else jnp.logical_and(a, b)

    def send_up(w, zs, own, when=None):
        for e in range(2):
            net.start(
                remote(
                    origin(w, 1 - e, zs, own), slot(w, e, zs, x),
                    w_up.at[w, e, zs], w_zr.at[w, e, zs], me.at(z=jnp.minimum(z + 1, nz - 1)),
                ),
                both(when, z + 1 + e < nz),
            )

    def send_down(w, zs, own, when=None):
        for e in range(2):
            net.start(
                remote(
                    origin(w, 1 - e, zs, own), slot(w, e, zs, x),
                    w_dn.at[w, e, zs], w_zr.at[w, e, zs], me.at(z=jnp.maximum(z - 1, 0)),
                ),
                both(when, z - 1 - e >= 0),
            )

    def send_across(w, zs, own, when=None):
        net.start(
            remote(
                origin(w, 0, zs, own), slot(w, 0, zs, x),
                w_xs.at[w, zs], w_xr.at[w, zs], me.at(x=other),
            ),
            when,
        )

    def landed(w, which, zs, when):
        copy = remote(
            slot(w, which, zs, x), slot(w, which, zs, x),
            w_up.at[w, which, zs], w_zr.at[w, which, zs], me.at(x=other),
        )
        guarded(when, copy.wait_recv)

    def pump(w, r):
        below, above = jnp.maximum(z - r, 0), jnp.minimum(z + r, nz - 1)
        has_below, has_above = z - r >= 0, z + r < nz
        landed(w, 0, below, has_below)
        landed(w, 1, below, both(has_below, z + 1 < nz))
        send_up(w, below, False, has_below)
        send_across(w, below, False, has_below)
        landed(w, 0, above, has_above)
        landed(w, 1, above, both(has_above, z - 1 >= 0))
        send_down(w, above, False, has_above)
        send_across(w, above, False, has_above)

    def piece(j, p):
        span = mine if p == 0 else theirs
        return kv.at[j, span, :], gk.at[j, :, span]

    def pass_on(j, p, when):
        data, gate = piece(j, p)
        above = me.at(z=jnp.minimum(z + 1, nz - 1))
        net.start(remote(data, data, kv_send.at[j, p], kv_recv.at[j, p], above), when)
        net.start(remote(gate, gate, g_send.at[j, p], g_recv.at[j, p], above), when)

    def take(j, p, when):
        data, gate = piece(j, p)
        above = me.at(z=jnp.minimum(z + 1, nz - 1))
        guarded(when, remote(data, data, kv_send.at[j, p], kv_recv.at[j, p], above).wait_recv)
        guarded(when, remote(gate, gate, g_send.at[j, p], g_recv.at[j, p], above).wait_recv)

    def forward_block(r):
        j = jnp.maximum(z - r, 0)
        for p in range(2):
            take(j, p, z - r >= 0)
            pass_on(j, p, jnp.logical_and(z - r >= 0, z + 1 < nz))

    block = 2 * rows // 3
    count = 3

    def head_facts(h):
        lanes = lax.broadcasted_iota(jnp.int32, (1, LANES), 1)
        low = jnp.where(h == 1, DS, 0)
        high = jnp.where(h == 0, DS, LANES)
        keep = jnp.logical_and(lanes >= low, lanes < high)
        column = pl.multiple_of(jnp.where(h == 2, LANES, 0), LANES)
        scale = jnp.where(h == 2, DL ** (-0.5), DS ** (-0.5)).astype(jnp.float32)
        return keep, column, scale

    def query_part(h, span):
        keep, column, scale = head_facts(h)
        q = q_buf[span, pl.ds(column, LANES)]
        return jnp.where(keep, q, jnp.zeros_like(q)), column, scale

    def shifted_scores(q, j, h, column, scale, keys):
        k = kv[j, keys, pl.ds(column, LANES)]
        scores = lax.dot_general(
            q, k, (((1,), (1,)), ((), ())), preferred_element_type=jnp.float32
        )
        return scores * scale - gk[j, pl.ds(h, 1), keys]

    def weighted(weights_, j, column, keys):
        v = kv[j, keys, pl.ds(column + 2 * LANES, LANES)]
        return jnp.dot(weights_.astype(jnp.bfloat16), v, preferred_element_type=jnp.float32)

    def attend_own():
        def head(h, carry):
            for i in range(count):
                span = pl.ds(i * block, block)
                keys = pl.ds(0, (i + 1) * block)
                q, column, scale = query_part(h, span)
                scores = shifted_scores(q, z, h, column, scale, keys)
                allowed = i * block + lax.broadcasted_iota(
                    jnp.int32, scores.shape, 0
                ) >= lax.broadcasted_iota(jnp.int32, scores.shape, 1)
                scores = jnp.where(allowed, scores, -jnp.inf)
                gate = gq[h, span, :]
                top = jnp.max(scores, axis=-1, keepdims=True) + gate
                weights_ = jnp.exp(scores + (gate - top))
                peak[h, span, :] = top
                total[h, span, :] = jnp.sum(weights_, axis=-1, keepdims=True)
                acc[h, span, :] = weighted(weights_, z, column, keys)
            return carry

        lax.fori_loop(0, 3, head, 0)

    def attend_earlier(j):
        def part(i, carry):
            h, b = i // count, i % count
            span = pl.ds(pl.multiple_of(b * block, LANES), block)
            keys = pl.ds(0, 2 * rows)
            q, column, scale = query_part(h, span)
            scores = shifted_scores(q, j, h, column, scale, keys)
            gate = gq[h, span, :]
            before = peak[h, span, :]
            top = jnp.maximum(before, jnp.max(scores, axis=-1, keepdims=True) + gate)
            factor = jnp.exp(before - top)
            weights_ = jnp.exp(scores + (gate - top))
            peak[h, span, :] = top
            total[h, span, :] = total[h, span, :] * factor + jnp.sum(
                weights_, axis=-1, keepdims=True
            )
            acc[h, span, :] = acc[h, span, :] * factor + weighted(weights_, j, column, keys)
            return carry

        lax.fori_loop(0, 3 * count, part, 0)

    for w in range(2):
        send_down(w, z, True)
    for copy in locals_:
        copy.wait()
    pass_on(z, 0, z + 1 < nz)
    send_up(0, z, True)
    for copy in mixer_locals:
        copy.wait()
    net.start(
        remote(mixer_slot(tp), mixer_slot(tp), m_send.at[0], m_recv.at[0], me.at(y=1 - me.y))
    )
    net.start(
        remote(mixer_slot(tp), mixer_slot(tp), m_send.at[1], m_recv.at[1], me.at(c=1 - me.c))
    )
    own_copies = []
    for w in range(3):
        target = bounce_b if w == 2 else bounce_a.at[w]
        own_copies.append(
            (
                pltpu.make_async_copy(half_of(w, me.parity), target, b_sem.at[w, 0]),
                pltpu.make_async_copy(target, slot(w, 0, z, x), b_sem.at[w, 1]),
            )
        )
    for first, _ in own_copies:
        first.start()
    for i, (source, target) in enumerate(parts(theirs)):
        remote(source.at[:, other_lanes], target, x_send.at[i], x_recv.at[i], me.at(x=other)).wait_recv()
    remote(gt.at[other], gk.at[z, :, theirs], x_send.at[6], x_recv.at[6], me.at(x=other)).wait_recv()
    pass_on(z, 1, z + 1 < nz)
    for w in range(2):
        send_across(w, z, True)
    send_up(1, z, True)
    for first, second in own_copies:
        first.wait()
        second.start()
    columns = jnp.transpose(gk[z])
    for h in range(3):
        gq[h] = columns[:, h : h + 1]
    attend_own()

    pumps = [[(0, 1)], [(1, 1), (0, 2)], [(1, 2), (0, 3)]]
    for r in range(1, nz):
        forward_block(r)
        for w, k in pumps[r - 1] if r - 1 < len(pumps) else []:
            if k < nz:
                pump(w, k)
        if r == 2:
            send_down(2, z, True)
            send_up(2, z, True)
            send_across(2, z, True)

        @pl.when(z - r >= 0)
        def _(r=r):
            attend_earlier(jnp.maximum(z - r, 0))

    for h in range(3):
        done = acc[h] / total[h]
        if h == 0:
            first_head = done
        elif h == 1:
            keep, _, _ = head_facts(1)
            o_buf[:, 0:LANES] = jnp.where(keep, done, first_head).astype(jnp.bfloat16)
        else:
            o_buf[:, LANES : 2 * LANES] = done.astype(jnp.bfloat16)

    ty = (1 - me.y) * 2 + me.c
    from_y = remote(mixer_slot(ty), mixer_slot(ty), m_send.at[2], m_recv.at[0], me.at(c=1 - me.c))
    from_y.wait_recv()
    net.start(
        remote(mixer_slot(ty), mixer_slot(ty), m_send.at[2], m_recv.at[2], me.at(c=1 - me.c))
    )

    def arrival(t, xs):
        return arrived.at[:, pl.ds(pl.multiple_of((t * 2 + xs) * 2 * LANES, 2 * LANES), 2 * LANES)]

    takes = []
    for k in range(1, 8):
        dx, dy, dc = k // 4, (k // 2) % 2, k % 2
        x2 = x + dx * (1 - 2 * x)
        y2 = me.y + dy * (1 - 2 * me.y)
        c2 = me.c + dc * (1 - 2 * me.c)
        t2 = y2 * 2 + c2
        net.start(
            remote(
                o_buf.at[pl.ds(x2 * rows + t2 * own_rows, own_rows), :], arrival(tp, x),
                o_send.at[k], o_recv.at[k], me.at(x=x2, y=y2, c=c2),
            )
        )
        takes.append(
            remote(
                o_buf.at[pl.ds(0, own_rows), :], arrival(t2, x2),
                o_send.at[k], o_recv.at[k], me.at(x=x2, y=y2, c=c2),
            )
        )
    own_span = pl.ds(pl.multiple_of((tp * 2 + x) * 2 * LANES, 2 * LANES), 2 * LANES)
    arrived[:, own_span] = o_buf[pl.ds(pl.multiple_of(x * rows + tp * own_rows, HALO), own_rows), :]
    pump(1, 3)
    pump(2, 1)
    remote(mixer_slot(0), mixer_slot(tp + 1 - 2 * me.c), m_send.at[1], m_recv.at[1], me.at(c=1 - me.c)).wait_recv()
    remote(mixer_slot(0), mixer_slot(ty + 1 - 2 * me.c), m_send.at[2], m_recv.at[2], me.at(c=1 - me.c)).wait_recv()
    for copy in takes:
        copy.wait_recv()

    features = gain.shape[1]
    step = 4 * LANES

    def mix_tile(n, carry):
        span = pl.ds(pl.multiple_of(n * step, step), step)
        y_buf[:, span] = residual_scale * res[:, span].astype(jnp.float32) + jnp.dot(
            arrived[...], mixers[:, span], preferred_element_type=jnp.float32
        )
        return carry

    lax.fori_loop(0, features // step, mix_tile, 0)
    o_mixed[...] = norm_rows(y_buf[...], gain[...]).astype(jnp.bfloat16)
    zero[...] = jnp.zeros_like(zero)

    parity, mate = me.parity, me.mate

    def rows_of(zi, t, part=None):
        base = HALO + t * own_rows
        if part is None:
            return o_rows.at[zi, pl.ds(base, own_rows), :]
        return o_rows.at[zi, pl.ds(base + part * (own_rows // 2), own_rows // 2), :]

    here = rows_of(parity, tp)
    up_y, up_z, up_c = me.at(y=1 - me.y), me.at(z=mate), me.at(c=1 - me.c)
    net.start(remote(o_mixed, here, a_send.at[0], a_recv.at[0], up_z))
    net.start(remote(o_mixed, here, a_send.at[1], a_recv.at[1], up_y))
    net.start(remote(o_mixed, here, a_send.at[2], a_recv.at[2], up_c))
    keep_rows = pltpu.make_async_copy(o_mixed, here, a_local.at[0])
    keep_rows.start()
    following = jnp.minimum(sp + 1, me.count - 1)
    fz = following // 2
    sends_halo = jnp.logical_and(sp + 1 < me.count, tp == 3)
    for k in range(8):
        dz, dy, dc = k // 4, (k // 2) % 2, k % 2
        z2 = fz - fz % 2 + dz
        net.start(
            remote(
                o_mixed.at[own_rows - HALO : own_rows, :],
                o_rows.at[fz % 2, 0:HALO, :],
                h_send.at[k], h_recv.at[fz % 2],
                (z2 * 2 + 1 - x, dy * 2 + dc),
            ),
            sends_halo,
        )
    first_rows = jnp.logical_and(z - parity == 0, x == 0)
    blank = pltpu.make_async_copy(zero, o_rows.at[0, 0:HALO, :], a_local.at[1])
    guarded(first_rows, blank.start)

    p_z, p_y = rows_of(1 - parity, tp), rows_of(parity, ty)
    remote(o_mixed, p_y, a_send.at[1], a_recv.at[1], up_y).wait_recv()
    half = rows_of(parity, ty, 0)
    net.start(remote(half, half, a_send.at[3], a_recv.at[3], up_z))
    net.start(remote(p_y, p_y, a_send.at[5], a_recv.at[5], up_c))
    remote(o_mixed, p_z, a_send.at[0], a_recv.at[0], up_z).wait_recv()
    half = rows_of(1 - parity, tp, 1)
    net.start(remote(half, half, a_send.at[4], a_recv.at[4], up_y))
    net.start(remote(p_z, p_z, a_send.at[6], a_recv.at[6], up_c))
    for k in range(2):
        half = rows_of(1 - parity, ty, k)
        remote(half, half, a_send.at[3 + k], a_recv.at[3 + k], up_c).wait_recv()
        net.start(remote(half, half, a_send.at[7 + k], a_recv.at[7 + k], up_c))

    pump(2, 2)
    pump(2, 3)

    tc, tyc = tp + 1 - 2 * me.c, ty + 1 - 2 * me.c
    for k, target in (
        (2, rows_of(parity, tc)),
        (5, rows_of(parity, tyc)),
        (6, rows_of(1 - parity, tc)),
        (7, rows_of(1 - parity, tyc, 0)),
        (8, rows_of(1 - parity, tyc, 1)),
    ):
        remote(target, target, a_send.at[k], a_recv.at[k], up_c).wait_recv()
    for i in range(2):
        halo = o_rows.at[i, 0:HALO, :]
        copy = remote(halo, halo, h_send.at[i], h_recv.at[i], up_c)
        guarded((z - parity + i) * 2 + x - 1 >= 0, copy.wait_recv)
    guarded(first_rows, blank.wait)
    keep_rows.wait()
    for w in range(3):
        for zs in range(nz):
            target = slot(w, 0, zs, other)
            remote(target, target, w_xs.at[w, zs], w_xr.at[w, zs], me.at(x=other)).wait_recv()
    for _, second in own_copies:
        second.wait()
    net.drain()


def front(qs, ql, ks, kl, vs, vl, gt, ms, ml, wv, wg, wd, res, gain):
    count = lax.axis_size("sp")
    nz = count // 2
    rows = qs.shape[0]
    own_rows = rows // 4
    features = gain.shape[1]
    depth, width = wv.shape[0], half_width(wv.shape[1])
    down_columns = wd.shape[1]
    bf16, f32 = jnp.bfloat16, jnp.float32
    dma = pltpu.SemaphoreType.DMA
    anywhere = pl.BlockSpec(memory_space=pl.ANY)
    vmem = pl.BlockSpec(memory_space=pltpu.VMEM)
    return pl.pallas_call(
        front_kernel,
        out_shape=[
            jax.ShapeDtypeStruct((2, count * depth, width), bf16),
            jax.ShapeDtypeStruct((2, count * depth, width), bf16),
            jax.ShapeDtypeStruct((2, count, width, down_columns), bf16),
            jax.ShapeDtypeStruct((2, HALO + rows, features), bf16),
            jax.ShapeDtypeStruct((own_rows, features), bf16),
        ],
        in_specs=[anywhere] * 12 + [vmem] * 2,
        out_specs=[anywhere] * 4 + [vmem],
        scratch_shapes=[
            pltpu.VMEM((2 * rows, 2 * LANES), bf16),
            pltpu.VMEM((nz, 2 * rows, 4 * LANES), bf16),
            pltpu.VMEM((nz, 8, 2 * rows), f32),
            pltpu.VMEM((3, 2 * rows, 1), f32),
            pltpu.VMEM((3, 2 * rows, 1), f32),
            pltpu.VMEM((3, 2 * rows, 1), f32),
            pltpu.VMEM((3, 2 * rows, LANES), f32),
            pltpu.VMEM((2 * rows, 2 * LANES), bf16),
            pltpu.VMEM((own_rows, 16 * LANES), bf16),
            pltpu.VMEM((16 * LANES, features), bf16),
            pltpu.VMEM((own_rows, features), f32),
            pltpu.VMEM((HALO, features), bf16),
            pltpu.VMEM((2, depth, width), bf16),
            pltpu.VMEM((width, down_columns), bf16),
            dma((7,)), dma((7,)), dma((7,)),
            dma((nz, 2)), dma((nz, 2)), dma((nz, 2)), dma((nz, 2)),
            dma((3, 2, nz)), dma((3, 2, nz)), dma((3, 2, nz)),
            dma((3, nz)), dma((3, nz)),
            dma((3, 2)), dma((4,)), dma((3,)), dma((3,)),
            dma((8,)), dma((8,)), dma((9,)), dma((9,)), dma((8,)), dma((2,)), dma((2,)),
        ],
        compiler_params=pltpu.CompilerParams(
            has_side_effects=True, vmem_limit_bytes=62 * 1024 * 1024
        ),
        name="front",
    )(qs, ql, ks, kl, vs, vl, gt, ms, ml, wv, wg, wd, res, gain)


def tail_kernel(
    x_rows, wv, wg, wd, mixed, gain, tv, tg,
    out,
    rows_buf, wv_buf, wg_buf, wd_buf, uv, ug, hidden, own, stage, from_c, send_a, from_a, send_b, from_b,
    load_sem, c_send, c_recv, a_send, a_recv, b_send, b_recv,
):
    me = Place()
    net = Traffic()
    rows = x_rows.shape[1] - HALO
    own_rows = rows // 4
    cut = own_rows // 2
    full_width = tv.shape[1]
    width = wv.shape[2]
    shards, down_columns = wd.shape[1], wd.shape[3]
    parity = me.parity
    tile = 2 * LANES
    loads = [
        pltpu.make_async_copy(x_rows.at[1 - parity], rows_buf.at[0], load_sem.at[0]),
        pltpu.make_async_copy(wv.at[0], wv_buf, load_sem.at[1]),
        pltpu.make_async_copy(wg.at[0], wg_buf, load_sem.at[2]),
        pltpu.make_async_copy(x_rows.at[parity], rows_buf.at[1], load_sem.at[3]),
        pltpu.make_async_copy(wd.at[0], wd_buf, load_sem.at[4]),
    ]
    for copy in loads:
        copy.start()
    offset = parity * (full_width - width)
    repeated = jnp.where(parity == 1, 2 * width - full_width, 0)

    def expand(b):
        def tile_of(n, carry):
            span = pl.ds(pl.multiple_of(n * tile, tile), tile)
            taps = pl.ds(pl.multiple_of(offset + n * tile, LANES), tile)
            filtered = []
            for buf, weight, tap in ((uv, wv_buf, tv), (ug, wg_buf, tg)):
                up = jnp.dot(rows_buf[b], weight[:, span], preferred_element_type=jnp.float32)
                buf[...] = up.astype(jnp.bfloat16).astype(jnp.float32)
                filtered.append(
                    tap[0:1, taps] * buf[HALO - 2 : HALO - 2 + rows, :]
                    + tap[1:2, taps] * buf[HALO - 1 : HALO - 1 + rows, :]
                    + tap[2:3, taps] * buf[HALO : HALO + rows, :]
                )
            value, gate = filtered
            result = value * (gate / (1.0 + jnp.exp(-gate)))
            unit = n * tile + lax.broadcasted_iota(jnp.int32, (1, tile), 1)
            result = jnp.where(unit >= repeated, result, 0.0)
            hidden[:, span] = result.astype(jnp.bfloat16)
            return carry

        lax.fori_loop(0, width // tile, tile_of, 0)

    def contract(t, write):
        part = hidden[pl.ds(pl.multiple_of(t * own_rows, HALO), own_rows), :]

        def columns(n, carry):
            write(
                pl.ds(pl.multiple_of(n * down_columns, LANES), down_columns),
                jnp.dot(part, wd_buf[n], preferred_element_type=jnp.float32),
            )
            return carry

        lax.fori_loop(0, shards, columns, 0)

    partner = me.at(c=1 - me.c)
    for b in range(2):
        if b == 0:
            for copy in loads[:3]:
                copy.wait()
        else:
            loads[3].wait()
        expand(b)
        if b == 0:
            loads[4].wait()
        for y2 in range(2):
            index = 2 * b + y2

            def keep(span, value, index=index):
                stage[index, :, span] = value.astype(jnp.bfloat16)

            contract(2 * y2 + 1 - me.c, keep)
            net.start(
                remote(
                    stage.at[index], from_c.at[index],
                    c_send.at[index], c_recv.at[index], partner,
                )
            )
        for y2 in range(2):
            index = 2 * b + y2

            def hold(span, value, index=index):
                own[index, :, span] = value

            contract(2 * y2 + me.c, hold)

    to_y, to_z = me.at(y=1 - me.y), me.at(z=me.mate)
    low, high = slice(0, cut), slice(cut, own_rows)
    yo = 1 - me.y

    def summed(b, y2, part):
        return own[2 * b + y2, part, :] + from_c[2 * b + y2, part, :].astype(jnp.float32)

    for index in range(4):
        remote(
            stage.at[index], from_c.at[index], c_send.at[index], c_recv.at[index], partner
        ).wait_recv()
    for k, (b, y2, part, device) in enumerate(
        (
            (0, yo, low, to_y),
            (0, yo, high, to_z),
            (1, yo, low, to_y),
            (0, me.y, high, to_z),
        )
    ):
        send_a[k] = summed(b, y2, part).astype(jnp.bfloat16)
        net.start(remote(send_a.at[k], from_a.at[k], a_send.at[k], a_recv.at[k], device))

    def wait_a(k, device):
        remote(send_a.at[k], from_a.at[k], a_send.at[k], a_recv.at[k], device).wait_recv()

    wait_a(0, to_y)
    send_b[0] = (summed(0, me.y, low) + from_a[0].astype(jnp.float32)).astype(jnp.bfloat16)
    net.start(remote(send_b.at[0], from_b.at[0], b_send.at[0], b_recv.at[0], to_z))
    wait_a(1, to_z)
    send_b[1] = (summed(1, yo, high) + from_a[1].astype(jnp.float32)).astype(jnp.bfloat16)
    net.start(remote(send_b.at[1], from_b.at[1], b_send.at[1], b_recv.at[1], to_y))
    wait_a(2, to_y)
    wait_a(3, to_z)
    for k, (part, device) in enumerate(((low, to_z), (high, to_y))):
        remote(send_b.at[k], from_b.at[k], b_send.at[k], b_recv.at[k], device).wait_recv()
        ffn = (
            summed(1, me.y, part)
            + from_a[2 + k].astype(jnp.float32)
            + from_b[k].astype(jnp.float32)
        )
        values = residual_scale * mixed[part, :].astype(jnp.float32) + ffn
        out[part, :] = norm_rows(values, gain[...]).astype(jnp.bfloat16)
    net.drain()


def tail(x_rows, wv, wg, wd, mixed, gain, tv, tg):
    rows = x_rows.shape[1] - HALO
    own_rows, features = mixed.shape
    depth, width = wv.shape[1], wv.shape[2]
    cut = own_rows // 2
    bf16, f32 = jnp.bfloat16, jnp.float32
    dma = pltpu.SemaphoreType.DMA
    anywhere = pl.BlockSpec(memory_space=pl.ANY)
    vmem = pl.BlockSpec(memory_space=pltpu.VMEM)
    return pl.pallas_call(
        tail_kernel,
        out_shape=jax.ShapeDtypeStruct((own_rows, features), bf16),
        in_specs=[anywhere] * 4 + [vmem] * 4,
        out_specs=vmem,
        scratch_shapes=[
            pltpu.VMEM((2, HALO + rows, features), bf16),
            pltpu.VMEM((depth, width), bf16),
            pltpu.VMEM((depth, width), bf16),
            pltpu.VMEM(wd.shape[1:], bf16),
            pltpu.VMEM((HALO + rows, 2 * LANES), f32),
            pltpu.VMEM((HALO + rows, 2 * LANES), f32),
            pltpu.VMEM((rows, width), bf16),
            pltpu.VMEM((4, own_rows, features), f32),
            pltpu.VMEM((4, own_rows, features), bf16),
            pltpu.VMEM((4, own_rows, features), bf16),
            pltpu.VMEM((4, cut, features), bf16),
            pltpu.VMEM((4, cut, features), bf16),
            pltpu.VMEM((2, cut, features), bf16),
            pltpu.VMEM((2, cut, features), bf16),
            dma((5,)), dma((4,)), dma((4,)), dma((4,)), dma((4,)), dma((2,)), dma((2,)),
        ],
        compiler_params=pltpu.CompilerParams(
            has_side_effects=True, vmem_limit_bytes=62 * 1024 * 1024
        ),
        name="tail",
    )(x_rows, wv, wg, wd, mixed, gain, tv, tg)


def relayed(
    query_small, key_small, value_small, gates_small,
    query_large, key_large, value_large, gates_large,
    residual, mixer_small, mixer_large, mix_gain,
    value_weight, gate_weight, value_taps, gate_taps, down_weight, final_gain,
):
    rows = query_small.shape[0]
    small, large = gates_small.T, gates_large.T
    blank = jnp.zeros((5, rows), jnp.float32)
    gate_rows = jnp.stack(
        [jnp.concatenate([small[2 * h : 2 * h + 2], large[h : h + 1], blank]) for h in range(2)]
    )
    wv, wg, wd, x_rows, mixed = front(
        query_small, query_large, key_small, key_large, value_small, value_large, gate_rows,
        mixer_small, mixer_large, value_weight, gate_weight, down_weight,
        residual, mix_gain[None],
    )
    return tail(x_rows, wv, wg, wd, mixed, final_gain[None], value_taps, gate_taps)


def solution(mesh):
    in_specs = (
        P("sp", "tp"),
        P("sp", "tp"),
        P("sp", "tp"),
        P("sp", "tp"),
        P("sp", "tp"),
        P("sp", "tp"),
        P("sp", "tp"),
        P("sp", "tp"),
        P(("sp", "tp"), None),
        P("tp", None),
        P("tp", None),
        P(),
        P("sp", "tp"),
        P("sp", "tp"),
        P(None, "tp"),
        P(None, "tp"),
        P("tp", "sp"),
        P(),
    )
    out_specs = P(("sp", "tp"), None)
    sp_count, tp_count = mesh.shape["sp"], mesh.shape["tp"]

    def step(*arrays):
        if fits(sp_count, tp_count, arrays):
            return relayed(*arrays)
        return per_device(*arrays)

    return jax.shard_map(
        step, mesh=mesh, in_specs=in_specs, out_specs=out_specs, check_vma=False
    )
```

```python
import jax
import jax.numpy as jnp
from jax import lax
from jax.experimental import pallas as pl
from jax.experimental.pallas import tpu as pltpu
from jax.sharding import PartitionSpec as P


DS = 64
DL = 128


residual_scale = 2.0**0.5
epsilon = 1e-05


def passed_along(value, axis, steps):
    count = lax.axis_size(axis)
    first, last = (max(0, -steps), min(count, count - steps))
    return lax.ppermute(value, axis, [(source, source + steps) for source in range(first, last)])


def rotated(value, axis, steps):
    count = lax.axis_size(axis)
    return lax.ppermute(value, axis, [(s, (s + steps) % count) for s in range(count)])


def swapped(value, axis):
    return lax.ppermute(value, axis, [(s, s ^ 1) for s in range(lax.axis_size(axis))])


def norm_rows(values, gain):
    center = jnp.mean(values, axis=-1, keepdims=True)
    spread = jnp.mean(jnp.square(values - center), axis=-1, keepdims=True)
    return (values - center) * lax.rsqrt(spread + epsilon) * gain


def attend_body(small_count, diagonal, *refs):
    if diagonal:
        q_ref, k_ref, v_ref, gk_ref, gq_ref, peak_out, sum_out, acc_out = refs
    else:
        valid_ref, q_ref, k_ref, v_ref, gk_ref, gq_ref = refs[:6]
        peak_in, sum_in, acc_in, peak_out, sum_out, acc_out = refs[6:]
    head = pl.program_id(0)
    scale = jnp.where(head < small_count, DS ** (-0.5), DL ** (-0.5)).astype(jnp.float32)

    def logits():
        scores = lax.dot_general(
            q_ref[0], k_ref[...], (((1,), (1,)), ((), ())), preferred_element_type=jnp.float32
        )
        return scores * scale + (gq_ref[0] - gk_ref[0])

    if diagonal:
        scores = logits()
        query_rows = pl.program_id(1) * scores.shape[0]
        allowed = query_rows + lax.broadcasted_iota(
            jnp.int32, scores.shape, 0
        ) >= lax.broadcasted_iota(jnp.int32, scores.shape, 1)
        scores = jnp.where(allowed, scores, -jnp.inf)
        peak = jnp.max(scores, axis=-1, keepdims=True)
        weights = jnp.exp(scores - peak)
        peak_out[0] = peak
        sum_out[0] = jnp.sum(weights, axis=-1, keepdims=True)
        acc_out[0] = jnp.dot(
            weights.astype(jnp.bfloat16), v_ref[...], preferred_element_type=jnp.float32
        )
        return

    @pl.when(valid_ref[0] > 0)
    def _():
        scores = logits()
        peak = jnp.maximum(peak_in[0], jnp.max(scores, axis=-1, keepdims=True))
        factor = jnp.exp(peak_in[0] - peak)
        weights = jnp.exp(scores - peak)
        peak_out[0] = peak
        sum_out[0] = sum_in[0] * factor + jnp.sum(weights, axis=-1, keepdims=True)
        acc_out[0] = acc_in[0] * factor + jnp.dot(
            weights.astype(jnp.bfloat16), v_ref[...], preferred_element_type=jnp.float32
        )

    @pl.when(valid_ref[0] <= 0)
    def _():
        peak_out[0] = peak_in[0]
        sum_out[0] = sum_in[0]
        acc_out[0] = acc_in[0]


def attend(q_heads, key_value, key_gates, query_gates, small_count, state, valid):
    heads, rows, width = q_heads.shape
    per_small = width // DS
    groups = key_value.shape[1] // (2 * width)
    block = rows // 3 if rows % 3 == 0 and (rows // 3) % 128 == 0 else rows
    diagonal = state is None
    small_groups = small_count // per_small

    def group(h):
        return jnp.where(h < small_count, h // per_small, h - small_count + small_groups)

    per_query = pl.BlockSpec((1, block, 1), lambda h, i: (h, i, 0))
    wide = pl.BlockSpec((1, block, width), lambda h, i: (h, i, 0))
    in_specs = [
        wide,
        pl.BlockSpec((rows, width), lambda h, i: (0, group(h))),
        pl.BlockSpec((rows, width), lambda h, i: (0, groups + group(h))),
        pl.BlockSpec((1, 1, rows), lambda h, i: (h, 0, 0)),
        per_query,
    ]
    operands = [q_heads, key_value, key_value, key_gates[:, None, :], query_gates[:, :, None]]
    aliases = {}
    if not diagonal:
        in_specs = [pl.BlockSpec(memory_space=pltpu.SMEM)] + in_specs + [per_query, per_query, wide]
        operands = [valid] + operands + list(state)
        aliases = {6: 0, 7: 1, 8: 2}
    column = jax.ShapeDtypeStruct((heads, rows, 1), jnp.float32)

    def kernel(*refs):
        attend_body(small_count, diagonal, *refs)

    return pl.pallas_call(
        kernel,
        grid=(heads, rows // block),
        in_specs=in_specs,
        out_specs=[per_query, per_query, wide],
        out_shape=[column, column, jax.ShapeDtypeStruct((heads, rows, width), jnp.float32)],
        input_output_aliases=aliases,
        cost_estimate=pl.CostEstimate(
            flops=heads * rows * rows * width * 4,
            bytes_accessed=heads * rows * width * 12,
            transcendentals=heads * rows * rows,
        ),
        compiler_params=pltpu.CompilerParams(
            dimension_semantics=("arbitrary", "arbitrary"), vmem_limit_bytes=56 * 1024 * 1024
        ),
    )(*operands)


def per_device(
    query_small,
    key_small,
    value_small,
    gates_small,
    query_large,
    key_large,
    value_large,
    gates_large,
    residual,
    mixer_small,
    mixer_large,
    mix_gain,
    value_weight,
    gate_weight,
    value_taps,
    gate_taps,
    down_weight,
    final_gain,
):
    shard_rows = query_small.shape[0]
    sp_index = lax.axis_index("sp")
    tp_index = lax.axis_index("tp")
    tensor_parts = lax.axis_size("tp")
    sp_count = lax.axis_size("sp")
    splits = all(
        count % 2 == 0 and count * size % (2 * DL) == 0
        for count, size in ((gates_small.shape[1], DS), (gates_large.shape[1], DL))
    )
    team = 2 if splits and sp_count % 2 == 0 else 1
    pair_count = sp_count // team
    pair, side = sp_index // team, sp_index % team
    half_small = query_small.shape[1] // team
    small_count = gates_small.shape[1] // team
    large_count = gates_large.shape[1] // team

    def half(array, which):
        width = array.shape[1] // team
        return lax.dynamic_slice_in_dim(array, which * width, width, 1)

    def halves(parts, which):
        return jnp.concatenate([half(a, which) for a in parts], axis=1)

    def exchanged(parts):
        if team == 1:
            return jnp.concatenate(parts, axis=1)
        return in_order(halves(parts, side), swapped(halves(parts, 1 - side), "sp"), 0)

    def in_order(own, other, axis):
        return jnp.where(
            side == 0,
            jnp.concatenate([own, other], axis=axis),
            jnp.concatenate([other, own], axis=axis),
        )

    gate_parts = (gates_small, gates_large)
    key_value = exchanged((key_small, key_large, value_small, value_large))
    if team == 1:
        own_gates = jnp.concatenate(gate_parts, axis=1).T
    else:
        own_gates = in_order(
            halves(gate_parts, side).T, swapped(halves(gate_parts, 1 - side).T, "sp"), 1
        )
    queries = exchanged((query_small, query_large))

    width = DL
    per_small = width // DS
    lane_head = jnp.arange(width) // DS
    q_heads = []
    for h in range(small_count):
        columns = queries[:, (h // per_small) * width : (h // per_small + 1) * width]
        q_heads.append(jnp.where(lane_head == h % per_small, columns, 0).astype(jnp.bfloat16))
    for h in range(large_count):
        q_heads.append(queries[:, half_small + h * width : half_small + (h + 1) * width])
    q_heads = jnp.stack(q_heads)

    mixers = jnp.concatenate([mixer_small, mixer_large], axis=0)
    mixer_of = [mixers]
    for s in range(1, tensor_parts):
        mixer_of.append(rotated(mixers, "tp", -s))
    full_value = lax.all_gather(value_weight, "sp", axis=0, tiled=True)
    full_gate = lax.all_gather(gate_weight, "sp", axis=0, tiled=True)
    down_pieces = down_parts(down_weight)

    arriving, gates_arriving = [key_value], [own_gates]
    for step in range(1, pair_count):
        gates_arriving.append(passed_along(own_gates, "sp", step * team))
        arriving.append(passed_along(arriving[-1], "sp", team))
    state = attend(q_heads, key_value, own_gates, own_gates, small_count, None, None)
    for step in range(1, pair_count):
        valid = (pair >= step).astype(jnp.int32).reshape(1)
        state = attend(
            q_heads, arriving[step], gates_arriving[step], own_gates, small_count, state, valid
        )
    head_out = (state[2] / state[1]).astype(jnp.bfloat16)
    columns = []
    for g in range(small_count // per_small):
        merged = head_out[g * per_small]
        for h in range(1, per_small):
            merged = jnp.where(lane_head == h, head_out[g * per_small + h], merged)
        columns.append(merged)
    for h in range(large_count):
        columns.append(head_out[small_count + h])
    attended = jnp.concatenate(columns, axis=1)
    joined = attended
    if team == 2:
        own = lax.dynamic_slice_in_dim(attended, side * shard_rows, shard_rows, 0)
        other = swapped(
            lax.dynamic_slice_in_dim(attended, (1 - side) * shard_rows, shard_rows, 0), "sp"
        )
        joined = jnp.concatenate(
            [
                in_order(own[:, :half_small], other[:, :half_small], 1),
                in_order(own[:, half_small:], other[:, half_small:], 1),
            ],
            axis=1,
        )
    own_rows = shard_rows // tensor_parts
    arrived = lax.all_to_all(joined, "tp", split_axis=0, concat_axis=1, tiled=True)
    mix = jnp.zeros((own_rows, mixers.shape[1]), jnp.float32)
    for s in range(tensor_parts):
        source = (tp_index + s) % tensor_parts
        mix = mix + jnp.dot(
            lax.dynamic_slice_in_dim(arrived, source * joined.shape[1], joined.shape[1], 1),
            mixer_of[s],
            preferred_element_type=jnp.float32,
        )
    mixed = norm_rows(residual_scale * residual.astype(jnp.float32) + mix, mix_gain).astype(
        jnp.bfloat16
    )
    block_input = jnp.zeros((shard_rows, mixed.shape[1]), jnp.bfloat16)
    for s in range(tensor_parts):
        piece = mixed if s == 0 else rotated(mixed, "tp", -s)
        source = (tp_index + s) % tensor_parts
        block_input = lax.dynamic_update_slice_in_dim(block_input, piece, source * own_rows, 0)

    up_value = jnp.dot(block_input, full_value, preferred_element_type=jnp.float32).astype(
        jnp.bfloat16
    )
    up_gate = jnp.dot(block_input, full_gate, preferred_element_type=jnp.float32).astype(
        jnp.bfloat16
    )
    down_base, up_value = lax.optimization_barrier((down_weight, up_value))
    full_down = assembled(down_base, down_pieces)
    hidden_width = up_value.shape[1]
    trailing = jnp.concatenate([up_value[-2:], up_gate[-2:]], axis=1)
    earlier = passed_along(trailing, "sp", 1)
    padded_value = jnp.concatenate([earlier[:, :hidden_width], up_value], axis=0).astype(
        jnp.float32
    )
    padded_gate = jnp.concatenate([earlier[:, hidden_width:], up_gate], axis=0).astype(jnp.float32)
    filt_value = (
        value_taps[0] * padded_value[:-2]
        + value_taps[1] * padded_value[1:-1]
        + value_taps[2] * padded_value[2:]
    )
    filt_gate = (
        gate_taps[0] * padded_gate[:-2]
        + gate_taps[1] * padded_gate[1:-1]
        + gate_taps[2] * padded_gate[2:]
    )
    hidden = (jax.nn.silu(filt_gate) * filt_value).astype(jnp.bfloat16)

    def ffn_rows(s):
        target = (tp_index + s) % tensor_parts
        part = lax.dynamic_slice_in_dim(hidden, target * own_rows, own_rows, 0)
        return jnp.dot(part, full_down, preferred_element_type=jnp.float32)

    order = [tensor_parts // 2] + [s for s in range(1, tensor_parts) if s != tensor_parts // 2]
    received = [rotated(ffn_rows(s).astype(jnp.bfloat16), "tp", s) for s in order]
    ffn = ffn_rows(0)
    for part in received:
        ffn = ffn + part.astype(jnp.float32)
    return norm_rows(residual_scale * mixed.astype(jnp.float32) + ffn, final_gain).astype(
        jnp.bfloat16
    )


def down_parts(down_weight):
    pieces = []
    for s in range(1, lax.axis_size("sp")):
        pieces.append(rotated(down_weight, "sp", -s))
    return pieces


def assembled(own, pieces):
    count = lax.axis_size("sp")
    width = own.shape[1]
    index = lax.axis_index("sp")
    full = jnp.zeros((own.shape[0], count * width), own.dtype)
    for s, piece in enumerate([own] + pieces):
        full = lax.dynamic_update_slice_in_dim(full, piece, ((index + s) % count) * width, 1)
    return full


MESH = pl.DeviceIdType.MESH
LANES = 128
HALO = 16


def fits(sp_count, tp_count, arrays):
    query, gates_small, gates_large = arrays[0], arrays[3], arrays[7]
    query_large, value_weight = arrays[4], arrays[12]
    rows = query.shape[0]
    own = rows // tp_count
    return (
        tp_count == 4
        and sp_count % 4 == 0
        and query.shape[1] == 2 * LANES
        and query_large.shape[1] == 2 * LANES
        and gates_small.shape[1] == 2 * LANES // DS
        and gates_large.shape[1] == 2
        and rows % (3 * LANES) == 0
        and own % (2 * HALO) == 0
        and value_weight.shape[1] % LANES == 0
        and value_weight.shape[0] % HALO == 0
    )


def half_width(columns):
    return -(-columns // (2 * LANES)) * LANES


class Place:
    def __init__(self):
        self.count = lax.axis_size("sp")
        self.nz = self.count // 2
        self.sp = lax.axis_index("sp")
        self.tp = lax.axis_index("tp")
        self.z, self.x = self.sp // 2, self.sp % 2
        self.y, self.c = self.tp // 2, self.tp % 2
        self.parity = self.z % 2
        self.mate = self.z + 1 - 2 * self.parity

    def at(self, z=None, x=None, y=None, c=None):
        z = self.z if z is None else z
        x = self.x if x is None else x
        y = self.y if y is None else y
        c = self.c if c is None else c
        return (z * 2 + x, y * 2 + c)


class Traffic:
    def __init__(self):
        self.sent = []

    def start(self, copy, when=None):
        guarded(when, copy.start)
        self.sent.append((copy, when))

    def drain(self):
        for copy, when in self.sent:
            guarded(when, copy.wait_send)


def guarded(when, action):
    if when is None:
        action()
    else:

        @pl.when(when)
        def _():
            action()


def remote(source, target, send, receive, device):
    return pltpu.make_async_remote_copy(
        src_ref=source,
        dst_ref=target,
        send_sem=send,
        recv_sem=receive,
        device_id=device,
        device_id_type=MESH,
    )


def front_kernel(
    qs, ql, ks, kl, vs, vl, gt, ms, ml, wv, wg, wd, res, gain, tv, tg,
    o_wv, o_wg, o_wd, o_rows, o_mixed, o_hidden,
    rows_buf, wv_buf, wg_buf, uv, ug, hidden, load_sem,
    q_buf, kv, gk, gq, peak, total, acc, o_buf, arrived, mixers, y_buf, zero, bounce_a, bounce_b,
    local_sem, x_send, x_recv, kv_send, kv_recv, g_send, g_recv,
    w_up, w_dn, w_zr, w_xs, w_xr, b_sem, m_local, m_send, m_recv,
    o_send, o_recv, a_send, a_recv, h_send, h_recv, a_local,
):
    me = Place()
    net = Traffic()
    nz, z, x, sp, tp = me.nz, me.z, me.x, me.sp, me.tp
    rows = qs.shape[0]
    own_rows = rows // 4
    other = 1 - x
    mine = pl.ds(pl.multiple_of(x * rows, LANES), rows)
    theirs = pl.ds(pl.multiple_of(other * rows, LANES), rows)
    own_lanes = pl.ds(pl.multiple_of(x * LANES, LANES), LANES)
    other_lanes = pl.ds(pl.multiple_of(other * LANES, LANES), LANES)
    weights = ((wv, o_wv), (wg, o_wg), (wd, o_wd))
    depth = wv.shape[0]
    full_width = wv.shape[1]
    width = half_width(full_width)

    def parts(which):
        return (
            (qs, q_buf.at[which, 0:LANES]),
            (ql, q_buf.at[which, LANES : 2 * LANES]),
            (ks, kv.at[z, which, 0:LANES]),
            (kl, kv.at[z, which, LANES : 2 * LANES]),
            (vs, kv.at[z, which, 2 * LANES : 3 * LANES]),
            (vl, kv.at[z, which, 3 * LANES : 4 * LANES]),
        )

    locals_ = []
    for i, (source, target) in enumerate(parts(mine)):
        net.start(
            remote(source.at[:, other_lanes], target, x_send.at[i], x_recv.at[i], me.at(x=other))
        )
        locals_.append(pltpu.make_async_copy(source.at[:, own_lanes], target, local_sem.at[i]))
    net.start(
        remote(gt.at[other], gk.at[z, :, mine], x_send.at[6], x_recv.at[6], me.at(x=other))
    )
    locals_.append(pltpu.make_async_copy(gt.at[x], gk.at[z, :, mine], local_sem.at[6]))
    for copy in locals_:
        copy.start()

    mixer_rows = 4 * LANES
    mixer_locals = []
    for h in range(2):
        for k, source in enumerate((ms, ml)):
            row = tp * mixer_rows + (2 * h + k) * LANES
            mixer_locals.append(
                pltpu.make_async_copy(
                    source.at[h * LANES : (h + 1) * LANES],
                    mixers.at[pl.ds(row, LANES)],
                    m_local.at[2 * h + k],
                )
            )
    for copy in mixer_locals:
        copy.start()

    def mixer_slot(t):
        return mixers.at[pl.ds(t * mixer_rows, mixer_rows)]

    def half_of(w, half):
        offset = pl.multiple_of(half * (full_width - width), LANES)
        source = weights[w][0]
        if w == 2:
            return source.at[pl.ds(offset, width), :]
        return source.at[:, pl.ds(offset, width)]

    def slot(w, which, zs, xs):
        shard = zs * 2 + xs
        if w == 2:
            return weights[w][1].at[which, shard]
        return weights[w][1].at[which, pl.ds(shard * depth, depth), :]

    def origin(w, which, zs, own):
        if not own:
            return slot(w, which, zs, x)
        return half_of(w, me.parity if which == 0 else 1 - me.parity)

    def both(a, b):
        return b if a is None else jnp.logical_and(a, b)

    upper, lower = jnp.minimum(z + 1, nz - 1), jnp.maximum(z - 1, 0)

    def go_up(w, e, zs, own, when=None):
        net.start(
            remote(
                origin(w, 1 - e, zs, own), slot(w, e, zs, x),
                w_up.at[w, e, zs], w_zr.at[w, e, zs], me.at(z=upper),
            ),
            both(when, z + 1 + e < nz),
        )

    def go_down(w, e, zs, own, when=None):
        net.start(
            remote(
                origin(w, 1 - e, zs, own), slot(w, e, zs, x),
                w_dn.at[w, e, zs], w_zr.at[w, e, zs], me.at(z=lower),
            ),
            both(when, z - 1 - e >= 0),
        )

    def own_up(w, when=None):
        go_up(w, 1, z, True, when)
        go_up(w, 0, z, True, when)

    def own_down(w, when=None):
        go_down(w, 1, z, True, when)
        go_down(w, 0, z, True, when)

    def send_across(w, zs, own, when=None):
        net.start(
            remote(
                origin(w, 0, zs, own), slot(w, 0, zs, x),
                w_xs.at[w, zs], w_xr.at[w, zs], me.at(x=other),
            ),
            when,
        )

    def landed(w, which, zs, when):
        copy = remote(
            slot(w, which, zs, x), slot(w, which, zs, x),
            w_up.at[w, which, zs], w_zr.at[w, which, zs], me.at(x=other),
        )
        guarded(when, copy.wait_recv)

    def up_pass(w, r, when=None):
        if r < nz:
            zs, here_ = jnp.maximum(z - r, 0), both(when, jnp.logical_and(z - r >= 0, z + 1 < nz))
            landed(w, 1, zs, here_)
            go_up(w, 0, zs, False, here_)

    def up_keep(w, r, when=None):
        if r < nz:
            zs, here_ = jnp.maximum(z - r, 0), both(when, z - r >= 0)
            landed(w, 0, zs, here_)
            go_up(w, 1, zs, False, here_)
            send_across(w, zs, False, here_)

    def down_pass(w, r, when=None):
        if r < nz:
            zs, here_ = jnp.minimum(z + r, nz - 1), both(when, jnp.logical_and(z + r < nz, z >= 1))
            landed(w, 1, zs, here_)
            go_down(w, 0, zs, False, here_)

    def down_keep(w, r, when=None):
        if r < nz:
            zs, here_ = jnp.minimum(z + r, nz - 1), both(when, z + r < nz)
            landed(w, 0, zs, here_)
            go_down(w, 1, zs, False, here_)
            send_across(w, zs, False, here_)

    def piece(j, p):
        span = mine if p == 0 else theirs
        return kv.at[j, span, :], gk.at[j, :, span]

    def pass_on(j, p, when):
        data, gate = piece(j, p)
        above = me.at(z=jnp.minimum(z + 1, nz - 1))
        net.start(remote(data, data, kv_send.at[j, p], kv_recv.at[j, p], above), when)
        net.start(remote(gate, gate, g_send.at[j, p], g_recv.at[j, p], above), when)

    def take(j, p, when):
        data, gate = piece(j, p)
        above = me.at(z=jnp.minimum(z + 1, nz - 1))
        guarded(when, remote(data, data, kv_send.at[j, p], kv_recv.at[j, p], above).wait_recv)
        guarded(when, remote(gate, gate, g_send.at[j, p], g_recv.at[j, p], above).wait_recv)

    def relay(r, p):
        if r >= nz:
            return
        j = jnp.maximum(z - r, 0)
        take(j, p, z - r >= 0)
        pass_on(j, p, jnp.logical_and(z - r >= 0, z + 1 < nz))

    block = 2 * rows // 3
    count = 3

    def head_facts(h):
        lanes = lax.broadcasted_iota(jnp.int32, (1, LANES), 1)
        low = jnp.where(h == 1, DS, 0)
        high = jnp.where(h == 0, DS, LANES)
        keep = jnp.logical_and(lanes >= low, lanes < high)
        column = pl.multiple_of(jnp.where(h == 2, LANES, 0), LANES)
        scale = jnp.where(h == 2, DL ** (-0.5), DS ** (-0.5)).astype(jnp.float32)
        return keep, column, scale

    def query_part(h, span):
        keep, column, scale = head_facts(h)
        q = q_buf[span, pl.ds(column, LANES)]
        return jnp.where(keep, q, jnp.zeros_like(q)), column, scale

    def shifted_scores(q, j, h, column, scale, keys):
        k = kv[j, keys, pl.ds(column, LANES)]
        scores = lax.dot_general(
            q, k, (((1,), (1,)), ((), ())), preferred_element_type=jnp.float32
        )
        return scores * scale - gk[j, pl.ds(h, 1), keys]

    def weighted(weights_, j, column, keys):
        v = kv[j, keys, pl.ds(column + 2 * LANES, LANES)]
        return jnp.dot(weights_.astype(jnp.bfloat16), v, preferred_element_type=jnp.float32)

    def attend_own():
        def head(h, carry):
            for i in range(count):
                span = pl.ds(i * block, block)
                keys = pl.ds(0, (i + 1) * block)
                q, column, scale = query_part(h, span)
                scores = shifted_scores(q, z, h, column, scale, keys)
                allowed = i * block + lax.broadcasted_iota(
                    jnp.int32, scores.shape, 0
                ) >= lax.broadcasted_iota(jnp.int32, scores.shape, 1)
                scores = jnp.where(allowed, scores, -jnp.inf)
                gate = gq[h, span, :]
                top = jnp.max(scores, axis=-1, keepdims=True) + gate
                weights_ = jnp.exp(scores + (gate - top))
                peak[h, span, :] = top
                total[h, span, :] = jnp.sum(weights_, axis=-1, keepdims=True)
                acc[h, span, :] = weighted(weights_, z, column, keys)
            return carry

        lax.fori_loop(0, 3, head, 0)

    def attend_earlier(j):
        def part(i, carry):
            h, b = i // count, i % count
            span = pl.ds(pl.multiple_of(b * block, LANES), block)
            keys = pl.ds(0, 2 * rows)
            q, column, scale = query_part(h, span)
            scores = shifted_scores(q, j, h, column, scale, keys)
            gate = gq[h, span, :]
            before = peak[h, span, :]
            top = jnp.maximum(before, jnp.max(scores, axis=-1, keepdims=True) + gate)
            factor = jnp.exp(before - top)
            weights_ = jnp.exp(scores + (gate - top))
            peak[h, span, :] = top
            total[h, span, :] = total[h, span, :] * factor + jnp.sum(
                weights_, axis=-1, keepdims=True
            )
            acc[h, span, :] = acc[h, span, :] * factor + weighted(weights_, j, column, keys)
            return carry

        lax.fori_loop(0, 3 * count, part, 0)

    ups = (0, 1)
    at_last, low_block = z == nz - 1, z <= 1
    at_one, not_one = z == 1, z != 1
    for w in ups:
        own_down(w, z + 1 < nz)
    for copy in locals_:
        copy.wait()
    pass_on(z, 0, z + 1 < nz)
    for copy in mixer_locals:
        copy.wait()
    net.start(
        remote(mixer_slot(tp), mixer_slot(tp), m_send.at[0], m_recv.at[0], me.at(y=1 - me.y))
    )
    net.start(
        remote(mixer_slot(tp), mixer_slot(tp), m_send.at[1], m_recv.at[1], me.at(c=1 - me.c))
    )
    own_copies = []
    for w in range(3):
        target = bounce_b if w == 2 else bounce_a.at[w]
        own_copies.append(
            (
                pltpu.make_async_copy(half_of(w, me.parity), target, b_sem.at[w, 0]),
                pltpu.make_async_copy(target, slot(w, 0, z, x), b_sem.at[w, 1]),
            )
        )
    for first, _ in own_copies:
        first.start()
    relay(1, 0)
    for i, (source, target) in enumerate(parts(theirs)):
        remote(source.at[:, other_lanes], target, x_send.at[i], x_recv.at[i], me.at(x=other)).wait_recv()
    remote(gt.at[other], gk.at[z, :, theirs], x_send.at[6], x_recv.at[6], me.at(x=other)).wait_recv()
    pass_on(z, 1, z + 1 < nz)
    for w in ups:
        own_down(w, at_last)
    own_down(2)
    for w in ups:
        send_across(w, z, True)
    for first, second in own_copies:
        first.wait()
        second.start()
    columns = jnp.transpose(gk[z])
    for h in range(3):
        gq[h] = columns[:, h : h + 1]
    attend_own()

    ty = (1 - me.y) * 2 + me.c
    from_y = remote(mixer_slot(ty), mixer_slot(ty), m_send.at[2], m_recv.at[0], me.at(c=1 - me.c))
    from_y.wait_recv()
    net.start(
        remote(mixer_slot(ty), mixer_slot(ty), m_send.at[2], m_recv.at[2], me.at(c=1 - me.c))
    )
    for r in range(1, nz):
        relay(r, 1)
        relay(r + 1, 0)
        if r == 1:
            for w in ups:
                own_up(w, low_block)
        if r == 2:
            for w in ups:
                own_up(w, z > 1)
            for w in ups:
                down_pass(w, 1)
                down_keep(w, 1)
            for w in ups:
                up_keep(w, 1, at_one)
            for w in ups:
                up_pass(w, 1, at_one)
            own_up(2, low_block)

        @pl.when(z - r >= 0)
        def _(r=r):
            attend_earlier(jnp.maximum(z - r, 0))

    for h in range(3):
        done = acc[h] / total[h]
        if h == 0:
            first_head = done
        elif h == 1:
            keep, _, _ = head_facts(1)
            o_buf[:, 0:LANES] = jnp.where(keep, done, first_head).astype(jnp.bfloat16)
        else:
            o_buf[:, LANES : 2 * LANES] = done.astype(jnp.bfloat16)

    for w in ups:
        up_pass(w, 1, not_one)

    def arrival(t, xs):
        return arrived.at[:, pl.ds(pl.multiple_of((t * 2 + xs) * 2 * LANES, 2 * LANES), 2 * LANES)]

    takes = []
    for k in range(1, 8):
        dx, dy, dc = k // 4, (k // 2) % 2, k % 2
        x2 = x + dx * (1 - 2 * x)
        y2 = me.y + dy * (1 - 2 * me.y)
        c2 = me.c + dc * (1 - 2 * me.c)
        t2 = y2 * 2 + c2
        net.start(
            remote(
                o_buf.at[pl.ds(x2 * rows + t2 * own_rows, own_rows), :], arrival(tp, x),
                o_send.at[k], o_recv.at[k], me.at(x=x2, y=y2, c=c2),
            )
        )
        takes.append(
            remote(
                o_buf.at[pl.ds(0, own_rows), :], arrival(t2, x2),
                o_send.at[k], o_recv.at[k], me.at(x=x2, y=y2, c=c2),
            )
        )
    own_span = pl.ds(pl.multiple_of((tp * 2 + x) * 2 * LANES, 2 * LANES), 2 * LANES)
    arrived[:, own_span] = o_buf[pl.ds(pl.multiple_of(x * rows + tp * own_rows, HALO), own_rows), :]
    for w in ups:
        up_keep(w, 1, not_one)
    for w in ups:
        down_pass(w, 2)
        down_keep(w, 2)
    for w in ups:
        up_pass(w, 2)
    remote(mixer_slot(0), mixer_slot(tp + 1 - 2 * me.c), m_send.at[1], m_recv.at[1], me.at(c=1 - me.c)).wait_recv()
    remote(mixer_slot(0), mixer_slot(ty + 1 - 2 * me.c), m_send.at[2], m_recv.at[2], me.at(c=1 - me.c)).wait_recv()
    for copy in takes:
        copy.wait_recv()

    features = gain.shape[1]
    step = 4 * LANES

    def mix_tile(n, carry):
        span = pl.ds(pl.multiple_of(n * step, step), step)
        y_buf[:, span] = residual_scale * res[:, span].astype(jnp.float32) + jnp.dot(
            arrived[...], mixers[:, span], preferred_element_type=jnp.float32
        )
        return carry

    lax.fori_loop(0, features // step, mix_tile, 0)
    o_mixed[...] = norm_rows(y_buf[...], gain[...]).astype(jnp.bfloat16)
    zero[...] = jnp.zeros_like(zero)

    parity, mate = me.parity, me.mate

    def rows_of(zi, t, part=None):
        base = HALO + t * own_rows
        if part is None:
            return o_rows.at[zi, pl.ds(base, own_rows), :]
        return o_rows.at[zi, pl.ds(base + part * (own_rows // 2), own_rows // 2), :]

    here = rows_of(parity, tp)
    up_y, up_z, up_c = me.at(y=1 - me.y), me.at(z=mate), me.at(c=1 - me.c)
    net.start(remote(o_mixed, here, a_send.at[0], a_recv.at[0], up_z))
    net.start(remote(o_mixed, here, a_send.at[1], a_recv.at[1], up_y))
    net.start(remote(o_mixed, here, a_send.at[2], a_recv.at[2], up_c))
    keep_rows = pltpu.make_async_copy(o_mixed, here, a_local.at[0])
    keep_rows.start()
    following = jnp.minimum(sp + 1, me.count - 1)
    fz = following // 2
    sends_halo = jnp.logical_and(sp + 1 < me.count, tp == 3)
    for k in range(8):
        dz, dy, dc = k // 4, (k // 2) % 2, k % 2
        z2 = fz - fz % 2 + dz
        net.start(
            remote(
                o_mixed.at[own_rows - HALO : own_rows, :],
                o_rows.at[fz % 2, 0:HALO, :],
                h_send.at[k], h_recv.at[fz % 2],
                (z2 * 2 + 1 - x, dy * 2 + dc),
            ),
            sends_halo,
        )
    first_rows = jnp.logical_and(z - parity == 0, x == 0)
    blank = pltpu.make_async_copy(zero, o_rows.at[0, 0:HALO, :], a_local.at[1])
    guarded(first_rows, blank.start)

    for k in range(2, nz):
        for w in ups:
            up_keep(w, k)
            if k > 2:
                down_keep(w, k)
                up_pass(w, k)
                down_pass(w, k)

    p_z, p_y = rows_of(1 - parity, tp), rows_of(parity, ty)
    remote(o_mixed, p_y, a_send.at[1], a_recv.at[1], up_y).wait_recv()
    half = rows_of(parity, ty, 0)
    net.start(remote(half, half, a_send.at[3], a_recv.at[3], up_z))
    net.start(remote(p_y, p_y, a_send.at[5], a_recv.at[5], up_c))
    remote(o_mixed, p_z, a_send.at[0], a_recv.at[0], up_z).wait_recv()
    half = rows_of(1 - parity, tp, 1)
    net.start(remote(half, half, a_send.at[4], a_recv.at[4], up_y))
    net.start(remote(p_z, p_z, a_send.at[6], a_recv.at[6], up_c))
    for k in range(2):
        half = rows_of(1 - parity, ty, k)
        remote(half, half, a_send.at[3 + k], a_recv.at[3 + k], up_c).wait_recv()
        net.start(remote(half, half, a_send.at[7 + k], a_recv.at[7 + k], up_c))

    own_up(2, z > 1)
    send_across(2, z, True)
    up_keep(2, 1, at_one)
    up_pass(2, 1, at_one)
    down_keep(2, 1, at_one)
    down_pass(2, 1, at_one)

    tc, tyc = tp + 1 - 2 * me.c, ty + 1 - 2 * me.c
    for k, target in (
        (2, rows_of(parity, tc)),
        (5, rows_of(parity, tyc)),
        (6, rows_of(1 - parity, tc)),
        (7, rows_of(1 - parity, tyc, 0)),
        (8, rows_of(1 - parity, tyc, 1)),
    ):
        remote(target, target, a_send.at[k], a_recv.at[k], up_c).wait_recv()
    for i in range(2):
        halo = o_rows.at[i, 0:HALO, :]
        copy = remote(halo, halo, h_send.at[i], h_recv.at[i], up_c)
        guarded((z - parity + i) * 2 + x - 1 >= 0, copy.wait_recv)
    guarded(first_rows, blank.wait)
    keep_rows.wait()
    for _, second in own_copies:
        second.wait()

    def from_across(w):
        for zs in range(nz):
            target = slot(w, 0, zs, other)
            remote(target, target, w_xs.at[w, zs], w_xr.at[w, zs], me.at(x=other)).wait_recv()

    from_across(0)
    from_across(1)

    loads = [
        pltpu.make_async_copy(o_rows.at[1 - parity], rows_buf.at[0], load_sem.at[0]),
        pltpu.make_async_copy(o_wv.at[0], wv_buf, load_sem.at[1]),
        pltpu.make_async_copy(o_wg.at[0], wg_buf, load_sem.at[2]),
        pltpu.make_async_copy(o_rows.at[parity], rows_buf.at[1], load_sem.at[3]),
    ]
    for copy in loads:
        copy.start()
    tile = 2 * LANES
    offset = parity * (full_width - width)
    repeated = jnp.where(parity == 1, 2 * width - full_width, 0)

    def expand(b):
        def tile_of(n, carry):
            span = pl.ds(pl.multiple_of(n * tile, tile), tile)
            taps = pl.ds(pl.multiple_of(offset + n * tile, LANES), tile)
            filtered = []
            for buf, weight, tap in ((uv, wv_buf, tv), (ug, wg_buf, tg)):
                up = jnp.dot(rows_buf[b], weight[:, span], preferred_element_type=jnp.float32)
                buf[...] = up.astype(jnp.bfloat16).astype(jnp.float32)
                filtered.append(
                    tap[0:1, taps] * buf[HALO - 2 : HALO - 2 + rows, :]
                    + tap[1:2, taps] * buf[HALO - 1 : HALO - 1 + rows, :]
                    + tap[2:3, taps] * buf[HALO : HALO + rows, :]
                )
            value, gate = filtered
            result = value * (gate / (1.0 + jnp.exp(-gate)))
            unit = n * tile + lax.broadcasted_iota(jnp.int32, (1, tile), 1)
            result = jnp.where(unit >= repeated, result, 0.0)
            hidden[b, :, span] = result.astype(jnp.bfloat16)
            return carry

        lax.fori_loop(0, width // tile, tile_of, 0)

    outs = [
        pltpu.make_async_copy(hidden.at[b], o_hidden.at[b], load_sem.at[4 + b]) for b in range(2)
    ]
    for copy in loads[:3]:
        copy.wait()
    down_pass(2, 1, not_one)
    down_keep(2, 1, not_one)
    up_keep(2, 1, not_one)
    up_pass(2, 1, not_one)
    inner = z < nz - 1
    down_pass(2, 2, inner)
    up_pass(2, 2, inner)
    up_keep(2, 2, inner)
    expand(0)
    outs[0].start()
    up_keep(2, 2, at_last)
    down_keep(2, 2)
    loads[3].wait()
    expand(1)
    outs[1].start()
    for k in range(3, nz):
        up_keep(2, k)
        down_keep(2, k)
        up_pass(2, k)
        down_pass(2, k)
    from_across(2)
    for copy in outs:
        copy.wait()
    net.drain()


def front(qs, ql, ks, kl, vs, vl, gt, ms, ml, wv, wg, wd, res, gain, tv, tg):
    count = lax.axis_size("sp")
    nz = count // 2
    rows = qs.shape[0]
    own_rows = rows // 4
    features = gain.shape[1]
    depth, width = wv.shape[0], half_width(wv.shape[1])
    down_columns = wd.shape[1]
    bf16, f32 = jnp.bfloat16, jnp.float32
    dma = pltpu.SemaphoreType.DMA
    anywhere = pl.BlockSpec(memory_space=pl.ANY)
    vmem = pl.BlockSpec(memory_space=pltpu.VMEM)
    return pl.pallas_call(
        front_kernel,
        out_shape=[
            jax.ShapeDtypeStruct((2, count * depth, width), bf16),
            jax.ShapeDtypeStruct((2, count * depth, width), bf16),
            jax.ShapeDtypeStruct((2, count, width, down_columns), bf16),
            jax.ShapeDtypeStruct((2, HALO + rows, features), bf16),
            jax.ShapeDtypeStruct((own_rows, features), bf16),
            jax.ShapeDtypeStruct((2, rows, width), bf16),
        ],
        in_specs=[anywhere] * 12 + [vmem] * 4,
        out_specs=[anywhere] * 4 + [vmem, anywhere],
        scratch_shapes=[
            pltpu.VMEM((2, HALO + rows, features), bf16),
            pltpu.VMEM((count * depth, width), bf16),
            pltpu.VMEM((count * depth, width), bf16),
            pltpu.VMEM((HALO + rows, 2 * LANES), f32),
            pltpu.VMEM((HALO + rows, 2 * LANES), f32),
            pltpu.VMEM((2, rows, width), bf16),
            dma((6,)),
            pltpu.VMEM((2 * rows, 2 * LANES), bf16),
            pltpu.VMEM((nz, 2 * rows, 4 * LANES), bf16),
            pltpu.VMEM((nz, 8, 2 * rows), f32),
            pltpu.VMEM((3, 2 * rows, 1), f32),
            pltpu.VMEM((3, 2 * rows, 1), f32),
            pltpu.VMEM((3, 2 * rows, 1), f32),
            pltpu.VMEM((3, 2 * rows, LANES), f32),
            pltpu.VMEM((2 * rows, 2 * LANES), bf16),
            pltpu.VMEM((own_rows, 16 * LANES), bf16),
            pltpu.VMEM((16 * LANES, features), bf16),
            pltpu.VMEM((own_rows, features), f32),
            pltpu.VMEM((HALO, features), bf16),
            pltpu.VMEM((2, depth, width), bf16),
            pltpu.VMEM((width, down_columns), bf16),
            dma((7,)), dma((7,)), dma((7,)),
            dma((nz, 2)), dma((nz, 2)), dma((nz, 2)), dma((nz, 2)),
            dma((3, 2, nz)), dma((3, 2, nz)), dma((3, 2, nz)),
            dma((3, nz)), dma((3, nz)),
            dma((3, 2)), dma((4,)), dma((3,)), dma((3,)),
            dma((8,)), dma((8,)), dma((9,)), dma((9,)), dma((8,)), dma((2,)), dma((2,)),
        ],
        compiler_params=pltpu.CompilerParams(
            has_side_effects=True, vmem_limit_bytes=62 * 1024 * 1024
        ),
        name="front",
    )(qs, ql, ks, kl, vs, vl, gt, ms, ml, wv, wg, wd, res, gain, tv, tg)


def tail_kernel(
    hidden, wd, mixed, gain,
    out,
    wd_buf, own, stage, from_c, send_a, from_a, send_b, from_b,
    load_sem, c_send, c_recv, a_send, a_recv, b_send, b_recv,
):
    me = Place()
    net = Traffic()
    own_rows = mixed.shape[0]
    cut = own_rows // 2
    shards, down_columns = wd.shape[1], wd.shape[3]
    load = pltpu.make_async_copy(wd.at[0], wd_buf, load_sem.at[0])
    load.start()
    load.wait()

    def contract(b, c2, target, kind):
        part = jnp.concatenate(
            [
                hidden[b, pl.ds(pl.multiple_of((2 * y2 + c2) * own_rows, HALO), own_rows), :]
                for y2 in range(2)
            ]
        )

        def columns(n, carry):
            span = pl.ds(pl.multiple_of(n * down_columns, LANES), down_columns)
            value = jnp.dot(part, wd_buf[n], preferred_element_type=jnp.float32).astype(kind)
            target[2 * b, :, span] = value[:own_rows]
            target[2 * b + 1, :, span] = value[own_rows:]
            return carry

        lax.fori_loop(0, shards, columns, 0)

    partner = me.at(c=1 - me.c)
    to_y, to_z = me.at(y=1 - me.y), me.at(z=me.mate)
    low, high = slice(0, cut), slice(cut, own_rows)
    yo = 1 - me.y

    def to_partner(index):
        return remote(
            stage.at[index], from_c.at[index], c_send.at[index], c_recv.at[index], partner
        )

    def summed(b, y2, part):
        return own[2 * b + y2, part, :] + from_c[2 * b + y2, part, :].astype(jnp.float32)

    def first_step(k, b, y2, part, device):
        send_a[k] = summed(b, y2, part).astype(jnp.bfloat16)
        net.start(remote(send_a.at[k], from_a.at[k], a_send.at[k], a_recv.at[k], device))

    for b in range(2):
        contract(b, 1 - me.c, stage, jnp.bfloat16)
        for index in (2 * b, 2 * b + 1):
            net.start(to_partner(index))
        if b == 0:
            contract(0, me.c, own, jnp.float32)
    for index in range(2):
        to_partner(index).wait_recv()
    first_step(0, 0, yo, low, to_y)
    first_step(1, 0, yo, high, to_z)
    first_step(3, 0, me.y, high, to_z)
    contract(1, me.c, own, jnp.float32)
    for index in range(2, 4):
        to_partner(index).wait_recv()
    first_step(2, 1, yo, low, to_y)

    def wait_a(k, device):
        remote(send_a.at[k], from_a.at[k], a_send.at[k], a_recv.at[k], device).wait_recv()

    wait_a(0, to_y)
    send_b[0] = (summed(0, me.y, low) + from_a[0].astype(jnp.float32)).astype(jnp.bfloat16)
    net.start(remote(send_b.at[0], from_b.at[0], b_send.at[0], b_recv.at[0], to_z))
    wait_a(1, to_z)
    send_b[1] = (summed(1, yo, high) + from_a[1].astype(jnp.float32)).astype(jnp.bfloat16)
    net.start(remote(send_b.at[1], from_b.at[1], b_send.at[1], b_recv.at[1], to_y))
    wait_a(2, to_y)
    wait_a(3, to_z)
    for k, (part, device) in enumerate(((low, to_z), (high, to_y))):
        remote(send_b.at[k], from_b.at[k], b_send.at[k], b_recv.at[k], device).wait_recv()
        ffn = (
            summed(1, me.y, part)
            + from_a[2 + k].astype(jnp.float32)
            + from_b[k].astype(jnp.float32)
        )
        values = residual_scale * mixed[part, :].astype(jnp.float32) + ffn
        out[part, :] = norm_rows(values, gain[...]).astype(jnp.bfloat16)
    net.drain()


def tail(hidden, wd, mixed, gain):
    own_rows, features = mixed.shape
    cut = own_rows // 2
    bf16, f32 = jnp.bfloat16, jnp.float32
    dma = pltpu.SemaphoreType.DMA
    anywhere = pl.BlockSpec(memory_space=pl.ANY)
    vmem = pl.BlockSpec(memory_space=pltpu.VMEM)
    return pl.pallas_call(
        tail_kernel,
        out_shape=jax.ShapeDtypeStruct((own_rows, features), bf16),
        in_specs=[vmem, anywhere, vmem, vmem],
        out_specs=vmem,
        scratch_shapes=[
            pltpu.VMEM(wd.shape[1:], bf16),
            pltpu.VMEM((4, own_rows, features), f32),
            pltpu.VMEM((4, own_rows, features), bf16),
            pltpu.VMEM((4, own_rows, features), bf16),
            pltpu.VMEM((4, cut, features), bf16),
            pltpu.VMEM((4, cut, features), bf16),
            pltpu.VMEM((2, cut, features), bf16),
            pltpu.VMEM((2, cut, features), bf16),
            dma((1,)), dma((4,)), dma((4,)), dma((4,)), dma((4,)), dma((2,)), dma((2,)),
        ],
        compiler_params=pltpu.CompilerParams(
            has_side_effects=True, vmem_limit_bytes=62 * 1024 * 1024
        ),
        name="tail",
    )(hidden, wd, mixed, gain)


def relayed(
    query_small, key_small, value_small, gates_small,
    query_large, key_large, value_large, gates_large,
    residual, mixer_small, mixer_large, mix_gain,
    value_weight, gate_weight, value_taps, gate_taps, down_weight, final_gain,
):
    rows = query_small.shape[0]
    small, large = gates_small.T, gates_large.T
    blank = jnp.zeros((5, rows), jnp.float32)
    gate_rows = jnp.stack(
        [jnp.concatenate([small[2 * h : 2 * h + 2], large[h : h + 1], blank]) for h in range(2)]
    )
    _, _, wd, _, mixed, hidden = front(
        query_small, query_large, key_small, key_large, value_small, value_large, gate_rows,
        mixer_small, mixer_large, value_weight, gate_weight, down_weight,
        residual, mix_gain[None], value_taps, gate_taps,
    )
    return tail(hidden, wd, mixed, final_gain[None])


def solution(mesh):
    in_specs = (
        P("sp", "tp"),
        P("sp", "tp"),
        P("sp", "tp"),
        P("sp", "tp"),
        P("sp", "tp"),
        P("sp", "tp"),
        P("sp", "tp"),
        P("sp", "tp"),
        P(("sp", "tp"), None),
        P("tp", None),
        P("tp", None),
        P(),
        P("sp", "tp"),
        P("sp", "tp"),
        P(None, "tp"),
        P(None, "tp"),
        P("tp", "sp"),
        P(),
    )
    out_specs = P(("sp", "tp"), None)
    sp_count, tp_count = mesh.shape["sp"], mesh.shape["tp"]

    def step(*arrays):
        if fits(sp_count, tp_count, arrays):
            return relayed(*arrays)
        return per_device(*arrays)

    return jax.shard_map(
        step, mesh=mesh, in_specs=in_specs, out_specs=out_specs, check_vma=False
    )
```

```python
import jax
import jax.numpy as jnp
from jax import lax
from jax.experimental import pallas as pl
from jax.experimental.pallas import tpu as pltpu
from jax.sharding import PartitionSpec as P


DS = 64
DL = 128


residual_scale = 2.0**0.5
epsilon = 1e-05


def passed_along(value, axis, steps):
    count = lax.axis_size(axis)
    first, last = (max(0, -steps), min(count, count - steps))
    return lax.ppermute(value, axis, [(source, source + steps) for source in range(first, last)])


def rotated(value, axis, steps):
    count = lax.axis_size(axis)
    return lax.ppermute(value, axis, [(s, (s + steps) % count) for s in range(count)])


def swapped(value, axis):
    return lax.ppermute(value, axis, [(s, s ^ 1) for s in range(lax.axis_size(axis))])


def norm_rows(values, gain):
    center = jnp.mean(values, axis=-1, keepdims=True)
    spread = jnp.mean(jnp.square(values - center), axis=-1, keepdims=True)
    return (values - center) * lax.rsqrt(spread + epsilon) * gain


def attend_body(small_count, diagonal, *refs):
    if diagonal:
        q_ref, k_ref, v_ref, gk_ref, gq_ref, peak_out, sum_out, acc_out = refs
    else:
        valid_ref, q_ref, k_ref, v_ref, gk_ref, gq_ref = refs[:6]
        peak_in, sum_in, acc_in, peak_out, sum_out, acc_out = refs[6:]
    head = pl.program_id(0)
    scale = jnp.where(head < small_count, DS ** (-0.5), DL ** (-0.5)).astype(jnp.float32)

    def logits():
        scores = lax.dot_general(
            q_ref[0], k_ref[...], (((1,), (1,)), ((), ())), preferred_element_type=jnp.float32
        )
        return scores * scale + (gq_ref[0] - gk_ref[0])

    if diagonal:
        scores = logits()
        query_rows = pl.program_id(1) * scores.shape[0]
        allowed = query_rows + lax.broadcasted_iota(
            jnp.int32, scores.shape, 0
        ) >= lax.broadcasted_iota(jnp.int32, scores.shape, 1)
        scores = jnp.where(allowed, scores, -jnp.inf)
        peak = jnp.max(scores, axis=-1, keepdims=True)
        weights = jnp.exp(scores - peak)
        peak_out[0] = peak
        sum_out[0] = jnp.sum(weights, axis=-1, keepdims=True)
        acc_out[0] = jnp.dot(
            weights.astype(jnp.bfloat16), v_ref[...], preferred_element_type=jnp.float32
        )
        return

    @pl.when(valid_ref[0] > 0)
    def _():
        scores = logits()
        peak = jnp.maximum(peak_in[0], jnp.max(scores, axis=-1, keepdims=True))
        factor = jnp.exp(peak_in[0] - peak)
        weights = jnp.exp(scores - peak)
        peak_out[0] = peak
        sum_out[0] = sum_in[0] * factor + jnp.sum(weights, axis=-1, keepdims=True)
        acc_out[0] = acc_in[0] * factor + jnp.dot(
            weights.astype(jnp.bfloat16), v_ref[...], preferred_element_type=jnp.float32
        )

    @pl.when(valid_ref[0] <= 0)
    def _():
        peak_out[0] = peak_in[0]
        sum_out[0] = sum_in[0]
        acc_out[0] = acc_in[0]


def attend(q_heads, key_value, key_gates, query_gates, small_count, state, valid):
    heads, rows, width = q_heads.shape
    per_small = width // DS
    groups = key_value.shape[1] // (2 * width)
    block = rows // 3 if rows % 3 == 0 and (rows // 3) % 128 == 0 else rows
    diagonal = state is None
    small_groups = small_count // per_small

    def group(h):
        return jnp.where(h < small_count, h // per_small, h - small_count + small_groups)

    per_query = pl.BlockSpec((1, block, 1), lambda h, i: (h, i, 0))
    wide = pl.BlockSpec((1, block, width), lambda h, i: (h, i, 0))
    in_specs = [
        wide,
        pl.BlockSpec((rows, width), lambda h, i: (0, group(h))),
        pl.BlockSpec((rows, width), lambda h, i: (0, groups + group(h))),
        pl.BlockSpec((1, 1, rows), lambda h, i: (h, 0, 0)),
        per_query,
    ]
    operands = [q_heads, key_value, key_value, key_gates[:, None, :], query_gates[:, :, None]]
    aliases = {}
    if not diagonal:
        in_specs = [pl.BlockSpec(memory_space=pltpu.SMEM)] + in_specs + [per_query, per_query, wide]
        operands = [valid] + operands + list(state)
        aliases = {6: 0, 7: 1, 8: 2}
    column = jax.ShapeDtypeStruct((heads, rows, 1), jnp.float32)

    def kernel(*refs):
        attend_body(small_count, diagonal, *refs)

    return pl.pallas_call(
        kernel,
        grid=(heads, rows // block),
        in_specs=in_specs,
        out_specs=[per_query, per_query, wide],
        out_shape=[column, column, jax.ShapeDtypeStruct((heads, rows, width), jnp.float32)],
        input_output_aliases=aliases,
        cost_estimate=pl.CostEstimate(
            flops=heads * rows * rows * width * 4,
            bytes_accessed=heads * rows * width * 12,
            transcendentals=heads * rows * rows,
        ),
        compiler_params=pltpu.CompilerParams(
            dimension_semantics=("arbitrary", "arbitrary"), vmem_limit_bytes=56 * 1024 * 1024
        ),
    )(*operands)


def per_device(
    query_small,
    key_small,
    value_small,
    gates_small,
    query_large,
    key_large,
    value_large,
    gates_large,
    residual,
    mixer_small,
    mixer_large,
    mix_gain,
    value_weight,
    gate_weight,
    value_taps,
    gate_taps,
    down_weight,
    final_gain,
):
    shard_rows = query_small.shape[0]
    sp_index = lax.axis_index("sp")
    tp_index = lax.axis_index("tp")
    tensor_parts = lax.axis_size("tp")
    sp_count = lax.axis_size("sp")
    splits = all(
        count % 2 == 0 and count * size % (2 * DL) == 0
        for count, size in ((gates_small.shape[1], DS), (gates_large.shape[1], DL))
    )
    team = 2 if splits and sp_count % 2 == 0 else 1
    pair_count = sp_count // team
    pair, side = sp_index // team, sp_index % team
    half_small = query_small.shape[1] // team
    small_count = gates_small.shape[1] // team
    large_count = gates_large.shape[1] // team

    def half(array, which):
        width = array.shape[1] // team
        return lax.dynamic_slice_in_dim(array, which * width, width, 1)

    def halves(parts, which):
        return jnp.concatenate([half(a, which) for a in parts], axis=1)

    def exchanged(parts):
        if team == 1:
            return jnp.concatenate(parts, axis=1)
        return in_order(halves(parts, side), swapped(halves(parts, 1 - side), "sp"), 0)

    def in_order(own, other, axis):
        return jnp.where(
            side == 0,
            jnp.concatenate([own, other], axis=axis),
            jnp.concatenate([other, own], axis=axis),
        )

    gate_parts = (gates_small, gates_large)
    key_value = exchanged((key_small, key_large, value_small, value_large))
    if team == 1:
        own_gates = jnp.concatenate(gate_parts, axis=1).T
    else:
        own_gates = in_order(
            halves(gate_parts, side).T, swapped(halves(gate_parts, 1 - side).T, "sp"), 1
        )
    queries = exchanged((query_small, query_large))

    width = DL
    per_small = width // DS
    lane_head = jnp.arange(width) // DS
    q_heads = []
    for h in range(small_count):
        columns = queries[:, (h // per_small) * width : (h // per_small + 1) * width]
        q_heads.append(jnp.where(lane_head == h % per_small, columns, 0).astype(jnp.bfloat16))
    for h in range(large_count):
        q_heads.append(queries[:, half_small + h * width : half_small + (h + 1) * width])
    q_heads = jnp.stack(q_heads)

    mixers = jnp.concatenate([mixer_small, mixer_large], axis=0)
    mixer_of = [mixers]
    for s in range(1, tensor_parts):
        mixer_of.append(rotated(mixers, "tp", -s))
    full_value = lax.all_gather(value_weight, "sp", axis=0, tiled=True)
    full_gate = lax.all_gather(gate_weight, "sp", axis=0, tiled=True)
    down_pieces = down_parts(down_weight)

    arriving, gates_arriving = [key_value], [own_gates]
    for step in range(1, pair_count):
        gates_arriving.append(passed_along(own_gates, "sp", step * team))
        arriving.append(passed_along(arriving[-1], "sp", team))
    state = attend(q_heads, key_value, own_gates, own_gates, small_count, None, None)
    for step in range(1, pair_count):
        valid = (pair >= step).astype(jnp.int32).reshape(1)
        state = attend(
            q_heads, arriving[step], gates_arriving[step], own_gates, small_count, state, valid
        )
    head_out = (state[2] / state[1]).astype(jnp.bfloat16)
    columns = []
    for g in range(small_count // per_small):
        merged = head_out[g * per_small]
        for h in range(1, per_small):
            merged = jnp.where(lane_head == h, head_out[g * per_small + h], merged)
        columns.append(merged)
    for h in range(large_count):
        columns.append(head_out[small_count + h])
    attended = jnp.concatenate(columns, axis=1)
    joined = attended
    if team == 2:
        own = lax.dynamic_slice_in_dim(attended, side * shard_rows, shard_rows, 0)
        other = swapped(
            lax.dynamic_slice_in_dim(attended, (1 - side) * shard_rows, shard_rows, 0), "sp"
        )
        joined = jnp.concatenate(
            [
                in_order(own[:, :half_small], other[:, :half_small], 1),
                in_order(own[:, half_small:], other[:, half_small:], 1),
            ],
            axis=1,
        )
    own_rows = shard_rows // tensor_parts
    arrived = lax.all_to_all(joined, "tp", split_axis=0, concat_axis=1, tiled=True)
    mix = jnp.zeros((own_rows, mixers.shape[1]), jnp.float32)
    for s in range(tensor_parts):
        source = (tp_index + s) % tensor_parts
        mix = mix + jnp.dot(
            lax.dynamic_slice_in_dim(arrived, source * joined.shape[1], joined.shape[1], 1),
            mixer_of[s],
            preferred_element_type=jnp.float32,
        )
    mixed = norm_rows(residual_scale * residual.astype(jnp.float32) + mix, mix_gain).astype(
        jnp.bfloat16
    )
    block_input = jnp.zeros((shard_rows, mixed.shape[1]), jnp.bfloat16)
    for s in range(tensor_parts):
        piece = mixed if s == 0 else rotated(mixed, "tp", -s)
        source = (tp_index + s) % tensor_parts
        block_input = lax.dynamic_update_slice_in_dim(block_input, piece, source * own_rows, 0)

    up_value = jnp.dot(block_input, full_value, preferred_element_type=jnp.float32).astype(
        jnp.bfloat16
    )
    up_gate = jnp.dot(block_input, full_gate, preferred_element_type=jnp.float32).astype(
        jnp.bfloat16
    )
    down_base, up_value = lax.optimization_barrier((down_weight, up_value))
    full_down = assembled(down_base, down_pieces)
    hidden_width = up_value.shape[1]
    trailing = jnp.concatenate([up_value[-2:], up_gate[-2:]], axis=1)
    earlier = passed_along(trailing, "sp", 1)
    padded_value = jnp.concatenate([earlier[:, :hidden_width], up_value], axis=0).astype(
        jnp.float32
    )
    padded_gate = jnp.concatenate([earlier[:, hidden_width:], up_gate], axis=0).astype(jnp.float32)
    filt_value = (
        value_taps[0] * padded_value[:-2]
        + value_taps[1] * padded_value[1:-1]
        + value_taps[2] * padded_value[2:]
    )
    filt_gate = (
        gate_taps[0] * padded_gate[:-2]
        + gate_taps[1] * padded_gate[1:-1]
        + gate_taps[2] * padded_gate[2:]
    )
    hidden = (jax.nn.silu(filt_gate) * filt_value).astype(jnp.bfloat16)

    def ffn_rows(s):
        target = (tp_index + s) % tensor_parts
        part = lax.dynamic_slice_in_dim(hidden, target * own_rows, own_rows, 0)
        return jnp.dot(part, full_down, preferred_element_type=jnp.float32)

    order = [tensor_parts // 2] + [s for s in range(1, tensor_parts) if s != tensor_parts // 2]
    received = [rotated(ffn_rows(s).astype(jnp.bfloat16), "tp", s) for s in order]
    ffn = ffn_rows(0)
    for part in received:
        ffn = ffn + part.astype(jnp.float32)
    return norm_rows(residual_scale * mixed.astype(jnp.float32) + ffn, final_gain).astype(
        jnp.bfloat16
    )


def down_parts(down_weight):
    pieces = []
    for s in range(1, lax.axis_size("sp")):
        pieces.append(rotated(down_weight, "sp", -s))
    return pieces


def assembled(own, pieces):
    count = lax.axis_size("sp")
    width = own.shape[1]
    index = lax.axis_index("sp")
    full = jnp.zeros((own.shape[0], count * width), own.dtype)
    for s, piece in enumerate([own] + pieces):
        full = lax.dynamic_update_slice_in_dim(full, piece, ((index + s) % count) * width, 1)
    return full


MESH = pl.DeviceIdType.MESH
LANES = 128
HALO = 16


def fits(sp_count, tp_count, arrays):
    query, gates_small, gates_large = arrays[0], arrays[3], arrays[7]
    query_large, value_weight = arrays[4], arrays[12]
    rows = query.shape[0]
    own = rows // tp_count
    return (
        tp_count == 4
        and sp_count % 4 == 0
        and sp_count >= 8
        and query.shape[1] == 2 * LANES
        and query_large.shape[1] == 2 * LANES
        and gates_small.shape[1] == 2 * LANES // DS
        and gates_large.shape[1] == 2
        and rows % (3 * LANES) == 0
        and own % (2 * HALO) == 0
        and value_weight.shape[1] % LANES == 0
        and value_weight.shape[0] % HALO == 0
        and 2 * (rows + HALO) <= 16 * LANES
        and (sp_count - 1) * value_weight.shape[0] >= half_width(value_weight.shape[1])
        and half_width(value_weight.shape[1]) >= arrays[16].shape[1]
    )


def half_width(columns):
    return -(-columns // (2 * LANES)) * LANES


class Place:
    def __init__(self):
        self.count = lax.axis_size("sp")
        self.nz = self.count // 2
        self.sp = lax.axis_index("sp")
        self.tp = lax.axis_index("tp")
        self.z, self.x = self.sp // 2, self.sp % 2
        self.y, self.c = self.tp // 2, self.tp % 2
        self.parity = self.z % 2
        self.mate = self.z + 1 - 2 * self.parity

    def at(self, z=None, x=None, y=None, c=None):
        z = self.z if z is None else z
        x = self.x if x is None else x
        y = self.y if y is None else y
        c = self.c if c is None else c
        return (z * 2 + x, y * 2 + c)


class Traffic:
    def __init__(self):
        self.sent = []

    def start(self, copy, when=None):
        guarded(when, copy.start)
        self.sent.append((copy, when))

    def drain(self):
        for copy, when in self.sent:
            guarded(when, copy.wait_send)


def guarded(when, action):
    if when is None:
        action()
    else:

        @pl.when(when)
        def _():
            action()


def remote(source, target, send, receive, device):
    return pltpu.make_async_remote_copy(
        src_ref=source,
        dst_ref=target,
        send_sem=send,
        recv_sem=receive,
        device_id=device,
        device_id_type=MESH,
    )


def front_kernel(
    qs, ql, ks, kl, vs, vl, gt, ms, ml, wv, wg, wd, res, gain, tv, tg,
    o_wv, o_wg, o_wd, o_rows, o_mixed, o_hidden,
    wv_buf, wg_buf, uv, ug, hidden, load_sem,
    q_last, gq_last, peak_last, total_last, acc_last, o_part, marks, q_send, q_recv, p_send, p_recv,
    q_buf, kv, gk, gq, peak, total, acc, o_buf, arrived, mixers, y_buf, zero,
    local_sem, x_send, x_recv, kv_send, kv_recv, g_send, g_recv,
    w_up, w_dn, w_zr, w_xs, w_xr, b_sem, m_local, m_send, m_recv,
    o_send, o_recv, a_send, a_recv, h_send, h_recv, a_local,
):
    me = Place()
    net = Traffic()
    nz, z, x, sp, tp = me.nz, me.z, me.x, me.sp, me.tp
    rows = qs.shape[0]
    own_rows = rows // 4
    other = 1 - x
    mine = pl.ds(pl.multiple_of(x * rows, LANES), rows)
    theirs = pl.ds(pl.multiple_of(other * rows, LANES), rows)
    own_lanes = pl.ds(pl.multiple_of(x * LANES, LANES), LANES)
    other_lanes = pl.ds(pl.multiple_of(other * LANES, LANES), LANES)
    weights = ((wv, o_wv), (wg, o_wg), (wd, o_wd))
    depth = wv.shape[0]
    full_width = wv.shape[1]
    width = half_width(full_width)

    def parts(which):
        return (
            (qs, q_buf.at[which, 0:LANES]),
            (ql, q_buf.at[which, LANES : 2 * LANES]),
            (ks, kv.at[z, which, 0:LANES]),
            (kl, kv.at[z, which, LANES : 2 * LANES]),
            (vs, kv.at[z, which, 2 * LANES : 3 * LANES]),
            (vl, kv.at[z, which, 3 * LANES : 4 * LANES]),
        )

    locals_ = []
    for i, (source, target) in enumerate(parts(mine)):
        net.start(
            remote(source.at[:, other_lanes], target, x_send.at[i], x_recv.at[i], me.at(x=other))
        )
        locals_.append(pltpu.make_async_copy(source.at[:, own_lanes], target, local_sem.at[i]))
    net.start(
        remote(gt.at[other], gk.at[z, :, mine], x_send.at[6], x_recv.at[6], me.at(x=other))
    )
    locals_.append(pltpu.make_async_copy(gt.at[x], gk.at[z, :, mine], local_sem.at[6]))
    for copy in locals_:
        copy.start()

    mixer_rows = 4 * LANES
    mixer_locals = []
    for h in range(2):
        for k, source in enumerate((ms, ml)):
            row = tp * mixer_rows + (2 * h + k) * LANES
            mixer_locals.append(
                pltpu.make_async_copy(
                    source.at[h * LANES : (h + 1) * LANES],
                    mixers.at[pl.ds(row, LANES)],
                    m_local.at[2 * h + k],
                )
            )
    for copy in mixer_locals:
        copy.start()

    def mixer_slot(t):
        return mixers.at[pl.ds(t * mixer_rows, mixer_rows)]

    def half_of(w, half):
        offset = pl.multiple_of(half * (full_width - width), LANES)
        source = weights[w][0]
        if w == 2:
            return source.at[pl.ds(offset, width), :]
        return source.at[:, pl.ds(offset, width)]

    def slot(w, which, zs, xs):
        shard = zs * 2 + xs
        if w == 2:
            return weights[w][1].at[which, shard]
        return weights[w][1].at[which, pl.ds(shard * depth, depth), :]

    def origin(w, which, zs, own):
        if not own:
            return slot(w, which, zs, x)
        return half_of(w, me.parity if which == 0 else 1 - me.parity)

    def both(a, b):
        return b if a is None else jnp.logical_and(a, b)

    upper, lower = jnp.minimum(z + 1, nz - 1), jnp.maximum(z - 1, 0)

    def go_up(w, e, zs, own, when=None):
        net.start(
            remote(
                origin(w, 1 - e, zs, own), slot(w, e, zs, x),
                w_up.at[w, e, zs], w_zr.at[w, e, zs], me.at(z=upper),
            ),
            both(when, z + 1 + e < nz),
        )

    def go_down(w, e, zs, own, when=None):
        net.start(
            remote(
                origin(w, 1 - e, zs, own), slot(w, e, zs, x),
                w_dn.at[w, e, zs], w_zr.at[w, e, zs], me.at(z=lower),
            ),
            both(when, z - 1 - e >= 0),
        )

    def own_up(w, when=None):
        go_up(w, 1, z, True, when)
        go_up(w, 0, z, True, when)

    def own_down(w, when=None):
        go_down(w, 1, z, True, when)
        go_down(w, 0, z, True, when)

    def send_across(w, zs, own, when=None):
        net.start(
            remote(
                origin(w, 0, zs, own), slot(w, 0, zs, x),
                w_xs.at[w, zs], w_xr.at[w, zs], me.at(x=other),
            ),
            when,
        )

    def landed(w, which, zs, when):
        copy = remote(
            slot(w, which, zs, x), slot(w, which, zs, x),
            w_up.at[w, which, zs], w_zr.at[w, which, zs], me.at(x=other),
        )
        guarded(when, copy.wait_recv)

    def up_pass(w, r, when=None):
        if r < nz:
            zs, here_ = jnp.maximum(z - r, 0), both(when, jnp.logical_and(z - r >= 0, z + 1 < nz))
            landed(w, 1, zs, here_)
            go_up(w, 0, zs, False, here_)

    def up_keep(w, r, when=None):
        if r < nz:
            zs, here_ = jnp.maximum(z - r, 0), both(when, z - r >= 0)
            landed(w, 0, zs, here_)
            go_up(w, 1, zs, False, here_)
            send_across(w, zs, False, here_)

    def down_pass(w, r, when=None):
        if r < nz:
            zs, here_ = jnp.minimum(z + r, nz - 1), both(when, jnp.logical_and(z + r < nz, z >= 1))
            landed(w, 1, zs, here_)
            go_down(w, 0, zs, False, here_)

    def down_keep(w, r, when=None):
        if r < nz:
            zs, here_ = jnp.minimum(z + r, nz - 1), both(when, z + r < nz)
            landed(w, 0, zs, here_)
            go_down(w, 1, zs, False, here_)
            send_across(w, zs, False, here_)

    def piece(j, p):
        span = mine if p == 0 else theirs
        return kv.at[j, span, :], gk.at[j, :, span]

    def pass_on(j, p, when):
        data, gate = piece(j, p)
        above = me.at(z=jnp.minimum(z + 1, nz - 1))
        net.start(remote(data, data, kv_send.at[j, p], kv_recv.at[j, p], above), when)
        net.start(remote(gate, gate, g_send.at[j, p], g_recv.at[j, p], above), when)

    def take(j, p, when):
        data, gate = piece(j, p)
        above = me.at(z=jnp.minimum(z + 1, nz - 1))
        guarded(when, remote(data, data, kv_send.at[j, p], kv_recv.at[j, p], above).wait_recv)
        guarded(when, remote(gate, gate, g_send.at[j, p], g_recv.at[j, p], above).wait_recv)

    def relay(r, p):
        if r > nz - 2:
            return
        j = jnp.maximum(z - r, 0)
        take(j, p, z - r >= 0)
        if r < nz - 2:
            pass_on(j, p, jnp.logical_and(z - r >= 0, z + 1 < nz))

    block = 2 * rows // 3
    count = 3

    def head_facts(h):
        lanes = lax.broadcasted_iota(jnp.int32, (1, LANES), 1)
        low = jnp.where(h == 1, DS, 0)
        high = jnp.where(h == 0, DS, LANES)
        keep = jnp.logical_and(lanes >= low, lanes < high)
        column = pl.multiple_of(jnp.where(h == 2, LANES, 0), LANES)
        scale = jnp.where(h == 2, DL ** (-0.5), DS ** (-0.5)).astype(jnp.float32)
        return keep, column, scale

    def query_part(h, span, queries=None):
        keep, column, scale = head_facts(h)
        q = (q_buf if queries is None else queries)[span, pl.ds(column, LANES)]
        return jnp.where(keep, q, jnp.zeros_like(q)), column, scale

    def shifted_scores(q, j, h, column, scale, keys):
        k = kv[j, keys, pl.ds(column, LANES)]
        scores = lax.dot_general(
            q, k, (((1,), (1,)), ((), ())), preferred_element_type=jnp.float32
        )
        return scores * scale - gk[j, pl.ds(h, 1), keys]

    def weighted(weights_, j, column, keys):
        v = kv[j, keys, pl.ds(column + 2 * LANES, LANES)]
        return jnp.dot(weights_.astype(jnp.bfloat16), v, preferred_element_type=jnp.float32)

    def attend_own():
        def head(h, carry):
            for i in range(count):
                span = pl.ds(i * block, block)
                keys = pl.ds(0, (i + 1) * block)
                q, column, scale = query_part(h, span)
                scores = shifted_scores(q, z, h, column, scale, keys)
                allowed = i * block + lax.broadcasted_iota(
                    jnp.int32, scores.shape, 0
                ) >= lax.broadcasted_iota(jnp.int32, scores.shape, 1)
                scores = jnp.where(allowed, scores, -jnp.inf)
                gate = gq[h, span, :]
                top = jnp.max(scores, axis=-1, keepdims=True) + gate
                weights_ = jnp.exp(scores + (gate - top))
                peak[h, span, :] = top
                total[h, span, :] = jnp.sum(weights_, axis=-1, keepdims=True)
                acc[h, span, :] = weighted(weights_, z, column, keys)
            return carry

        lax.fori_loop(0, 3, head, 0)

    own_state = (q_buf, gq, peak, total, acc)
    last_state = (q_last, gq_last, peak_last, total_last, acc_last)

    def attend_earlier(j, state):
        queries, gates, peaks, totals, sums = state

        def part(i, carry):
            h, b = i // count, i % count
            span = pl.ds(pl.multiple_of(b * block, LANES), block)
            keys = pl.ds(0, 2 * rows)
            q, column, scale = query_part(h, span, queries)
            scores = shifted_scores(q, j, h, column, scale, keys)
            gate = gates[h, span, :]
            before = peaks[h, span, :]
            top = jnp.maximum(before, jnp.max(scores, axis=-1, keepdims=True) + gate)
            factor = jnp.exp(before - top)
            weights_ = jnp.exp(scores + (gate - top))
            peaks[h, span, :] = top
            totals[h, span, :] = totals[h, span, :] * factor + jnp.sum(
                weights_, axis=-1, keepdims=True
            )
            sums[h, span, :] = sums[h, span, :] * factor + weighted(weights_, j, column, keys)
            return carry

        lax.fori_loop(0, 3 * count, part, 0)

    is_last, is_helper = z == nz - 1, z == nz - 2
    helper, ahead = me.at(z=jnp.maximum(z - 1, 0)), me.at(z=jnp.minimum(z + 1, nz - 1))

    def lend(p, send):
        span = mine if p == 0 else theirs
        gate = gk.at[nz - 1, :, span]
        for k, (source, target) in enumerate(
            ((q_buf.at[span, :], q_last.at[span, :]), (gate, gate))
        ):
            copy = remote(source, target, q_send.at[p, k], q_recv.at[p, k], helper)
            if send:
                net.start(copy, is_last)
            else:
                guarded(is_helper, copy.wait_recv)

    def part_copies():
        return (
            remote(o_part, o_part, p_send.at[0], p_recv.at[0], ahead),
            remote(marks, marks, p_send.at[1], p_recv.at[1], ahead),
        )

    def finished(totals, sums):
        first_head = sums[0] / totals[0]
        keep, _, _ = head_facts(1)
        return jnp.where(keep, sums[1] / totals[1], first_head), sums[2] / totals[2]

    def give_back():
        for n, pair in enumerate(finished(total_last, acc_last)):
            o_part[:, n * LANES : (n + 1) * LANES] = pair.astype(jnp.bfloat16)
        columns = [peak_last[h] for h in range(3)] + [total_last[h] for h in range(3)]
        lanes = lax.broadcasted_iota(jnp.int32, (1, 8), 1)
        table = jnp.zeros((2 * rows, 8), jnp.float32)
        for n, column in enumerate(columns):
            table = jnp.where(lanes == n, column, table)
        marks[...] = jnp.transpose(table)

    def merge():
        table = jnp.transpose(marks[...])
        _, _, _ = head_facts(1)
        for h in range(3):
            lane = 0 if h < 2 else LANES
            top = jnp.maximum(peak[h], table[:, h : h + 1])
            mine_, other_ = jnp.exp(peak[h] - top), jnp.exp(table[:, h : h + 1] - top)
            other_ = other_ * table[:, 3 + h : 4 + h]
            acc[h] = acc[h] * mine_ + o_part[:, lane : lane + LANES].astype(jnp.float32) * other_
            total[h] = total[h] * mine_ + other_

    ups = (0, 1)
    at_last, low_block = z == nz - 1, z <= 1
    at_one, not_one = z == 1, z != 1
    for w in ups:
        own_down(w, z + 1 < nz)
    for copy in locals_:
        copy.wait()
    pass_on(z, 0, z + 1 < nz)
    lend(0, True)
    for copy in mixer_locals:
        copy.wait()
    mixer_sends = [
        remote(mixer_slot(tp), mixer_slot(tp), m_send.at[0], m_recv.at[0], me.at(y=1 - me.y)),
        remote(mixer_slot(tp), mixer_slot(tp), m_send.at[1], m_recv.at[1], me.at(c=1 - me.c)),
    ]
    for copy in mixer_sends:
        copy.start()
    own_copies = []
    for w in range(3):
        if w == 2:
            target = wv_buf.at[depth : depth + width, 0 : wd.shape[1]]
        else:
            target = (wv_buf, wg_buf)[w].at[0:depth, :]
        own_copies.append(
            (
                pltpu.make_async_copy(half_of(w, me.parity), target, b_sem.at[w, 0]),
                pltpu.make_async_copy(target, slot(w, 0, z, x), b_sem.at[w, 1]),
            )
        )
    for first, _ in own_copies:
        first.start()
    relay(1, 0)
    for i, (source, target) in enumerate(parts(theirs)):
        remote(source.at[:, other_lanes], target, x_send.at[i], x_recv.at[i], me.at(x=other)).wait_recv()
    remote(gt.at[other], gk.at[z, :, theirs], x_send.at[6], x_recv.at[6], me.at(x=other)).wait_recv()
    pass_on(z, 1, z + 1 < nz)
    lend(1, True)
    for w in ups:
        own_down(w, at_last)
    own_down(2)
    for w in ups:
        send_across(w, z, True)
    for first, second in own_copies:
        first.wait()
        second.start()
    columns = jnp.transpose(gk[z])
    for h in range(3):
        gq[h] = columns[:, h : h + 1]
    attend_own()

    ty = (1 - me.y) * 2 + me.c
    from_y = remote(mixer_slot(ty), mixer_slot(ty), m_send.at[2], m_recv.at[0], me.at(c=1 - me.c))
    from_y.wait_recv()
    mixer_sends.append(
        remote(mixer_slot(ty), mixer_slot(ty), m_send.at[2], m_recv.at[2], me.at(c=1 - me.c))
    )
    mixer_sends[2].start()
    for r in range(1, nz):
        relay(r, 1)
        relay(r + 1, 0)
        if r == 1:
            for w in ups:
                own_up(w, low_block)
        if r == 2:
            for w in ups:
                own_up(w, z > 1)
            for w in ups:
                down_pass(w, 1)
                down_keep(w, 1)
            for w in ups:
                up_keep(w, 1, at_one)
            for w in ups:
                up_pass(w, 1, at_one)
            own_up(2, low_block)

        j = jnp.maximum(z - r, 0)
        if r == nz - 2:
            lend(0, False)
            lend(1, False)

            @pl.when(is_helper)
            def _(j=j):
                columns = jnp.transpose(gk[nz - 1])
                for h in range(3):
                    gq_last[h] = columns[:, h : h + 1]
                peak_last[...] = jnp.full_like(peak_last, -jnp.inf)
                total_last[...] = jnp.zeros_like(total_last)
                acc_last[...] = jnp.zeros_like(acc_last)
                attend_earlier(j, last_state)
                give_back()

            for copy in part_copies():
                net.start(copy, is_helper)
        if r < nz - 1:

            @pl.when(z - r >= 0)
            def _(j=j):
                attend_earlier(j, own_state)

    for copy in part_copies():
        guarded(is_last, copy.wait_recv)
    guarded(is_last, merge)
    for n, pair in enumerate(finished(total, acc)):
        o_buf[:, n * LANES : (n + 1) * LANES] = pair.astype(jnp.bfloat16)

    for w in ups:
        up_pass(w, 1, not_one)

    def arrival(t, xs):
        return arrived.at[:, pl.ds(pl.multiple_of((t * 2 + xs) * 2 * LANES, 2 * LANES), 2 * LANES)]

    takes = []
    for k in range(1, 8):
        dx, dy, dc = k // 4, (k // 2) % 2, k % 2
        x2 = x + dx * (1 - 2 * x)
        y2 = me.y + dy * (1 - 2 * me.y)
        c2 = me.c + dc * (1 - 2 * me.c)
        t2 = y2 * 2 + c2
        net.start(
            remote(
                o_buf.at[pl.ds(x2 * rows + t2 * own_rows, own_rows), :], arrival(tp, x),
                o_send.at[k], o_recv.at[k], me.at(x=x2, y=y2, c=c2),
            )
        )
        takes.append(
            remote(
                o_buf.at[pl.ds(0, own_rows), :], arrival(t2, x2),
                o_send.at[k], o_recv.at[k], me.at(x=x2, y=y2, c=c2),
            )
        )
    own_span = pl.ds(pl.multiple_of((tp * 2 + x) * 2 * LANES, 2 * LANES), 2 * LANES)
    arrived[:, own_span] = o_buf[pl.ds(pl.multiple_of(x * rows + tp * own_rows, HALO), own_rows), :]
    for w in ups:
        up_keep(w, 1, not_one)
    for w in ups:
        down_pass(w, 2)
        down_keep(w, 2)
    down_pass(2, 1)
    down_keep(2, 1)
    for w in ups:
        up_pass(w, 2)
    remote(mixer_slot(0), mixer_slot(tp + 1 - 2 * me.c), m_send.at[1], m_recv.at[1], me.at(c=1 - me.c)).wait_recv()
    remote(mixer_slot(0), mixer_slot(ty + 1 - 2 * me.c), m_send.at[2], m_recv.at[2], me.at(c=1 - me.c)).wait_recv()
    for copy in takes:
        copy.wait_recv()

    features = gain.shape[1]
    step = 4 * LANES

    def mix_tile(n, carry):
        span = pl.ds(pl.multiple_of(n * step, step), step)
        y_buf[:, span] = residual_scale * res[:, span].astype(jnp.float32) + jnp.dot(
            arrived[...], mixers[:, span], preferred_element_type=jnp.float32
        )
        return carry

    lax.fori_loop(0, features // step, mix_tile, 0)
    o_mixed[...] = norm_rows(y_buf[...], gain[...]).astype(jnp.bfloat16)
    zero[...] = jnp.zeros_like(zero)

    parity, mate = me.parity, me.mate

    def rows_of(zi, t, part=None):
        base = HALO + t * own_rows
        if part is None:
            return o_rows.at[zi, pl.ds(base, own_rows), :]
        return o_rows.at[zi, pl.ds(base + part * (own_rows // 2), own_rows // 2), :]

    here = rows_of(parity, tp)
    up_y, up_z, up_c = me.at(y=1 - me.y), me.at(z=mate), me.at(c=1 - me.c)
    net.start(remote(o_mixed, here, a_send.at[0], a_recv.at[0], up_z))
    net.start(remote(o_mixed, here, a_send.at[1], a_recv.at[1], up_y))
    net.start(remote(o_mixed, here, a_send.at[2], a_recv.at[2], up_c))
    keep_rows = pltpu.make_async_copy(o_mixed, here, a_local.at[0])
    keep_rows.start()
    following = jnp.minimum(sp + 1, me.count - 1)
    fz = following // 2
    sends_halo = jnp.logical_and(sp + 1 < me.count, tp == 3)
    for k in range(8):
        dz, dy, dc = k // 4, (k // 2) % 2, k % 2
        z2 = fz - fz % 2 + dz
        net.start(
            remote(
                o_mixed.at[own_rows - HALO : own_rows, :],
                o_rows.at[fz % 2, 0:HALO, :],
                h_send.at[k], h_recv.at[fz % 2],
                (z2 * 2 + 1 - x, dy * 2 + dc),
            ),
            sends_halo,
        )
    first_rows = jnp.logical_and(z - parity == 0, x == 0)
    blank = pltpu.make_async_copy(zero, o_rows.at[0, 0:HALO, :], a_local.at[1])
    guarded(first_rows, blank.start)

    for k in range(2, nz):
        for w in ups:
            up_keep(w, k)
            if k > 2:
                down_keep(w, k)
                up_pass(w, k)
                down_pass(w, k)

    p_z, p_y = rows_of(1 - parity, tp), rows_of(parity, ty)
    remote(o_mixed, p_y, a_send.at[1], a_recv.at[1], up_y).wait_recv()
    half = rows_of(parity, ty, 0)
    net.start(remote(half, half, a_send.at[3], a_recv.at[3], up_z))
    net.start(remote(p_y, p_y, a_send.at[5], a_recv.at[5], up_c))
    remote(o_mixed, p_z, a_send.at[0], a_recv.at[0], up_z).wait_recv()
    half = rows_of(1 - parity, tp, 1)
    net.start(remote(half, half, a_send.at[4], a_recv.at[4], up_y))
    net.start(remote(p_z, p_z, a_send.at[6], a_recv.at[6], up_c))
    for k in range(2):
        half = rows_of(1 - parity, ty, k)
        remote(half, half, a_send.at[3 + k], a_recv.at[3 + k], up_c).wait_recv()
        net.start(remote(half, half, a_send.at[7 + k], a_recv.at[7 + k], up_c))

    down_pass(2, 2)
    down_keep(2, 2)
    own_up(2, z > 1)
    send_across(2, z, True)
    up_keep(2, 1, at_one)
    up_pass(2, 1, at_one)

    tc, tyc = tp + 1 - 2 * me.c, ty + 1 - 2 * me.c
    for k, target in (
        (2, rows_of(parity, tc)),
        (5, rows_of(parity, tyc)),
        (6, rows_of(1 - parity, tc)),
        (7, rows_of(1 - parity, tyc, 0)),
        (8, rows_of(1 - parity, tyc, 1)),
    ):
        remote(target, target, a_send.at[k], a_recv.at[k], up_c).wait_recv()
    for i in range(2):
        halo = o_rows.at[i, 0:HALO, :]
        copy = remote(halo, halo, h_send.at[i], h_recv.at[i], up_c)
        guarded((z - parity + i) * 2 + x - 1 >= 0, copy.wait_recv)
    guarded(first_rows, blank.wait)
    keep_rows.wait()
    for _, second in own_copies:
        second.wait()

    def from_across(w):
        for zs in range(nz):
            target = slot(w, 0, zs, other)
            remote(target, target, w_xs.at[w, zs], w_xr.at[w, zs], me.at(x=other)).wait_recv()

    from_across(0)
    from_across(1)

    for copy in mixer_sends:
        copy.wait_send()
    tall = HALO + rows
    held = [mixers.at[b * tall : (b + 1) * tall, :] for b in range(2)]
    loads = [
        pltpu.make_async_copy(o_rows.at[1 - parity], held[0], load_sem.at[0]),
        pltpu.make_async_copy(o_wv.at[0], wv_buf, load_sem.at[1]),
        pltpu.make_async_copy(o_wg.at[0], wg_buf, load_sem.at[2]),
        pltpu.make_async_copy(o_rows.at[parity], held[1], load_sem.at[3]),
    ]
    for copy in loads:
        copy.start()
    tile = 2 * LANES
    offset = parity * (full_width - width)
    repeated = jnp.where(parity == 1, 2 * width - full_width, 0)

    def expand(b, first_tile, end_tile):
        def tile_of(n, carry):
            span = pl.ds(pl.multiple_of(n * tile, tile), tile)
            taps = pl.ds(pl.multiple_of(offset + n * tile, LANES), tile)
            filtered = []
            for buf, weight, tap in ((uv, wv_buf, tv), (ug, wg_buf, tg)):
                up = jnp.dot(held[b][...], weight[:, span], preferred_element_type=jnp.float32)
                buf[...] = up.astype(jnp.bfloat16).astype(jnp.float32)
                filtered.append(
                    tap[0:1, taps] * buf[HALO - 2 : HALO - 2 + rows, :]
                    + tap[1:2, taps] * buf[HALO - 1 : HALO - 1 + rows, :]
                    + tap[2:3, taps] * buf[HALO : HALO + rows, :]
                )
            value, gate = filtered
            result = value * (gate / (1.0 + jnp.exp(-gate)))
            unit = n * tile + lax.broadcasted_iota(jnp.int32, (1, tile), 1)
            result = jnp.where(unit >= repeated, result, 0.0)
            hidden[b, :, span] = result.astype(jnp.bfloat16)
            return carry

        lax.fori_loop(first_tile, end_tile, tile_of, 0)

    outs = [
        pltpu.make_async_copy(hidden.at[b], o_hidden.at[b], load_sem.at[4 + b]) for b in range(2)
    ]
    for copy in loads[:3]:
        copy.wait()
    up_keep(2, 1, not_one)
    up_pass(2, 1, not_one)
    inner = z < nz - 1
    up_pass(2, 2, inner)
    up_keep(2, 2, inner)
    for k in range(3, nz):
        down_pass(2, k)
        down_keep(2, k)
    tiles = width // tile
    expand(0, 0, tiles)
    outs[0].start()
    up_keep(2, 2, at_last)
    loads[3].wait()
    expand(1, 0, tiles - 1)
    for k in range(3, nz):
        up_pass(2, k)
        up_keep(2, k)
    expand(1, tiles - 1, tiles)
    outs[1].start()
    from_across(2)
    for copy in outs:
        copy.wait()
    net.drain()


def front(qs, ql, ks, kl, vs, vl, gt, ms, ml, wv, wg, wd, res, gain, tv, tg):
    count = lax.axis_size("sp")
    nz = count // 2
    rows = qs.shape[0]
    own_rows = rows // 4
    features = gain.shape[1]
    depth, width = wv.shape[0], half_width(wv.shape[1])
    down_columns = wd.shape[1]
    bf16, f32 = jnp.bfloat16, jnp.float32
    dma = pltpu.SemaphoreType.DMA
    anywhere = pl.BlockSpec(memory_space=pl.ANY)
    vmem = pl.BlockSpec(memory_space=pltpu.VMEM)
    return pl.pallas_call(
        front_kernel,
        out_shape=[
            jax.ShapeDtypeStruct((2, count * depth, width), bf16),
            jax.ShapeDtypeStruct((2, count * depth, width), bf16),
            jax.ShapeDtypeStruct((2, count, width, down_columns), bf16),
            jax.ShapeDtypeStruct((2, HALO + rows, features), bf16),
            jax.ShapeDtypeStruct((own_rows, features), bf16),
            jax.ShapeDtypeStruct((2, rows, width), bf16),
        ],
        in_specs=[anywhere] * 12 + [vmem] * 4,
        out_specs=[anywhere] * 4 + [vmem, anywhere],
        scratch_shapes=[
            pltpu.VMEM((count * depth, width), bf16),
            pltpu.VMEM((count * depth, width), bf16),
            pltpu.VMEM((HALO + rows, 2 * LANES), f32),
            pltpu.VMEM((HALO + rows, 2 * LANES), f32),
            pltpu.VMEM((2, rows, width), bf16),
            dma((6,)),
            pltpu.VMEM((2 * rows, 2 * LANES), bf16),
            pltpu.VMEM((3, 2 * rows, 1), f32),
            pltpu.VMEM((3, 2 * rows, 1), f32),
            pltpu.VMEM((3, 2 * rows, 1), f32),
            pltpu.VMEM((3, 2 * rows, LANES), f32),
            pltpu.VMEM((2 * rows, 2 * LANES), bf16),
            pltpu.VMEM((8, 2 * rows), f32),
            dma((2, 2)), dma((2, 2)), dma((2,)), dma((2,)),
            pltpu.VMEM((2 * rows, 2 * LANES), bf16),
            pltpu.VMEM((nz, 2 * rows, 4 * LANES), bf16),
            pltpu.VMEM((nz, 8, 2 * rows), f32),
            pltpu.VMEM((3, 2 * rows, 1), f32),
            pltpu.VMEM((3, 2 * rows, 1), f32),
            pltpu.VMEM((3, 2 * rows, 1), f32),
            pltpu.VMEM((3, 2 * rows, LANES), f32),
            pltpu.VMEM((2 * rows, 2 * LANES), bf16),
            pltpu.VMEM((own_rows, 16 * LANES), bf16),
            pltpu.VMEM((16 * LANES, features), bf16),
            pltpu.VMEM((own_rows, features), f32),
            pltpu.VMEM((HALO, features), bf16),
            dma((7,)), dma((7,)), dma((7,)),
            dma((nz, 2)), dma((nz, 2)), dma((nz, 2)), dma((nz, 2)),
            dma((3, 2, nz)), dma((3, 2, nz)), dma((3, 2, nz)),
            dma((3, nz)), dma((3, nz)),
            dma((3, 2)), dma((4,)), dma((3,)), dma((3,)),
            dma((8,)), dma((8,)), dma((9,)), dma((9,)), dma((8,)), dma((2,)), dma((2,)),
        ],
        compiler_params=pltpu.CompilerParams(
            has_side_effects=True, vmem_limit_bytes=62 * 1024 * 1024
        ),
        name="front",
    )(qs, ql, ks, kl, vs, vl, gt, ms, ml, wv, wg, wd, res, gain, tv, tg)


def tail_kernel(
    hidden, wd, mixed, gain,
    out,
    wd_buf, own, stage, from_c, send_a, from_a, send_b, from_b,
    load_sem, c_send, c_recv, a_send, a_recv, b_send, b_recv,
):
    me = Place()
    net = Traffic()
    own_rows = mixed.shape[0]
    cut = own_rows // 2
    shards, down_columns = wd.shape[1], wd.shape[3]
    load = pltpu.make_async_copy(wd.at[0], wd_buf, load_sem.at[0])
    load.start()
    barrier = pltpu.get_barrier_semaphore()
    for device in (me.at(y=1 - me.y), me.at(z=me.mate), me.at(c=1 - me.c)):
        pl.semaphore_signal(barrier, inc=1, device_id=device, device_id_type=MESH)
    pl.semaphore_wait(barrier, 3)
    load.wait()

    def contract(b, c2, target, kind):
        part = jnp.concatenate(
            [
                hidden[b, pl.ds(pl.multiple_of((2 * y2 + c2) * own_rows, HALO), own_rows), :]
                for y2 in range(2)
            ]
        )

        def columns(n, carry):
            span = pl.ds(pl.multiple_of(n * down_columns, LANES), down_columns)
            value = jnp.dot(part, wd_buf[n], preferred_element_type=jnp.float32).astype(kind)
            target[2 * b, :, span] = value[:own_rows]
            target[2 * b + 1, :, span] = value[own_rows:]
            return carry

        lax.fori_loop(0, shards, columns, 0)

    partner = me.at(c=1 - me.c)
    to_y, to_z = me.at(y=1 - me.y), me.at(z=me.mate)
    low, high = slice(0, cut), slice(cut, own_rows)
    yo = 1 - me.y

    def to_partner(index):
        return remote(
            stage.at[index], from_c.at[index], c_send.at[index], c_recv.at[index], partner
        )

    def summed(b, y2, part):
        return own[2 * b + y2, part, :] + from_c[2 * b + y2, part, :].astype(jnp.float32)

    def first_step(k, b, y2, part, device):
        send_a[k] = summed(b, y2, part).astype(jnp.bfloat16)
        net.start(remote(send_a.at[k], from_a.at[k], a_send.at[k], a_recv.at[k], device))

    for b in range(2):
        contract(b, 1 - me.c, stage, jnp.bfloat16)
        for index in (2 * b, 2 * b + 1):
            net.start(to_partner(index))
        if b == 0:
            contract(0, me.c, own, jnp.float32)
    for index in range(2):
        to_partner(index).wait_recv()
    first_step(0, 0, yo, low, to_y)
    first_step(1, 0, yo, high, to_z)
    first_step(3, 0, me.y, high, to_z)
    contract(1, me.c, own, jnp.float32)
    for index in range(2, 4):
        to_partner(index).wait_recv()
    first_step(2, 1, yo, low, to_y)

    def wait_a(k, device):
        remote(send_a.at[k], from_a.at[k], a_send.at[k], a_recv.at[k], device).wait_recv()

    wait_a(0, to_y)
    send_b[0] = (summed(0, me.y, low) + from_a[0].astype(jnp.float32)).astype(jnp.bfloat16)
    net.start(remote(send_b.at[0], from_b.at[0], b_send.at[0], b_recv.at[0], to_z))
    wait_a(1, to_z)
    send_b[1] = (summed(1, yo, high) + from_a[1].astype(jnp.float32)).astype(jnp.bfloat16)
    net.start(remote(send_b.at[1], from_b.at[1], b_send.at[1], b_recv.at[1], to_y))
    wait_a(2, to_y)
    wait_a(3, to_z)
    for k, (part, device) in enumerate(((low, to_z), (high, to_y))):
        remote(send_b.at[k], from_b.at[k], b_send.at[k], b_recv.at[k], device).wait_recv()
        ffn = (
            summed(1, me.y, part)
            + from_a[2 + k].astype(jnp.float32)
            + from_b[k].astype(jnp.float32)
        )
        values = residual_scale * mixed[part, :].astype(jnp.float32) + ffn
        out[part, :] = norm_rows(values, gain[...]).astype(jnp.bfloat16)
    net.drain()


def tail(hidden, wd, mixed, gain):
    own_rows, features = mixed.shape
    cut = own_rows // 2
    bf16, f32 = jnp.bfloat16, jnp.float32
    dma = pltpu.SemaphoreType.DMA
    anywhere = pl.BlockSpec(memory_space=pl.ANY)
    vmem = pl.BlockSpec(memory_space=pltpu.VMEM)
    return pl.pallas_call(
        tail_kernel,
        out_shape=jax.ShapeDtypeStruct((own_rows, features), bf16),
        in_specs=[vmem, anywhere, vmem, vmem],
        out_specs=vmem,
        scratch_shapes=[
            pltpu.VMEM(wd.shape[1:], bf16),
            pltpu.VMEM((4, own_rows, features), f32),
            pltpu.VMEM((4, own_rows, features), bf16),
            pltpu.VMEM((4, own_rows, features), bf16),
            pltpu.VMEM((4, cut, features), bf16),
            pltpu.VMEM((4, cut, features), bf16),
            pltpu.VMEM((2, cut, features), bf16),
            pltpu.VMEM((2, cut, features), bf16),
            dma((1,)), dma((4,)), dma((4,)), dma((4,)), dma((4,)), dma((2,)), dma((2,)),
        ],
        compiler_params=pltpu.CompilerParams(
            collective_id=0, has_side_effects=True, vmem_limit_bytes=62 * 1024 * 1024
        ),
        name="tail",
    )(hidden, wd, mixed, gain)


def relayed(
    query_small, key_small, value_small, gates_small,
    query_large, key_large, value_large, gates_large,
    residual, mixer_small, mixer_large, mix_gain,
    value_weight, gate_weight, value_taps, gate_taps, down_weight, final_gain,
):
    rows = query_small.shape[0]
    small, large = gates_small.T, gates_large.T
    blank = jnp.zeros((5, rows), jnp.float32)
    gate_rows = jnp.stack(
        [jnp.concatenate([small[2 * h : 2 * h + 2], large[h : h + 1], blank]) for h in range(2)]
    )
    _, _, wd, _, mixed, hidden = front(
        query_small, query_large, key_small, key_large, value_small, value_large, gate_rows,
        mixer_small, mixer_large, value_weight, gate_weight, down_weight,
        residual, mix_gain[None], value_taps, gate_taps,
    )
    return tail(hidden, wd, mixed, final_gain[None])


def solution(mesh):
    in_specs = (
        P("sp", "tp"),
        P("sp", "tp"),
        P("sp", "tp"),
        P("sp", "tp"),
        P("sp", "tp"),
        P("sp", "tp"),
        P("sp", "tp"),
        P("sp", "tp"),
        P(("sp", "tp"), None),
        P("tp", None),
        P("tp", None),
        P(),
        P("sp", "tp"),
        P("sp", "tp"),
        P(None, "tp"),
        P(None, "tp"),
        P("tp", "sp"),
        P(),
    )
    out_specs = P(("sp", "tp"), None)
    sp_count, tp_count = mesh.shape["sp"], mesh.shape["tp"]

    def step(*arrays):
        if fits(sp_count, tp_count, arrays):
            return relayed(*arrays)
        return per_device(*arrays)

    return jax.shard_map(
        step, mesh=mesh, in_specs=in_specs, out_specs=out_specs, check_vma=False
    )
```

```python
import jax
import jax.numpy as jnp
from jax import lax
from jax.experimental import pallas as pl
from jax.experimental.pallas import tpu as pltpu
from jax.sharding import PartitionSpec as P


DS = 64
DL = 128


residual_scale = 2.0**0.5
epsilon = 1e-05


def passed_along(value, axis, steps):
    count = lax.axis_size(axis)
    first, last = (max(0, -steps), min(count, count - steps))
    return lax.ppermute(value, axis, [(source, source + steps) for source in range(first, last)])


def rotated(value, axis, steps):
    count = lax.axis_size(axis)
    return lax.ppermute(value, axis, [(s, (s + steps) % count) for s in range(count)])


def swapped(value, axis):
    return lax.ppermute(value, axis, [(s, s ^ 1) for s in range(lax.axis_size(axis))])


def norm_rows(values, gain):
    center = jnp.mean(values, axis=-1, keepdims=True)
    spread = jnp.mean(jnp.square(values - center), axis=-1, keepdims=True)
    return (values - center) * lax.rsqrt(spread + epsilon) * gain


def attend_body(small_count, diagonal, *refs):
    if diagonal:
        q_ref, k_ref, v_ref, gk_ref, gq_ref, peak_out, sum_out, acc_out = refs
    else:
        valid_ref, q_ref, k_ref, v_ref, gk_ref, gq_ref = refs[:6]
        peak_in, sum_in, acc_in, peak_out, sum_out, acc_out = refs[6:]
    head = pl.program_id(0)
    scale = jnp.where(head < small_count, DS ** (-0.5), DL ** (-0.5)).astype(jnp.float32)

    def logits():
        scores = lax.dot_general(
            q_ref[0], k_ref[...], (((1,), (1,)), ((), ())), preferred_element_type=jnp.float32
        )
        return scores * scale + (gq_ref[0] - gk_ref[0])

    if diagonal:
        scores = logits()
        query_rows = pl.program_id(1) * scores.shape[0]
        allowed = query_rows + lax.broadcasted_iota(
            jnp.int32, scores.shape, 0
        ) >= lax.broadcasted_iota(jnp.int32, scores.shape, 1)
        scores = jnp.where(allowed, scores, -jnp.inf)
        peak = jnp.max(scores, axis=-1, keepdims=True)
        weights = jnp.exp(scores - peak)
        peak_out[0] = peak
        sum_out[0] = jnp.sum(weights, axis=-1, keepdims=True)
        acc_out[0] = jnp.dot(
            weights.astype(jnp.bfloat16), v_ref[...], preferred_element_type=jnp.float32
        )
        return

    @pl.when(valid_ref[0] > 0)
    def _():
        scores = logits()
        peak = jnp.maximum(peak_in[0], jnp.max(scores, axis=-1, keepdims=True))
        factor = jnp.exp(peak_in[0] - peak)
        weights = jnp.exp(scores - peak)
        peak_out[0] = peak
        sum_out[0] = sum_in[0] * factor + jnp.sum(weights, axis=-1, keepdims=True)
        acc_out[0] = acc_in[0] * factor + jnp.dot(
            weights.astype(jnp.bfloat16), v_ref[...], preferred_element_type=jnp.float32
        )

    @pl.when(valid_ref[0] <= 0)
    def _():
        peak_out[0] = peak_in[0]
        sum_out[0] = sum_in[0]
        acc_out[0] = acc_in[0]


def attend(q_heads, key_value, key_gates, query_gates, small_count, state, valid):
    heads, rows, width = q_heads.shape
    per_small = width // DS
    groups = key_value.shape[1] // (2 * width)
    block = rows // 3 if rows % 3 == 0 and (rows // 3) % 128 == 0 else rows
    diagonal = state is None
    small_groups = small_count // per_small

    def group(h):
        return jnp.where(h < small_count, h // per_small, h - small_count + small_groups)

    per_query = pl.BlockSpec((1, block, 1), lambda h, i: (h, i, 0))
    wide = pl.BlockSpec((1, block, width), lambda h, i: (h, i, 0))
    in_specs = [
        wide,
        pl.BlockSpec((rows, width), lambda h, i: (0, group(h))),
        pl.BlockSpec((rows, width), lambda h, i: (0, groups + group(h))),
        pl.BlockSpec((1, 1, rows), lambda h, i: (h, 0, 0)),
        per_query,
    ]
    operands = [q_heads, key_value, key_value, key_gates[:, None, :], query_gates[:, :, None]]
    aliases = {}
    if not diagonal:
        in_specs = [pl.BlockSpec(memory_space=pltpu.SMEM)] + in_specs + [per_query, per_query, wide]
        operands = [valid] + operands + list(state)
        aliases = {6: 0, 7: 1, 8: 2}
    column = jax.ShapeDtypeStruct((heads, rows, 1), jnp.float32)

    def kernel(*refs):
        attend_body(small_count, diagonal, *refs)

    return pl.pallas_call(
        kernel,
        grid=(heads, rows // block),
        in_specs=in_specs,
        out_specs=[per_query, per_query, wide],
        out_shape=[column, column, jax.ShapeDtypeStruct((heads, rows, width), jnp.float32)],
        input_output_aliases=aliases,
        cost_estimate=pl.CostEstimate(
            flops=heads * rows * rows * width * 4,
            bytes_accessed=heads * rows * width * 12,
            transcendentals=heads * rows * rows,
        ),
        compiler_params=pltpu.CompilerParams(
            dimension_semantics=("arbitrary", "arbitrary"), vmem_limit_bytes=56 * 1024 * 1024
        ),
    )(*operands)


def per_device(
    query_small,
    key_small,
    value_small,
    gates_small,
    query_large,
    key_large,
    value_large,
    gates_large,
    residual,
    mixer_small,
    mixer_large,
    mix_gain,
    value_weight,
    gate_weight,
    value_taps,
    gate_taps,
    down_weight,
    final_gain,
):
    shard_rows = query_small.shape[0]
    sp_index = lax.axis_index("sp")
    tp_index = lax.axis_index("tp")
    tensor_parts = lax.axis_size("tp")
    sp_count = lax.axis_size("sp")
    splits = all(
        count % 2 == 0 and count * size % (2 * DL) == 0
        for count, size in ((gates_small.shape[1], DS), (gates_large.shape[1], DL))
    )
    team = 2 if splits and sp_count % 2 == 0 else 1
    pair_count = sp_count // team
    pair, side = sp_index // team, sp_index % team
    half_small = query_small.shape[1] // team
    small_count = gates_small.shape[1] // team
    large_count = gates_large.shape[1] // team

    def half(array, which):
        width = array.shape[1] // team
        return lax.dynamic_slice_in_dim(array, which * width, width, 1)

    def halves(parts, which):
        return jnp.concatenate([half(a, which) for a in parts], axis=1)

    def exchanged(parts):
        if team == 1:
            return jnp.concatenate(parts, axis=1)
        return in_order(halves(parts, side), swapped(halves(parts, 1 - side), "sp"), 0)

    def in_order(own, other, axis):
        return jnp.where(
            side == 0,
            jnp.concatenate([own, other], axis=axis),
            jnp.concatenate([other, own], axis=axis),
        )

    gate_parts = (gates_small, gates_large)
    key_value = exchanged((key_small, key_large, value_small, value_large))
    if team == 1:
        own_gates = jnp.concatenate(gate_parts, axis=1).T
    else:
        own_gates = in_order(
            halves(gate_parts, side).T, swapped(halves(gate_parts, 1 - side).T, "sp"), 1
        )
    queries = exchanged((query_small, query_large))

    width = DL
    per_small = width // DS
    lane_head = jnp.arange(width) // DS
    q_heads = []
    for h in range(small_count):
        columns = queries[:, (h // per_small) * width : (h // per_small + 1) * width]
        q_heads.append(jnp.where(lane_head == h % per_small, columns, 0).astype(jnp.bfloat16))
    for h in range(large_count):
        q_heads.append(queries[:, half_small + h * width : half_small + (h + 1) * width])
    q_heads = jnp.stack(q_heads)

    mixers = jnp.concatenate([mixer_small, mixer_large], axis=0)
    mixer_of = [mixers]
    for s in range(1, tensor_parts):
        mixer_of.append(rotated(mixers, "tp", -s))
    full_value = lax.all_gather(value_weight, "sp", axis=0, tiled=True)
    full_gate = lax.all_gather(gate_weight, "sp", axis=0, tiled=True)
    down_pieces = down_parts(down_weight)

    arriving, gates_arriving = [key_value], [own_gates]
    for step in range(1, pair_count):
        gates_arriving.append(passed_along(own_gates, "sp", step * team))
        arriving.append(passed_along(arriving[-1], "sp", team))
    state = attend(q_heads, key_value, own_gates, own_gates, small_count, None, None)
    for step in range(1, pair_count):
        valid = (pair >= step).astype(jnp.int32).reshape(1)
        state = attend(
            q_heads, arriving[step], gates_arriving[step], own_gates, small_count, state, valid
        )
    head_out = (state[2] / state[1]).astype(jnp.bfloat16)
    columns = []
    for g in range(small_count // per_small):
        merged = head_out[g * per_small]
        for h in range(1, per_small):
            merged = jnp.where(lane_head == h, head_out[g * per_small + h], merged)
        columns.append(merged)
    for h in range(large_count):
        columns.append(head_out[small_count + h])
    attended = jnp.concatenate(columns, axis=1)
    joined = attended
    if team == 2:
        own = lax.dynamic_slice_in_dim(attended, side * shard_rows, shard_rows, 0)
        other = swapped(
            lax.dynamic_slice_in_dim(attended, (1 - side) * shard_rows, shard_rows, 0), "sp"
        )
        joined = jnp.concatenate(
            [
                in_order(own[:, :half_small], other[:, :half_small], 1),
                in_order(own[:, half_small:], other[:, half_small:], 1),
            ],
            axis=1,
        )
    own_rows = shard_rows // tensor_parts
    arrived = lax.all_to_all(joined, "tp", split_axis=0, concat_axis=1, tiled=True)
    mix = jnp.zeros((own_rows, mixers.shape[1]), jnp.float32)
    for s in range(tensor_parts):
        source = (tp_index + s) % tensor_parts
        mix = mix + jnp.dot(
            lax.dynamic_slice_in_dim(arrived, source * joined.shape[1], joined.shape[1], 1),
            mixer_of[s],
            preferred_element_type=jnp.float32,
        )
    mixed = norm_rows(residual_scale * residual.astype(jnp.float32) + mix, mix_gain).astype(
        jnp.bfloat16
    )
    block_input = jnp.zeros((shard_rows, mixed.shape[1]), jnp.bfloat16)
    for s in range(tensor_parts):
        piece = mixed if s == 0 else rotated(mixed, "tp", -s)
        source = (tp_index + s) % tensor_parts
        block_input = lax.dynamic_update_slice_in_dim(block_input, piece, source * own_rows, 0)

    up_value = jnp.dot(block_input, full_value, preferred_element_type=jnp.float32).astype(
        jnp.bfloat16
    )
    up_gate = jnp.dot(block_input, full_gate, preferred_element_type=jnp.float32).astype(
        jnp.bfloat16
    )
    down_base, up_value = lax.optimization_barrier((down_weight, up_value))
    full_down = assembled(down_base, down_pieces)
    hidden_width = up_value.shape[1]
    trailing = jnp.concatenate([up_value[-2:], up_gate[-2:]], axis=1)
    earlier = passed_along(trailing, "sp", 1)
    padded_value = jnp.concatenate([earlier[:, :hidden_width], up_value], axis=0).astype(
        jnp.float32
    )
    padded_gate = jnp.concatenate([earlier[:, hidden_width:], up_gate], axis=0).astype(jnp.float32)
    filt_value = (
        value_taps[0] * padded_value[:-2]
        + value_taps[1] * padded_value[1:-1]
        + value_taps[2] * padded_value[2:]
    )
    filt_gate = (
        gate_taps[0] * padded_gate[:-2]
        + gate_taps[1] * padded_gate[1:-1]
        + gate_taps[2] * padded_gate[2:]
    )
    hidden = (jax.nn.silu(filt_gate) * filt_value).astype(jnp.bfloat16)

    def ffn_rows(s):
        target = (tp_index + s) % tensor_parts
        part = lax.dynamic_slice_in_dim(hidden, target * own_rows, own_rows, 0)
        return jnp.dot(part, full_down, preferred_element_type=jnp.float32)

    order = [tensor_parts // 2] + [s for s in range(1, tensor_parts) if s != tensor_parts // 2]
    received = [rotated(ffn_rows(s).astype(jnp.bfloat16), "tp", s) for s in order]
    ffn = ffn_rows(0)
    for part in received:
        ffn = ffn + part.astype(jnp.float32)
    return norm_rows(residual_scale * mixed.astype(jnp.float32) + ffn, final_gain).astype(
        jnp.bfloat16
    )


def down_parts(down_weight):
    pieces = []
    for s in range(1, lax.axis_size("sp")):
        pieces.append(rotated(down_weight, "sp", -s))
    return pieces


def assembled(own, pieces):
    count = lax.axis_size("sp")
    width = own.shape[1]
    index = lax.axis_index("sp")
    full = jnp.zeros((own.shape[0], count * width), own.dtype)
    for s, piece in enumerate([own] + pieces):
        full = lax.dynamic_update_slice_in_dim(full, piece, ((index + s) % count) * width, 1)
    return full


MESH = pl.DeviceIdType.MESH
LANES = 128
HALO = 16


def fits(sp_count, tp_count, arrays):
    query, gates_small, gates_large = arrays[0], arrays[3], arrays[7]
    query_large, value_weight = arrays[4], arrays[12]
    rows = query.shape[0]
    own = rows // tp_count
    return (
        tp_count == 4
        and sp_count % 4 == 0
        and sp_count >= 8
        and query.shape[1] == 2 * LANES
        and query_large.shape[1] == 2 * LANES
        and gates_small.shape[1] == 2 * LANES // DS
        and gates_large.shape[1] == 2
        and rows % (3 * LANES) == 0
        and own % (2 * HALO) == 0
        and value_weight.shape[1] % LANES == 0
        and value_weight.shape[0] % HALO == 0
        and 2 * (rows + HALO) <= 16 * LANES
        and (sp_count - 1) * value_weight.shape[0] >= half_width(value_weight.shape[1])
        and half_width(value_weight.shape[1]) >= arrays[16].shape[1]
    )


def half_width(columns):
    return -(-columns // (2 * LANES)) * LANES


class Place:
    def __init__(self):
        self.count = lax.axis_size("sp")
        self.nz = self.count // 2
        self.sp = lax.axis_index("sp")
        self.tp = lax.axis_index("tp")
        self.z, self.x = self.sp // 2, self.sp % 2
        self.y, self.c = self.tp // 2, self.tp % 2
        self.parity = self.z % 2
        self.mate = self.z + 1 - 2 * self.parity

    def at(self, z=None, x=None, y=None, c=None):
        z = self.z if z is None else z
        x = self.x if x is None else x
        y = self.y if y is None else y
        c = self.c if c is None else c
        return (z * 2 + x, y * 2 + c)


class Traffic:
    def __init__(self):
        self.sent = []

    def start(self, copy, when=None):
        guarded(when, copy.start)
        self.sent.append((copy, when))

    def drain(self):
        for copy, when in self.sent:
            guarded(when, copy.wait_send)


def guarded(when, action):
    if when is None:
        action()
    else:

        @pl.when(when)
        def _():
            action()


def remote(source, target, send, receive, device):
    return pltpu.make_async_remote_copy(
        src_ref=source,
        dst_ref=target,
        send_sem=send,
        recv_sem=receive,
        device_id=device,
        device_id_type=MESH,
    )


def front_kernel(
    qs, ql, ks, kl, vs, vl, gt, ms, ml, wv, wg, wd, res, gain, tv, tg,
    o_wv, o_wg, o_wd, o_rows, o_mixed, o_hidden,
    wv_buf, wg_buf, uv, ug, hidden, load_sem,
    q_last, gq_last, peak_last, total_last, acc_last, o_part, marks, q_send, q_recv, p_send, p_recv,
    q_buf, kv, gk, gq, peak, total, acc, o_buf, arrived, mixers, y_buf, zero,
    local_sem, x_send, x_recv, kv_send, kv_recv, g_send, g_recv,
    w_up, w_dn, w_zr, w_xs, w_xr, b_sem, m_local, m_send, m_recv,
    o_send, o_recv, a_send, a_recv, h_send, h_recv, a_local,
):
    me = Place()
    net = Traffic()
    nz, z, x, sp, tp = me.nz, me.z, me.x, me.sp, me.tp
    rows = qs.shape[0]
    own_rows = rows // 4
    other = 1 - x
    mine = pl.ds(pl.multiple_of(x * rows, LANES), rows)
    theirs = pl.ds(pl.multiple_of(other * rows, LANES), rows)
    own_lanes = pl.ds(pl.multiple_of(x * LANES, LANES), LANES)
    other_lanes = pl.ds(pl.multiple_of(other * LANES, LANES), LANES)
    weights = ((wv, o_wv), (wg, o_wg), (wd, o_wd))
    depth = wv.shape[0]
    full_width = wv.shape[1]
    width = half_width(full_width)

    def parts(which):
        return (
            (qs, q_buf.at[which, 0:LANES]),
            (ql, q_buf.at[which, LANES : 2 * LANES]),
            (ks, kv.at[z, which, 0:LANES]),
            (kl, kv.at[z, which, LANES : 2 * LANES]),
            (vs, kv.at[z, which, 2 * LANES : 3 * LANES]),
            (vl, kv.at[z, which, 3 * LANES : 4 * LANES]),
        )

    locals_ = []
    for i, (source, target) in enumerate(parts(mine)):
        locals_.append(pltpu.make_async_copy(source.at[:, own_lanes], target, local_sem.at[i]))
    locals_.append(pltpu.make_async_copy(gt.at[x], gk.at[z, :, mine], local_sem.at[6]))
    for copy in locals_:
        copy.start()

    mixer_rows = 4 * LANES
    mixer_locals = []
    for h in range(2):
        for k, source in enumerate((ms, ml)):
            row = tp * mixer_rows + (2 * h + k) * LANES
            mixer_locals.append(
                pltpu.make_async_copy(
                    source.at[h * LANES : (h + 1) * LANES],
                    mixers.at[pl.ds(row, LANES)],
                    m_local.at[2 * h + k],
                )
            )
    for copy in mixer_locals:
        copy.start()

    barrier = pltpu.get_barrier_semaphore()

    def greet(i, carry):
        @pl.when(i != sp * 4 + tp)
        def _():
            pl.semaphore_signal(
                barrier, inc=1, device_id=(i // 4, i % 4), device_id_type=MESH
            )

        return carry

    lax.fori_loop(0, 4 * me.count, greet, 0)
    pl.semaphore_wait(barrier, 4 * me.count - 1)
    for i, (source, target) in enumerate(parts(mine)):
        net.start(
            remote(source.at[:, other_lanes], target, x_send.at[i], x_recv.at[i], me.at(x=other))
        )
    net.start(
        remote(gt.at[other], gk.at[z, :, mine], x_send.at[6], x_recv.at[6], me.at(x=other))
    )

    def mixer_slot(t):
        return mixers.at[pl.ds(t * mixer_rows, mixer_rows)]

    def half_of(w, half):
        offset = pl.multiple_of(half * (full_width - width), LANES)
        source = weights[w][0]
        if w == 2:
            return source.at[pl.ds(offset, width), :]
        return source.at[:, pl.ds(offset, width)]

    def slot(w, which, zs, xs):
        shard = zs * 2 + xs
        if w == 2:
            return weights[w][1].at[which, shard]
        return weights[w][1].at[which, pl.ds(shard * depth, depth), :]

    def origin(w, which, zs, own):
        if not own:
            return slot(w, which, zs, x)
        return half_of(w, me.parity if which == 0 else 1 - me.parity)

    def both(a, b):
        return b if a is None else jnp.logical_and(a, b)

    upper, lower = jnp.minimum(z + 1, nz - 1), jnp.maximum(z - 1, 0)

    def go_up(w, e, zs, own, when=None):
        net.start(
            remote(
                origin(w, 1 - e, zs, own), slot(w, e, zs, x),
                w_up.at[w, e, zs], w_zr.at[w, e, zs], me.at(z=upper),
            ),
            both(when, z + 1 + e < nz),
        )

    def go_down(w, e, zs, own, when=None):
        net.start(
            remote(
                origin(w, 1 - e, zs, own), slot(w, e, zs, x),
                w_dn.at[w, e, zs], w_zr.at[w, e, zs], me.at(z=lower),
            ),
            both(when, z - 1 - e >= 0),
        )

    def own_up(w, when=None):
        go_up(w, 1, z, True, when)
        go_up(w, 0, z, True, when)

    def own_down(w, when=None):
        go_down(w, 1, z, True, when)
        go_down(w, 0, z, True, when)

    def send_across(w, zs, own, when=None):
        net.start(
            remote(
                origin(w, 0, zs, own), slot(w, 0, zs, x),
                w_xs.at[w, zs], w_xr.at[w, zs], me.at(x=other),
            ),
            when,
        )

    def landed(w, which, zs, when):
        copy = remote(
            slot(w, which, zs, x), slot(w, which, zs, x),
            w_up.at[w, which, zs], w_zr.at[w, which, zs], me.at(x=other),
        )
        guarded(when, copy.wait_recv)

    def up_pass(w, r, when=None):
        if r < nz:
            zs, here_ = jnp.maximum(z - r, 0), both(when, jnp.logical_and(z - r >= 0, z + 1 < nz))
            landed(w, 1, zs, here_)
            go_up(w, 0, zs, False, here_)

    def up_keep(w, r, when=None):
        if r < nz:
            zs, here_ = jnp.maximum(z - r, 0), both(when, z - r >= 0)
            landed(w, 0, zs, here_)
            go_up(w, 1, zs, False, here_)
            send_across(w, zs, False, here_)

    def down_pass(w, r, when=None):
        if r < nz:
            zs, here_ = jnp.minimum(z + r, nz - 1), both(when, jnp.logical_and(z + r < nz, z >= 1))
            landed(w, 1, zs, here_)
            go_down(w, 0, zs, False, here_)

    def down_keep(w, r, when=None):
        if r < nz:
            zs, here_ = jnp.minimum(z + r, nz - 1), both(when, z + r < nz)
            landed(w, 0, zs, here_)
            go_down(w, 1, zs, False, here_)
            send_across(w, zs, False, here_)

    def piece(j, p):
        span = mine if p == 0 else theirs
        return kv.at[j, span, :], gk.at[j, :, span]

    def pass_on(j, p, when):
        data, gate = piece(j, p)
        above = me.at(z=jnp.minimum(z + 1, nz - 1))
        net.start(remote(data, data, kv_send.at[j, p], kv_recv.at[j, p], above), when)
        net.start(remote(gate, gate, g_send.at[j, p], g_recv.at[j, p], above), when)

    def take(j, p, when):
        data, gate = piece(j, p)
        above = me.at(z=jnp.minimum(z + 1, nz - 1))
        guarded(when, remote(data, data, kv_send.at[j, p], kv_recv.at[j, p], above).wait_recv)
        guarded(when, remote(gate, gate, g_send.at[j, p], g_recv.at[j, p], above).wait_recv)

    def relay(r, p):
        if r > nz - 2:
            return
        j = jnp.maximum(z - r, 0)
        take(j, p, z - r >= 0)
        if r < nz - 2:
            pass_on(j, p, jnp.logical_and(z - r >= 0, z + 1 < nz))

    block = 2 * rows // 3
    count = 3

    def head_facts(h):
        lanes = lax.broadcasted_iota(jnp.int32, (1, LANES), 1)
        low = jnp.where(h == 1, DS, 0)
        high = jnp.where(h == 0, DS, LANES)
        keep = jnp.logical_and(lanes >= low, lanes < high)
        column = pl.multiple_of(jnp.where(h == 2, LANES, 0), LANES)
        scale = jnp.where(h == 2, DL ** (-0.5), DS ** (-0.5)).astype(jnp.float32)
        return keep, column, scale

    def query_part(h, span, queries=None):
        keep, column, scale = head_facts(h)
        q = (q_buf if queries is None else queries)[span, pl.ds(column, LANES)]
        return jnp.where(keep, q, jnp.zeros_like(q)), column, scale

    def shifted_scores(q, j, h, column, scale, keys):
        k = kv[j, keys, pl.ds(column, LANES)]
        scores = lax.dot_general(
            q, k, (((1,), (1,)), ((), ())), preferred_element_type=jnp.float32
        )
        return scores * scale - gk[j, pl.ds(h, 1), keys]

    def weighted(weights_, j, column, keys):
        v = kv[j, keys, pl.ds(column + 2 * LANES, LANES)]
        return jnp.dot(weights_.astype(jnp.bfloat16), v, preferred_element_type=jnp.float32)

    def attend_own():
        def head(h, carry):
            for i in range(count):
                span = pl.ds(i * block, block)
                keys = pl.ds(0, (i + 1) * block)
                q, column, scale = query_part(h, span)
                scores = shifted_scores(q, z, h, column, scale, keys)
                allowed = i * block + lax.broadcasted_iota(
                    jnp.int32, scores.shape, 0
                ) >= lax.broadcasted_iota(jnp.int32, scores.shape, 1)
                scores = jnp.where(allowed, scores, -jnp.inf)
                gate = gq[h, span, :]
                top = jnp.max(scores, axis=-1, keepdims=True) + gate
                weights_ = jnp.exp(scores + (gate - top))
                peak[h, span, :] = top
                total[h, span, :] = jnp.sum(weights_, axis=-1, keepdims=True)
                acc[h, span, :] = weighted(weights_, z, column, keys)
            return carry

        lax.fori_loop(0, 3, head, 0)

    own_state = (q_buf, gq, peak, total, acc)
    last_state = (q_last, gq_last, peak_last, total_last, acc_last)

    def attend_earlier(j, state):
        queries, gates, peaks, totals, sums = state

        def part(i, carry):
            h, b = i // count, i % count
            span = pl.ds(pl.multiple_of(b * block, LANES), block)
            keys = pl.ds(0, 2 * rows)
            q, column, scale = query_part(h, span, queries)
            scores = shifted_scores(q, j, h, column, scale, keys)
            gate = gates[h, span, :]
            before = peaks[h, span, :]
            top = jnp.maximum(before, jnp.max(scores, axis=-1, keepdims=True) + gate)
            factor = jnp.exp(before - top)
            weights_ = jnp.exp(scores + (gate - top))
            peaks[h, span, :] = top
            totals[h, span, :] = totals[h, span, :] * factor + jnp.sum(
                weights_, axis=-1, keepdims=True
            )
            sums[h, span, :] = sums[h, span, :] * factor + weighted(weights_, j, column, keys)
            return carry

        lax.fori_loop(0, 3 * count, part, 0)

    is_last, is_helper = z == nz - 1, z == nz - 2
    helper, ahead = me.at(z=jnp.maximum(z - 1, 0)), me.at(z=jnp.minimum(z + 1, nz - 1))

    def lend(p, send):
        span = mine if p == 0 else theirs
        gate = gk.at[nz - 1, :, span]
        for k, (source, target) in enumerate(
            ((q_buf.at[span, :], q_last.at[span, :]), (gate, gate))
        ):
            copy = remote(source, target, q_send.at[p, k], q_recv.at[p, k], helper)
            if send:
                net.start(copy, is_last)
            else:
                guarded(is_helper, copy.wait_recv)

    def part_copies():
        return (
            remote(o_part, o_part, p_send.at[0], p_recv.at[0], ahead),
            remote(marks, marks, p_send.at[1], p_recv.at[1], ahead),
        )

    def finished(totals, sums):
        first_head = sums[0] / totals[0]
        keep, _, _ = head_facts(1)
        return jnp.where(keep, sums[1] / totals[1], first_head), sums[2] / totals[2]

    def give_back():
        for n, pair in enumerate(finished(total_last, acc_last)):
            o_part[:, n * LANES : (n + 1) * LANES] = pair.astype(jnp.bfloat16)
        columns = [peak_last[h] for h in range(3)] + [total_last[h] for h in range(3)]
        lanes = lax.broadcasted_iota(jnp.int32, (1, 8), 1)
        table = jnp.zeros((2 * rows, 8), jnp.float32)
        for n, column in enumerate(columns):
            table = jnp.where(lanes == n, column, table)
        marks[...] = jnp.transpose(table)

    def merge():
        table = jnp.transpose(marks[...])
        _, _, _ = head_facts(1)
        for h in range(3):
            lane = 0 if h < 2 else LANES
            top = jnp.maximum(peak[h], table[:, h : h + 1])
            mine_, other_ = jnp.exp(peak[h] - top), jnp.exp(table[:, h : h + 1] - top)
            other_ = other_ * table[:, 3 + h : 4 + h]
            acc[h] = acc[h] * mine_ + o_part[:, lane : lane + LANES].astype(jnp.float32) * other_
            total[h] = total[h] * mine_ + other_

    ups = (0, 1)
    at_last, low_block = z == nz - 1, z <= 1
    at_one, not_one = z == 1, z != 1
    for w in ups:
        own_down(w, z + 1 < nz)
    for copy in locals_:
        copy.wait()
    pass_on(z, 0, z + 1 < nz)
    lend(0, True)
    for copy in mixer_locals:
        copy.wait()
    mixer_sends = [
        remote(mixer_slot(tp), mixer_slot(tp), m_send.at[0], m_recv.at[0], me.at(y=1 - me.y)),
        remote(mixer_slot(tp), mixer_slot(tp), m_send.at[1], m_recv.at[1], me.at(c=1 - me.c)),
    ]
    for copy in mixer_sends:
        copy.start()
    own_copies = []
    for w in range(3):
        if w == 2:
            target = wv_buf.at[depth : depth + width, 0 : wd.shape[1]]
        else:
            target = (wv_buf, wg_buf)[w].at[0:depth, :]
        own_copies.append(
            (
                pltpu.make_async_copy(half_of(w, me.parity), target, b_sem.at[w, 0]),
                pltpu.make_async_copy(target, slot(w, 0, z, x), b_sem.at[w, 1]),
            )
        )
    for first, _ in own_copies:
        first.start()
    relay(1, 0)
    for i, (source, target) in enumerate(parts(theirs)):
        remote(source.at[:, other_lanes], target, x_send.at[i], x_recv.at[i], me.at(x=other)).wait_recv()
    remote(gt.at[other], gk.at[z, :, theirs], x_send.at[6], x_recv.at[6], me.at(x=other)).wait_recv()
    pass_on(z, 1, z + 1 < nz)
    lend(1, True)
    for w in ups:
        own_down(w, at_last)
    own_down(2)
    for w in ups:
        send_across(w, z, True)
    for first, second in own_copies:
        first.wait()
        second.start()
    columns = jnp.transpose(gk[z])
    for h in range(3):
        gq[h] = columns[:, h : h + 1]
    attend_own()

    ty = (1 - me.y) * 2 + me.c
    from_y = remote(mixer_slot(ty), mixer_slot(ty), m_send.at[2], m_recv.at[0], me.at(c=1 - me.c))
    from_y.wait_recv()
    mixer_sends.append(
        remote(mixer_slot(ty), mixer_slot(ty), m_send.at[2], m_recv.at[2], me.at(c=1 - me.c))
    )
    mixer_sends[2].start()
    for r in range(1, nz):
        relay(r, 1)
        relay(r + 1, 0)
        if r == 1:
            for w in ups:
                own_up(w, low_block)
        if r == 2:
            for w in ups:
                own_up(w, z > 1)
            for w in ups:
                down_pass(w, 1)
                down_keep(w, 1)
            for w in ups:
                up_keep(w, 1, at_one)
            for w in ups:
                up_pass(w, 1, at_one)
            own_up(2, low_block)

        j = jnp.maximum(z - r, 0)
        if r == nz - 2:
            lend(0, False)
            lend(1, False)

            @pl.when(is_helper)
            def _(j=j):
                columns = jnp.transpose(gk[nz - 1])
                for h in range(3):
                    gq_last[h] = columns[:, h : h + 1]
                peak_last[...] = jnp.full_like(peak_last, -jnp.inf)
                total_last[...] = jnp.zeros_like(total_last)
                acc_last[...] = jnp.zeros_like(acc_last)
                attend_earlier(j, last_state)
                give_back()

            for copy in part_copies():
                net.start(copy, is_helper)
        if r < nz - 1:

            @pl.when(z - r >= 0)
            def _(j=j):
                attend_earlier(j, own_state)

    for copy in part_copies():
        guarded(is_last, copy.wait_recv)
    guarded(is_last, merge)
    for n, pair in enumerate(finished(total, acc)):
        o_buf[:, n * LANES : (n + 1) * LANES] = pair.astype(jnp.bfloat16)

    for w in ups:
        up_pass(w, 1, not_one)

    def arrival(t, xs):
        return arrived.at[:, pl.ds(pl.multiple_of((t * 2 + xs) * 2 * LANES, 2 * LANES), 2 * LANES)]

    takes = []
    for k in range(1, 8):
        dx, dy, dc = k // 4, (k // 2) % 2, k % 2
        x2 = x + dx * (1 - 2 * x)
        y2 = me.y + dy * (1 - 2 * me.y)
        c2 = me.c + dc * (1 - 2 * me.c)
        t2 = y2 * 2 + c2
        net.start(
            remote(
                o_buf.at[pl.ds(x2 * rows + t2 * own_rows, own_rows), :], arrival(tp, x),
                o_send.at[k], o_recv.at[k], me.at(x=x2, y=y2, c=c2),
            )
        )
        takes.append(
            remote(
                o_buf.at[pl.ds(0, own_rows), :], arrival(t2, x2),
                o_send.at[k], o_recv.at[k], me.at(x=x2, y=y2, c=c2),
            )
        )
    own_span = pl.ds(pl.multiple_of((tp * 2 + x) * 2 * LANES, 2 * LANES), 2 * LANES)
    arrived[:, own_span] = o_buf[pl.ds(pl.multiple_of(x * rows + tp * own_rows, HALO), own_rows), :]
    for w in ups:
        up_keep(w, 1, not_one)
    for w in ups:
        down_pass(w, 2)
        down_keep(w, 2)
    down_pass(2, 1)
    down_keep(2, 1)
    for w in ups:
        up_pass(w, 2)
    remote(mixer_slot(0), mixer_slot(tp + 1 - 2 * me.c), m_send.at[1], m_recv.at[1], me.at(c=1 - me.c)).wait_recv()
    remote(mixer_slot(0), mixer_slot(ty + 1 - 2 * me.c), m_send.at[2], m_recv.at[2], me.at(c=1 - me.c)).wait_recv()
    for copy in takes:
        copy.wait_recv()

    features = gain.shape[1]
    step = 4 * LANES

    def mix_tile(n, carry):
        span = pl.ds(pl.multiple_of(n * step, step), step)
        y_buf[:, span] = residual_scale * res[:, span].astype(jnp.float32) + jnp.dot(
            arrived[...], mixers[:, span], preferred_element_type=jnp.float32
        )
        return carry

    lax.fori_loop(0, features // step, mix_tile, 0)
    o_mixed[...] = norm_rows(y_buf[...], gain[...]).astype(jnp.bfloat16)
    zero[...] = jnp.zeros_like(zero)

    parity, mate = me.parity, me.mate

    def rows_of(zi, t, part=None):
        base = HALO + t * own_rows
        if part is None:
            return o_rows.at[zi, pl.ds(base, own_rows), :]
        return o_rows.at[zi, pl.ds(base + part * (own_rows // 2), own_rows // 2), :]

    here = rows_of(parity, tp)
    up_y, up_z, up_c = me.at(y=1 - me.y), me.at(z=mate), me.at(c=1 - me.c)
    net.start(remote(o_mixed, here, a_send.at[0], a_recv.at[0], up_z))
    net.start(remote(o_mixed, here, a_send.at[1], a_recv.at[1], up_y))
    net.start(remote(o_mixed, here, a_send.at[2], a_recv.at[2], up_c))
    keep_rows = pltpu.make_async_copy(o_mixed, here, a_local.at[0])
    keep_rows.start()
    following = jnp.minimum(sp + 1, me.count - 1)
    fz = following // 2
    sends_halo = jnp.logical_and(sp + 1 < me.count, tp == 3)
    for k in range(8):
        dz, dy, dc = k // 4, (k // 2) % 2, k % 2
        z2 = fz - fz % 2 + dz
        net.start(
            remote(
                o_mixed.at[own_rows - HALO : own_rows, :],
                o_rows.at[fz % 2, 0:HALO, :],
                h_send.at[k], h_recv.at[fz % 2],
                (z2 * 2 + 1 - x, dy * 2 + dc),
            ),
            sends_halo,
        )
    first_rows = jnp.logical_and(z - parity == 0, x == 0)
    blank = pltpu.make_async_copy(zero, o_rows.at[0, 0:HALO, :], a_local.at[1])
    guarded(first_rows, blank.start)

    for k in range(2, nz):
        for w in ups:
            up_keep(w, k)
            if k > 2:
                down_keep(w, k)
                up_pass(w, k)
                down_pass(w, k)

    p_z, p_y = rows_of(1 - parity, tp), rows_of(parity, ty)
    remote(o_mixed, p_y, a_send.at[1], a_recv.at[1], up_y).wait_recv()
    half = rows_of(parity, ty, 0)
    net.start(remote(half, half, a_send.at[3], a_recv.at[3], up_z))
    net.start(remote(p_y, p_y, a_send.at[5], a_recv.at[5], up_c))
    remote(o_mixed, p_z, a_send.at[0], a_recv.at[0], up_z).wait_recv()
    half = rows_of(1 - parity, tp, 1)
    net.start(remote(half, half, a_send.at[4], a_recv.at[4], up_y))
    net.start(remote(p_z, p_z, a_send.at[6], a_recv.at[6], up_c))
    for k in range(2):
        half = rows_of(1 - parity, ty, k)
        remote(half, half, a_send.at[3 + k], a_recv.at[3 + k], up_c).wait_recv()
        net.start(remote(half, half, a_send.at[7 + k], a_recv.at[7 + k], up_c))

    down_pass(2, 2)
    down_keep(2, 2)
    own_up(2, z > 1)
    send_across(2, z, True)
    up_keep(2, 1, at_one)
    up_pass(2, 1, at_one)

    tc, tyc = tp + 1 - 2 * me.c, ty + 1 - 2 * me.c
    for k, target in (
        (2, rows_of(parity, tc)),
        (5, rows_of(parity, tyc)),
        (6, rows_of(1 - parity, tc)),
        (7, rows_of(1 - parity, tyc, 0)),
        (8, rows_of(1 - parity, tyc, 1)),
    ):
        remote(target, target, a_send.at[k], a_recv.at[k], up_c).wait_recv()
    for i in range(2):
        halo = o_rows.at[i, 0:HALO, :]
        copy = remote(halo, halo, h_send.at[i], h_recv.at[i], up_c)
        guarded((z - parity + i) * 2 + x - 1 >= 0, copy.wait_recv)
    guarded(first_rows, blank.wait)
    keep_rows.wait()
    for _, second in own_copies:
        second.wait()

    def from_across(w):
        for zs in range(nz):
            target = slot(w, 0, zs, other)
            remote(target, target, w_xs.at[w, zs], w_xr.at[w, zs], me.at(x=other)).wait_recv()

    from_across(0)
    from_across(1)

    for copy in mixer_sends:
        copy.wait_send()
    tall = HALO + rows
    held = [mixers.at[b * tall : (b + 1) * tall, :] for b in range(2)]
    loads = [
        pltpu.make_async_copy(o_rows.at[1 - parity], held[0], load_sem.at[0]),
        pltpu.make_async_copy(o_wv.at[0], wv_buf, load_sem.at[1]),
        pltpu.make_async_copy(o_wg.at[0], wg_buf, load_sem.at[2]),
        pltpu.make_async_copy(o_rows.at[parity], held[1], load_sem.at[3]),
    ]
    for copy in loads:
        copy.start()
    tile = 2 * LANES
    offset = parity * (full_width - width)
    repeated = jnp.where(parity == 1, 2 * width - full_width, 0)

    def expand(b, first_tile, end_tile):
        def tile_of(n, carry):
            span = pl.ds(pl.multiple_of(n * tile, tile), tile)
            taps = pl.ds(pl.multiple_of(offset + n * tile, LANES), tile)
            filtered = []
            for buf, weight, tap in ((uv, wv_buf, tv), (ug, wg_buf, tg)):
                up = jnp.dot(held[b][...], weight[:, span], preferred_element_type=jnp.float32)
                buf[...] = up.astype(jnp.bfloat16).astype(jnp.float32)
                filtered.append(
                    tap[0:1, taps] * buf[HALO - 2 : HALO - 2 + rows, :]
                    + tap[1:2, taps] * buf[HALO - 1 : HALO - 1 + rows, :]
                    + tap[2:3, taps] * buf[HALO : HALO + rows, :]
                )
            value, gate = filtered
            result = value * (gate / (1.0 + jnp.exp(-gate)))
            unit = n * tile + lax.broadcasted_iota(jnp.int32, (1, tile), 1)
            result = jnp.where(unit >= repeated, result, 0.0)
            hidden[b, :, span] = result.astype(jnp.bfloat16)
            return carry

        lax.fori_loop(first_tile, end_tile, tile_of, 0)

    outs = [
        pltpu.make_async_copy(hidden.at[b], o_hidden.at[b], load_sem.at[4 + b]) for b in range(2)
    ]
    for copy in loads[:3]:
        copy.wait()
    up_keep(2, 1, not_one)
    up_pass(2, 1, not_one)
    inner = z < nz - 1
    up_pass(2, 2, inner)
    up_keep(2, 2, inner)
    for k in range(3, nz):
        down_pass(2, k)
        down_keep(2, k)
    tiles = width // tile
    expand(0, 0, tiles)
    outs[0].start()
    up_keep(2, 2, at_last)
    loads[3].wait()
    expand(1, 0, tiles - 1)
    for k in range(3, nz):
        up_pass(2, k)
        up_keep(2, k)
    expand(1, tiles - 1, tiles)
    outs[1].start()
    from_across(2)
    for copy in outs:
        copy.wait()
    net.drain()


def front(qs, ql, ks, kl, vs, vl, gt, ms, ml, wv, wg, wd, res, gain, tv, tg):
    count = lax.axis_size("sp")
    nz = count // 2
    rows = qs.shape[0]
    own_rows = rows // 4
    features = gain.shape[1]
    depth, width = wv.shape[0], half_width(wv.shape[1])
    down_columns = wd.shape[1]
    bf16, f32 = jnp.bfloat16, jnp.float32
    dma = pltpu.SemaphoreType.DMA
    anywhere = pl.BlockSpec(memory_space=pl.ANY)
    vmem = pl.BlockSpec(memory_space=pltpu.VMEM)
    return pl.pallas_call(
        front_kernel,
        out_shape=[
            jax.ShapeDtypeStruct((2, count * depth, width), bf16),
            jax.ShapeDtypeStruct((2, count * depth, width), bf16),
            jax.ShapeDtypeStruct((2, count, width, down_columns), bf16),
            jax.ShapeDtypeStruct((2, HALO + rows, features), bf16),
            jax.ShapeDtypeStruct((own_rows, features), bf16),
            jax.ShapeDtypeStruct((2, rows, width), bf16),
        ],
        in_specs=[anywhere] * 12 + [vmem] * 4,
        out_specs=[anywhere] * 4 + [vmem, anywhere],
        scratch_shapes=[
            pltpu.VMEM((count * depth, width), bf16),
            pltpu.VMEM((count * depth, width), bf16),
            pltpu.VMEM((HALO + rows, 2 * LANES), f32),
            pltpu.VMEM((HALO + rows, 2 * LANES), f32),
            pltpu.VMEM((2, rows, width), bf16),
            dma((6,)),
            pltpu.VMEM((2 * rows, 2 * LANES), bf16),
            pltpu.VMEM((3, 2 * rows, 1), f32),
            pltpu.VMEM((3, 2 * rows, 1), f32),
            pltpu.VMEM((3, 2 * rows, 1), f32),
            pltpu.VMEM((3, 2 * rows, LANES), f32),
            pltpu.VMEM((2 * rows, 2 * LANES), bf16),
            pltpu.VMEM((8, 2 * rows), f32),
            dma((2, 2)), dma((2, 2)), dma((2,)), dma((2,)),
            pltpu.VMEM((2 * rows, 2 * LANES), bf16),
            pltpu.VMEM((nz, 2 * rows, 4 * LANES), bf16),
            pltpu.VMEM((nz, 8, 2 * rows), f32),
            pltpu.VMEM((3, 2 * rows, 1), f32),
            pltpu.VMEM((3, 2 * rows, 1), f32),
            pltpu.VMEM((3, 2 * rows, 1), f32),
            pltpu.VMEM((3, 2 * rows, LANES), f32),
            pltpu.VMEM((2 * rows, 2 * LANES), bf16),
            pltpu.VMEM((own_rows, 16 * LANES), bf16),
            pltpu.VMEM((16 * LANES, features), bf16),
            pltpu.VMEM((own_rows, features), f32),
            pltpu.VMEM((HALO, features), bf16),
            dma((7,)), dma((7,)), dma((7,)),
            dma((nz, 2)), dma((nz, 2)), dma((nz, 2)), dma((nz, 2)),
            dma((3, 2, nz)), dma((3, 2, nz)), dma((3, 2, nz)),
            dma((3, nz)), dma((3, nz)),
            dma((3, 2)), dma((4,)), dma((3,)), dma((3,)),
            dma((8,)), dma((8,)), dma((9,)), dma((9,)), dma((8,)), dma((2,)), dma((2,)),
        ],
        compiler_params=pltpu.CompilerParams(
            collective_id=1, has_side_effects=True, vmem_limit_bytes=62 * 1024 * 1024
        ),
        name="front",
    )(qs, ql, ks, kl, vs, vl, gt, ms, ml, wv, wg, wd, res, gain, tv, tg)


def tail_kernel(
    hidden, wd, mixed, gain,
    out,
    wd_buf, own, stage, from_c, send_a, from_a, send_b, from_b,
    load_sem, c_send, c_recv, a_send, a_recv, b_send, b_recv,
):
    me = Place()
    net = Traffic()
    own_rows = mixed.shape[0]
    cut = own_rows // 2
    shards, down_columns = wd.shape[1], wd.shape[3]
    load = pltpu.make_async_copy(wd.at[0], wd_buf, load_sem.at[0])
    load.start()
    barrier = pltpu.get_barrier_semaphore()
    for device in (me.at(y=1 - me.y), me.at(z=me.mate), me.at(c=1 - me.c)):
        pl.semaphore_signal(barrier, inc=1, device_id=device, device_id_type=MESH)
    pl.semaphore_wait(barrier, 3)
    load.wait()

    def contract(b, c2, target, kind):
        part = jnp.concatenate(
            [
                hidden[b, pl.ds(pl.multiple_of((2 * y2 + c2) * own_rows, HALO), own_rows), :]
                for y2 in range(2)
            ]
        )

        def columns(n, carry):
            span = pl.ds(pl.multiple_of(n * down_columns, LANES), down_columns)
            value = jnp.dot(part, wd_buf[n], preferred_element_type=jnp.float32).astype(kind)
            target[2 * b, :, span] = value[:own_rows]
            target[2 * b + 1, :, span] = value[own_rows:]
            return carry

        lax.fori_loop(0, shards, columns, 0)

    partner = me.at(c=1 - me.c)
    to_y, to_z = me.at(y=1 - me.y), me.at(z=me.mate)
    low, high = slice(0, cut), slice(cut, own_rows)
    yo = 1 - me.y

    def to_partner(index):
        return remote(
            stage.at[index], from_c.at[index], c_send.at[index], c_recv.at[index], partner
        )

    def summed(b, y2, part):
        return own[2 * b + y2, part, :] + from_c[2 * b + y2, part, :].astype(jnp.float32)

    def first_step(k, b, y2, part, device):
        send_a[k] = summed(b, y2, part).astype(jnp.bfloat16)
        net.start(remote(send_a.at[k], from_a.at[k], a_send.at[k], a_recv.at[k], device))

    for b in range(2):
        contract(b, 1 - me.c, stage, jnp.bfloat16)
        for index in (2 * b, 2 * b + 1):
            net.start(to_partner(index))
        if b == 0:
            contract(0, me.c, own, jnp.float32)
    for index in range(2):
        to_partner(index).wait_recv()
    first_step(0, 0, yo, low, to_y)
    first_step(1, 0, yo, high, to_z)
    first_step(3, 0, me.y, high, to_z)
    contract(1, me.c, own, jnp.float32)
    for index in range(2, 4):
        to_partner(index).wait_recv()
    first_step(2, 1, yo, low, to_y)

    def wait_a(k, device):
        remote(send_a.at[k], from_a.at[k], a_send.at[k], a_recv.at[k], device).wait_recv()

    wait_a(0, to_y)
    send_b[0] = (summed(0, me.y, low) + from_a[0].astype(jnp.float32)).astype(jnp.bfloat16)
    net.start(remote(send_b.at[0], from_b.at[0], b_send.at[0], b_recv.at[0], to_z))
    wait_a(1, to_z)
    send_b[1] = (summed(1, yo, high) + from_a[1].astype(jnp.float32)).astype(jnp.bfloat16)
    net.start(remote(send_b.at[1], from_b.at[1], b_send.at[1], b_recv.at[1], to_y))
    wait_a(2, to_y)
    wait_a(3, to_z)
    for k, (part, device) in enumerate(((low, to_z), (high, to_y))):
        remote(send_b.at[k], from_b.at[k], b_send.at[k], b_recv.at[k], device).wait_recv()
        ffn = (
            summed(1, me.y, part)
            + from_a[2 + k].astype(jnp.float32)
            + from_b[k].astype(jnp.float32)
        )
        values = residual_scale * mixed[part, :].astype(jnp.float32) + ffn
        out[part, :] = norm_rows(values, gain[...]).astype(jnp.bfloat16)
    net.drain()


def tail(hidden, wd, mixed, gain):
    own_rows, features = mixed.shape
    cut = own_rows // 2
    bf16, f32 = jnp.bfloat16, jnp.float32
    dma = pltpu.SemaphoreType.DMA
    anywhere = pl.BlockSpec(memory_space=pl.ANY)
    vmem = pl.BlockSpec(memory_space=pltpu.VMEM)
    return pl.pallas_call(
        tail_kernel,
        out_shape=jax.ShapeDtypeStruct((own_rows, features), bf16),
        in_specs=[vmem, anywhere, vmem, vmem],
        out_specs=vmem,
        scratch_shapes=[
            pltpu.VMEM(wd.shape[1:], bf16),
            pltpu.VMEM((4, own_rows, features), f32),
            pltpu.VMEM((4, own_rows, features), bf16),
            pltpu.VMEM((4, own_rows, features), bf16),
            pltpu.VMEM((4, cut, features), bf16),
            pltpu.VMEM((4, cut, features), bf16),
            pltpu.VMEM((2, cut, features), bf16),
            pltpu.VMEM((2, cut, features), bf16),
            dma((1,)), dma((4,)), dma((4,)), dma((4,)), dma((4,)), dma((2,)), dma((2,)),
        ],
        compiler_params=pltpu.CompilerParams(
            collective_id=0, has_side_effects=True, vmem_limit_bytes=62 * 1024 * 1024
        ),
        name="tail",
    )(hidden, wd, mixed, gain)


def relayed(
    query_small, key_small, value_small, gates_small,
    query_large, key_large, value_large, gates_large,
    residual, mixer_small, mixer_large, mix_gain,
    value_weight, gate_weight, value_taps, gate_taps, down_weight, final_gain,
):
    rows = query_small.shape[0]
    small, large = gates_small.T, gates_large.T
    blank = jnp.zeros((5, rows), jnp.float32)
    gate_rows = jnp.stack(
        [jnp.concatenate([small[2 * h : 2 * h + 2], large[h : h + 1], blank]) for h in range(2)]
    )
    _, _, wd, _, mixed, hidden = front(
        query_small, query_large, key_small, key_large, value_small, value_large, gate_rows,
        mixer_small, mixer_large, value_weight, gate_weight, down_weight,
        residual, mix_gain[None], value_taps, gate_taps,
    )
    return tail(hidden, wd, mixed, final_gain[None])


def solution(mesh):
    in_specs = (
        P("sp", "tp"),
        P("sp", "tp"),
        P("sp", "tp"),
        P("sp", "tp"),
        P("sp", "tp"),
        P("sp", "tp"),
        P("sp", "tp"),
        P("sp", "tp"),
        P(("sp", "tp"), None),
        P("tp", None),
        P("tp", None),
        P(),
        P("sp", "tp"),
        P("sp", "tp"),
        P(None, "tp"),
        P(None, "tp"),
        P("tp", "sp"),
        P(),
    )
    out_specs = P(("sp", "tp"), None)
    sp_count, tp_count = mesh.shape["sp"], mesh.shape["tp"]

    def step(*arrays):
        if fits(sp_count, tp_count, arrays):
            return relayed(*arrays)
        return per_device(*arrays)

    return jax.shard_map(
        step, mesh=mesh, in_specs=in_specs, out_specs=out_specs, check_vma=False
    )
```
